512 devices in a mesh: sp: 64 (over z, y), tp: 8 (over x, core).
Axes of the slice: x: 4, y: 4, z: 16, core: 2. Of those that a mesh axis runs over, the one named last changes fastest.
Arguments:
- receptance: bfloat16 [12288, 1024], P('sp', 'tp'), may hold values from -6 to 6
- head_keys: bfloat16 [12288, 1024], P('sp', 'tp'), may hold values from -6 to 6
- head_values: bfloat16 [12288, 1024], P('sp', 'tp'), may hold values from -6 to 6
- decay_preact: float32 [12288, 1024], P('sp', 'tp'), may hold values from -13.5 to -0.5
- learning_rate_preact: float32 [12288, 1024], P('sp', 'tp'), may hold values from -10.5 to 2.5
- output_gate_preact: bfloat16 [12288, 1024], P('sp', 'tp'), may hold values from -8 to 8
- self_token_weight: float32 [16, 64], P('tp'), may hold values from -0.6 to 0.6
- head_norm_gain: float32 [1024], P('tp'), may hold values from 0.1 to 1.9
- output_weight: bfloat16 [1024, 2048], P('tp'), may hold values from -0.1875 to 0.1875
- residual: bfloat16 [12288, 2048], P('sp'), may hold values from -6 to 6
- premixer_norm_gain: float32 [2048], replicated, may hold values from 0.1 to 1.9
- mixer_gate_weight: bfloat16 [2048, 5120], P('sp', 'tp'), may hold values from -0.125 to 0.125
- mixer_up_weight: bfloat16 [2048, 5120], P('sp', 'tp'), may hold values from -0.125 to 0.125
- mixer_down_weight: bfloat16 [5120, 2048], P('tp', 'sp'), may hold values from -0.078125 to 0.078125
Outputs:
- layer_out: bfloat16 [12288, 2048], P(('sp', 'tp'))
The draws below stay inside these ranges and needn't reach their ends.
All inputs are finite; a program needn't handle non-finite values.
Results may differ from the reference program's by a relative error of at most 0.015.
Values may be sent and summed in bfloat16 or wider, within the bound.
A program may use at most 64 MiB of HBM per device.

```python
import jax
import jax.numpy as jnp
from jax import lax

D = 2048
WIDTH = 1024
HEAD_SIZE = 64
RECURRENT_HEADS = 16
FF = 5120
TOK_DEV = 192
TOKENS = 12288
N_TP = 8


def head_speed(key):
    chosen = jax.random.permutation(jax.random.fold_in(key, 4711), WIDTH // HEAD_SIZE)
    fast_count = WIDTH // HEAD_SIZE // 2
    return chosen < fast_count


def draw_decay_preact(key, part):
    fast_heads = head_speed(key)
    head_total = WIDTH // HEAD_SIZE
    keys_all = jax.random.split(jax.random.fold_in(key, 17), 5)
    fast_base = jax.random.uniform(keys_all[0], (head_total,), jnp.float32, -3.5, -2.5)
    slow_base = jax.random.uniform(keys_all[1], (head_total,), jnp.float32, -11.5, -10.5)
    head_base = jnp.where(fast_heads, fast_base, slow_base)
    shards = TOKENS // TOK_DEV
    block_shift = jax.random.uniform(keys_all[2], (shards, head_total), jnp.float32, -1.0, 1.0)
    block_shift = jnp.repeat(block_shift, TOK_DEV, axis=0)
    jitter = jax.random.uniform(keys_all[3], (TOKENS, head_total, HEAD_SIZE), jnp.float32, -1.0, 1.0)
    return (head_base[None, :, None] + block_shift[:, :, None] + jitter).reshape(TOKENS, WIDTH)


def draw_learning_rate_preact(key, part):
    fast_heads = head_speed(key)
    head_total = WIDTH // HEAD_SIZE
    keys_all = jax.random.split(jax.random.fold_in(key, 29), 2)
    fast_part = jax.random.uniform(keys_all[0], (TOKENS, head_total, HEAD_SIZE), jnp.float32, -2.5, 2.5)
    slow_part = jax.random.uniform(keys_all[1], (TOKENS, head_total, HEAD_SIZE), jnp.float32, -10.5, -7.5)
    return jnp.where(fast_heads[None, :, None], fast_part, slow_part).reshape(TOKENS, WIDTH)


def block_scale(own_key, dims, cuts, smallest, high):
    factor_of, own = 1.0, jax.random.fold_in(own_key, 6)
    for axis_at, shards_of in cuts:
        draws = jnp.exp(jax.random.uniform(jax.random.fold_in(own, axis_at), (shards_of,), jnp.float32, smallest / len(cuts), high / len(cuts)))
        factor_of = factor_of * jnp.repeat(draws, dims[axis_at] // shards_of).reshape([-1 if axis == axis_at else 1 for axis in range(len(dims))])
    return factor_of


def centred(key, shape, scale, most, cuts=(), held_as=jnp.bfloat16):
    drawn = jax.random.normal(key, shape, jnp.float32) * scale
    if len(cuts) > 0:
        drawn = block_scale(key, shape, cuts, -0.22, 0.18) * drawn
    return jnp.clip(drawn, min=-most, max=most).astype(held_as)


def setup_inputs(seed: int = 0) -> dict:
    keys = jax.random.split(jax.random.key(seed), 15)
    return {
        "receptance": centred(keys[0], (TOKENS, WIDTH), 1.0, 6.0, ((0, 64), (1, 8))),
        "head_keys": centred(keys[1], (TOKENS, WIDTH), 1.0, 6.0, ((0, 64), (1, 8))),
        "head_values": centred(keys[2], (TOKENS, WIDTH), 1.0, 6.0, ((0, 64), (1, 8))),
        "decay_preact": draw_decay_preact(jax.random.fold_in(keys[14], 71), 0),
        "learning_rate_preact": draw_learning_rate_preact(jax.random.fold_in(keys[14], 71), 0),
        "output_gate_preact": centred(keys[5], (TOKENS, WIDTH), 1.5, 8.0, ((0, 64), (1, 8))),
        "self_token_weight": centred(keys[6], (RECURRENT_HEADS, HEAD_SIZE), 0.1, 0.6, ((0, 8),), jnp.float32),
        "head_norm_gain": jnp.clip(1.0 + 0.18 * jax.random.normal(keys[7], (WIDTH,), jnp.float32), 0.1, 1.9),
        "output_weight": centred(keys[8], (WIDTH, D), WIDTH ** -0.5, 0.1875, ((0, 8),)),
        "residual": centred(keys[9], (TOKENS, D), 1.0, 6.0, ((0, 64),)),
        "premixer_norm_gain": jnp.clip(1.0 + 0.18 * jax.random.normal(keys[10], (D,), jnp.float32), 0.1, 1.9),
        "mixer_gate_weight": centred(keys[11], (D, FF), D ** -0.5, 0.125, ((0, 64), (1, 8))),
        "mixer_up_weight": centred(keys[12], (D, FF), D ** -0.5, 0.125, ((0, 64), (1, 8))),
        "mixer_down_weight": centred(keys[13], (FF, D), FF ** -0.5, 0.078125, ((0, 8), (1, 64))),
    }


GROUP_EPS = 0.00064
NORM_EPS = 1e-06
EXACT = lax.Precision.HIGHEST

def final_output(layer_result, receptance_rows, keys_single, values_single, self_token_weight, head_norm_gain, output_gate_preact):
    centre = lax.optimization_barrier(jnp.mean(layer_result, axis=-1, keepdims=True))
    spread = lax.optimization_barrier(jnp.mean(jnp.square(layer_result - centre), axis=-1, keepdims=True))
    scaled_rows = (layer_result - centre) * lax.rsqrt(spread + GROUP_EPS)
    self_token_term = lax.optimization_barrier(jnp.sum(receptance_rows * keys_single * self_token_weight[None], axis=-1, keepdims=True)) * values_single
    sequence_length = layer_result.shape[0]
    heads_merged = scaled_rows.reshape(sequence_length, -1) * head_norm_gain[None] + self_token_term.reshape(sequence_length, -1)
    return (heads_merged * jax.nn.sigmoid(output_gate_preact.astype(jnp.float32))).astype(jnp.bfloat16)

def reference(receptance, head_keys, head_values, decay_preact, learning_rate_preact, output_gate_preact, self_token_weight, head_norm_gain, output_weight, residual, premixer_norm_gain, mixer_gate_weight, mixer_up_weight, mixer_down_weight):
    sequence_length = receptance.shape[0]
    head_count = WIDTH // HEAD_SIZE
    layout = (sequence_length, head_count, HEAD_SIZE)
    receptance_rows = receptance.astype(jnp.float32).reshape(layout)
    keys_single = head_keys.astype(jnp.float32).reshape(layout)
    values_single = head_values.astype(jnp.float32).reshape(layout)
    decay_rate = jnp.exp(-jnp.exp(-jax.nn.softplus(-decay_preact) - 0.5)).reshape(layout)
    learn_rate = jax.nn.sigmoid(learning_rate_preact).reshape(layout)
    unit_key = keys_single / jnp.maximum(jnp.linalg.norm(keys_single, axis=-1, keepdims=True), 1.0)
    remove_dir = -unit_key
    insert_dir = unit_key * learn_rate

    def advance(memory, inputs):
        decay_t, key_t, value_t, remove_t, insert_t, recept_t = inputs
        erased = jnp.einsum('hij,hj->hi', memory, remove_t, precision=EXACT)
        memory = memory * decay_t[:, None, :] + erased[:, :, None] * insert_t[:, None, :] + value_t[:, :, None] * key_t[:, None, :]
        return (memory, jnp.einsum('hij,hj->hi', memory, recept_t, precision=EXACT))
    start_state = jnp.zeros((head_count, HEAD_SIZE, HEAD_SIZE), jnp.float32)
    _, recurrence_output = lax.scan(advance, start_state, (decay_rate, keys_single, values_single, remove_dir, insert_dir, receptance_rows))
    mixer_output = final_output(recurrence_output, receptance_rows, keys_single, values_single, self_token_weight, head_norm_gain, output_gate_preact)
    group = WIDTH // N_TP

    def add_group(total, which):
        begin = (which * group).astype(jnp.int32)
        columns = lax.dynamic_slice_in_dim(mixer_output, begin, group, 1)
        rows_part = lax.dynamic_slice_in_dim(output_weight, begin, group, 0)
        product = jnp.dot(columns.astype(jnp.float32), rows_part.astype(jnp.float32), preferred_element_type=jnp.float32)
        return (total + lax.optimization_barrier(product.astype(jnp.bfloat16)).astype(jnp.float32), None)
    mix_sum, _ = lax.scan(add_group, jnp.zeros((sequence_length, D), jnp.float32), jnp.arange(N_TP, dtype=jnp.int32))
    mix = lax.optimization_barrier(mix_sum.astype(jnp.bfloat16)).astype(jnp.float32)
    after_mix = (residual.astype(jnp.float32) + mix).astype(jnp.bfloat16)
    widened = after_mix.astype(jnp.float32)
    normed = (widened * lax.rsqrt(lax.optimization_barrier(jnp.mean(widened * widened, axis=-1, keepdims=True)) + NORM_EPS) * premixer_norm_gain[None]).astype(jnp.bfloat16)
    hidden_group = FF // N_TP

    def add_hidden(total, which):
        begin = (which * hidden_group).astype(jnp.int32)
        gate_sum = jnp.dot(normed.astype(jnp.float32), lax.dynamic_slice_in_dim(mixer_gate_weight, begin, hidden_group, 1).astype(jnp.float32), preferred_element_type=jnp.float32)
        up_sum = jnp.dot(normed.astype(jnp.float32), lax.dynamic_slice_in_dim(mixer_up_weight, begin, hidden_group, 1).astype(jnp.float32), preferred_element_type=jnp.float32)
        hidden = (jax.nn.silu(gate_sum) * up_sum).astype(jnp.bfloat16)
        product = jnp.dot(hidden.astype(jnp.float32), lax.dynamic_slice_in_dim(mixer_down_weight, begin, hidden_group, 0).astype(jnp.float32), preferred_element_type=jnp.float32)
        return (total + lax.optimization_barrier(product.astype(jnp.bfloat16)).astype(jnp.float32), None)
    down_sum, _ = lax.scan(add_hidden, jnp.zeros((sequence_length, D), jnp.float32), jnp.arange(N_TP, dtype=jnp.int32))
    return (after_mix.astype(jnp.float32) + down_sum).astype(jnp.bfloat16)
```

```python
import functools

import jax
import jax.numpy as jnp
from jax import lax
from jax.experimental import pallas as pl
from jax.experimental.pallas import tpu as pltpu
from jax.sharding import PartitionSpec as P

HEAD = 64
LANES = 2 * HEAD
GROUP_EPS = 0.00064
NORM_EPS = 1e-06
NN = (((1,), (0,)), ((), ()))
NT = (((1,), (1,)), ((), ()))
TN = (((0,), (0,)), ((), ()))
NX, NY, NZ, NC = 4, 4, 16, 2
NTP = NX * NC
NG = 4
HOPS = NZ // 2
MESH = pl.DeviceIdType.MESH
PACKET = LANES + 16


def split(x):
    high = x.astype(jnp.bfloat16)
    return high, (x - high.astype(jnp.float32)).astype(jnp.bfloat16)


def dot1(a, b, dims=NN):
    return lax.dot_general(
        a.astype(jnp.bfloat16), b.astype(jnp.bfloat16), dims, preferred_element_type=jnp.float32
    )


def dot3(a, b, dims=NN):
    ah, al = a if isinstance(a, tuple) else split(a)
    bh, bl = b if isinstance(b, tuple) else split(b)
    d = functools.partial(
        lax.dot_general, dimension_numbers=dims, preferred_element_type=jnp.float32
    )
    return d(ah, bh) + (d(ah, bl) + d(al, bh))


def per_head_sum(x, first):
    s0 = jnp.sum(jnp.where(first, x, 0.0), axis=-1, keepdims=True)
    s1 = jnp.sum(jnp.where(first, 0.0, x), axis=-1, keepdims=True)
    return jnp.where(first, s0, s1)


def block_diag_mask():
    row = lax.broadcasted_iota(jnp.int32, (LANES, LANES), 0)
    col = lax.broadcasted_iota(jnp.int32, (LANES, LANES), 1)
    return row // HEAD == col // HEAD


def fold(full):
    kept = jnp.where(block_diag_mask(), full, 0.0)
    return kept[:HEAD] + kept[HEAD:]


def unfold(packed):
    return jnp.where(block_diag_mask(), jnp.concatenate([packed, packed], axis=0), 0.0)


def fold_diag(d):
    row = lax.broadcasted_iota(jnp.int32, (HEAD, LANES), 0)
    col = lax.broadcasted_iota(jnp.int32, (HEAD, LANES), 1)
    return jnp.where(col % HEAD == row, d, 0.0)


def compose(a, b):
    both = dot3(jnp.concatenate([a[0], a[1]], axis=0), unfold(b[0]))
    return both[:HEAD], both[HEAD:] + b[1]


def put_packet(ref, slot, prod, state, decay):
    high, low = split(decay)
    row = lax.broadcasted_iota(jnp.int32, (16, LANES), 0)
    high, low = high.astype(jnp.float32), low.astype(jnp.float32)
    tail = jnp.where(row == 0, high, jnp.where(row == 1, low, 0.0))
    ref[slot, :HEAD, :] = (prod - fold_diag(decay)).astype(jnp.bfloat16)
    ref[slot, HEAD:LANES, :] = state.astype(jnp.bfloat16)
    ref[slot, LANES:, :] = tail.astype(jnp.bfloat16)


def get_packet(ref, slot):
    f32 = jnp.float32
    tail = ref[slot, LANES:, :].astype(f32)
    decay = tail[0:1] + tail[1:2]
    prod = ref[slot, :HEAD, :].astype(f32) + fold_diag(decay)
    return prod, ref[slot, HEAD:LANES, :].astype(f32), decay


def local_part(r_ref, k_ref, v_ref, dw_ref, lw_ref):
    steps = r_ref.shape[0]
    f32 = jnp.float32
    first = lax.broadcasted_iota(jnp.int32, (steps, LANES), 1) < HEAD
    row = lax.broadcasted_iota(jnp.int32, (steps, steps), 0)
    col = lax.broadcasted_iota(jnp.int32, (steps, steps), 1)
    r, k, v = (x[...].astype(f32) for x in (r_ref, k_ref, v_ref))
    log_decay = jax.nn.sigmoid(dw_ref[...]) * (-0.6065306597126334)
    ones = (row >= col).astype(jnp.bfloat16)
    h0 = log_decay.astype(jnp.bfloat16)
    rest = log_decay - h0.astype(f32)
    h1 = rest.astype(jnp.bfloat16)
    h2 = (rest - h1.astype(f32)).astype(jnp.bfloat16)
    total = dot1(ones, h0) + (dot1(ones, h1) + dot1(ones, h2))
    last = total[steps - 1 :, :]
    unit = k / jnp.maximum(jnp.sqrt(per_head_sum(k * k, first)), 1.0)
    insert = unit * jax.nn.sigmoid(lw_ref[...])
    undo = jnp.exp(-total)
    remaining = jnp.exp(last - total)
    a_bar = -unit * jnp.exp(total - log_decay)
    r_bar = r * jnp.exp(total)
    b_hat = insert * undo
    k_hat = k * undo
    right = split(jnp.concatenate([b_hat, k_hat], axis=0))
    left = jnp.concatenate([a_bar, r_bar], axis=0)
    first2 = jnp.concatenate([first, first], axis=0)
    grams = [
        dot3(jnp.where(first2 if h == 0 else ~first2, left, 0.0), right, NT) for h in (0, 1)
    ]
    strict, incl = row > col, row >= col
    ab = [jnp.where(strict, g[:steps, :steps], 0.0) for g in grams]
    ak = [jnp.where(strict, g[:steps, steps:], 0.0) for g in grams]
    rb = [jnp.where(incl, g[steps:, :steps], 0.0) for g in grams]
    rk = [jnp.where(incl, g[steps:, steps:], 0.0) for g in grams]
    vb = v_ref[...]

    def times_v(m):
        mh, ml = split(m)
        return dot1(mh, vb) + dot1(ml, vb)

    seeds = [jnp.concatenate([a_bar, times_v(m)], axis=1) for m in ak]
    ab16 = [m.astype(jnp.bfloat16) for m in ab]
    eye = (row == col).astype(f32)
    size = 1
    inv = None
    while size < steps:
        joined = (
            (row // (2 * size) == col // (2 * size))
            & ((row // size) % 2 == 1)
            & ((col // size) % 2 == 0)
        )
        parts = [jnp.where(joined, m, jnp.zeros_like(m)) for m in ab16]
        if inv is None:
            inv = [eye + p.astype(f32) for p in parts]
        else:
            t16 = [t.astype(jnp.bfloat16) for t in inv]
            mid = [dot1(t, p) for t, p in zip(t16, parts)]
            inv = [t + dot1(m, tt) for t, m, tt in zip(inv, mid, t16)]
        size *= 2
    inv16 = [t.astype(jnp.bfloat16) for t in inv]
    absp = [split(m) for m in ab]
    sol = [dot1(t, s) for t, s in zip(inv16, seeds)]
    for _ in range(2):
        res = [s - x + dot3(m, x) for s, x, m in zip(seeds, sol, absp)]
        sol = [x + dot1(t, e) for x, t, e in zip(sol, inv16, res)]
    w = jnp.where(first, sol[0][:, :LANES], sol[1][:, :LANES])
    u = jnp.where(first, sol[0][:, LANES:], sol[1][:, LANES:])
    b_end = split(insert * remaining)
    decay = jnp.exp(last)
    prod = fold(dot3(w, b_end, TN)) + fold_diag(decay)
    kh, kl = split(k * remaining)
    state = fold(dot3(u, b_end, TN) + dot1(vb, kh, TN) + dot1(vb, kl, TN))

    def outputs():
        outs = [dot3(m, x) for m, x in zip(rb, sol)]
        own = [times_v(m) for m in rk]
        q = r_bar + jnp.where(first, outs[0][:, :LANES], outs[1][:, :LANES])
        y = jnp.where(first, outs[0][:, LANES:] + own[0], outs[1][:, LANES:] + own[1])
        return q, y

    return prod, state, decay, outputs


def layer_kernel(
    r_ref, k_ref, v_ref, dw_ref, lw_ref, gate_ref, tw_ref, hg_ref, wg_ref, wu_ref, wd_ref,
    gain_ref, wo_hbm, res_hbm,
    out_ref,
    wall, wo, mixed, resid, after, normed, hid, parts, pair_in, pair_sum, last_in,
    ybuf, zbuf, gbuf, q_s, y_s, ent,
    send, r_wo, r_za, r_zb, r_ya, r_yf, r_yb, r_l1, r_l2, r_l3, r_mx, r_pair, r_last, loc,
):
    f32, bf16 = jnp.float32, jnp.bfloat16
    steps = r_ref.shape[0]
    depth, ff = wg_ref.shape
    plane = NY * depth
    half, phalf = depth // 2, plane // 2
    ca = 2 * ff
    model = wo.shape[1]
    own_rows = out_ref.shape[0]
    sp, tp = lax.axis_index("sp"), lax.axis_index("tp")
    z, y = sp // NY, sp % NY
    x, c = tp // NC, tp % NC
    zg, zl = z // NG, z % NG

    def dev(zz=None, yy=None, tt=None):
        zz = z if zz is None else zz
        yy = y if yy is None else yy
        return (zz * NY + yy, tp if tt is None else tt)

    def rcopy(src, dst, s, r, device):
        return pltpu.make_async_remote_copy(
            src_ref=src, dst_ref=dst, send_sem=s, recv_sem=r, device_id=device, device_id_type=MESH
        )

    def wait_bytes(ref, sem):
        pltpu.make_async_copy(ref, ref, sem).wait()

    up, down = (z + 1) % NZ, (z + NZ - 1) % NZ
    others_y = [dev(yy=(y + d) % NY) for d in range(1, NY)]
    others_zl = [dev(zz=zg * NG + (zl + d) % NG) for d in range(1, NG)]
    others_zg = [dev(zz=((zg + d) % NG) * NG + zl) for d in range(1, NG)]
    others_tp = [dev(tt=(tp + d) % NTP) for d in range(1, NTP)]
    ring = [dev(zz=up), dev(zz=down)]

    barrier = pltpu.get_barrier_semaphore()
    greet = others_y + others_zl + others_zg + others_tp + ring
    for d in greet:
        pl.semaphore_signal(barrier, inc=1, device_id=d, device_id_type=MESH)

    res_copy = pltpu.make_async_copy(res_hbm, resid, loc.at[0])
    res_copy.start()
    wo_rows = lambda t: wo.at[pl.ds(pl.multiple_of(t * LANES, LANES), LANES), :]
    wo_own = pltpu.make_async_copy(wo_hbm, wo_rows(tp), loc.at[1])
    wo_own.start()
    my_row = pl.multiple_of(sp * depth, depth)
    wall[pl.ds(my_row, depth), 0:ff] = wg_ref[...]
    wall[pl.ds(my_row, depth), ff:ca] = wu_ref[...]
    eye = (
        lax.broadcasted_iota(jnp.int32, (depth, depth), 0)
        == lax.broadcasted_iota(jnp.int32, (depth, depth), 1)
    ).astype(bf16)
    wall[pl.ds(my_row, depth), ca:] = dot1(eye, wd_ref[...], NT).astype(bf16)

    def rows(zz, yy, lo=0, n=None):
        return pl.ds(pl.multiple_of(zz * plane + yy * depth + lo, half), depth if n is None else n)

    def a_block(zz, yy, lo=0, n=None):
        return wall.at[rows(zz, yy, lo, n), 0:ca]

    def b_slab(zz, lo=0, n=None):
        n = plane if n is None else n
        return wall.at[pl.ds(pl.multiple_of(zz * plane + lo, phalf), n), ca:]

    def za(s):
        out = []
        for dirn in (0, 1):
            zz = (z + NZ - s) % NZ if dirn == 0 else (z + s) % NZ
            ref = a_block(zz, y) if s < HOPS - 1 else a_block(zz, y, half * dirn, half)
            out.append(rcopy(ref, ref, send.at[0], r_za.at[dirn, s], ring[dirn]))
        return out

    def zb(s):
        out = []
        for dirn in (0, 1):
            zz = (z + NZ - s) % NZ if dirn == 0 else (z + s) % NZ
            ref = b_slab(zz) if s < HOPS - 1 else b_slab(zz, phalf * dirn, phalf)
            out.append(rcopy(ref, ref, send.at[1], r_zb.at[dirn, s], ring[dirn]))
        return out

    def plane_of(i):
        if i == 0:
            return z
        s, dirn = (i - 1) // 2, (i - 1) % 2
        return (z + NZ - 1 - s) % NZ if dirn == 0 else (z + 1 + s) % NZ

    side = [dev(yy=(y + 1) % NY), dev(yy=(y + NY - 1) % NY)]

    def ya(i):
        ref = a_block(plane_of(i), y)
        return [rcopy(ref, ref, send.at[2], r_ya.at[d, i], side[d]) for d in (0, 1)]

    def yf(i):
        out = []
        for d in (0, 1):
            ref = a_block(plane_of(i), (y + NY - 1) % NY if d == 0 else (y + 1) % NY, half * d, half)
            out.append(rcopy(ref, ref, send.at[3], r_yf.at[0], side[d]))
        return out

    def start(copies):
        for cp in copies:
            cp.start()

    def wait_recv(copies):
        for cp in copies:
            cp.wait_recv()

    def yb():
        ref = wall.at[rows(z, y), ca:]
        return [rcopy(ref, ref, send.at[4], r_yb.at[d], others_y[d]) for d in range(NY - 1)]

    def exchange(buf, slot, sem, s, targets):
        return [
            rcopy(buf.at[slot], buf.at[slot], send.at[s], sem.at[d], t)
            for d, t in enumerate(targets)
        ]

    def wo_same(d):
        t = ((x + d) % NX) * NC + c
        return rcopy(wo_hbm, wo_rows(tp), send.at[5], r_wo.at[d - 1], dev(tt=t))

    partner = dev(tt=x * NC + 1 - c)

    def wo_relay(d):
        ref = wo_rows(((x + NX - d) % NX) * NC + c)
        return rcopy(ref, ref, send.at[6], r_wo.at[NX - 1], partner)

    pl.semaphore_wait(barrier, len(greet))

    for d in range(1, NX):
        wo_same(d).start()
    start(yb())
    start(za(0))
    start(ya(0))

    work = []

    def job(f, *a):
        work.append(functools.partial(f, *a))

    def b_open():
        wait_recv(yb())
        start(zb(0))

    def a_step(s):
        wait_recv(za(s))
        if s < HOPS - 1:
            start(za(s + 1))
        for i in [2 * s + 1, 2 * s + 2] if s < HOPS - 1 else [2 * s + 1]:
            start(ya(i))

    def b_step(s):
        wait_recv(zb(s))
        if s < HOPS - 1:
            start(zb(s + 1))

    def f_step(s):
        for i in [0] if s < 0 else [2 * s + 1, 2 * s + 2] if s < HOPS - 1 else [2 * s + 1]:
            wait_recv(ya(i))
            start(yf(i))

    job(b_open)
    job(f_step, -1)
    for s in range(HOPS):
        job(a_step, s)
        job(b_step, s)
        job(f_step, s)

    def serve(n):
        for _ in range(min(n, len(work))):
            work.pop(0)()

    prod, state, decay, outputs = local_part(r_ref, k_ref, v_ref, dw_ref, lw_ref)
    put_packet(ybuf, y, prod, state, decay)
    l1 = exchange(ybuf, y, r_l1, 7, others_y)
    start(l1)
    q, y_own = outputs()
    q_s[...] = q
    y_s[...] = y_own
    wo_own.wait()
    wo_relay(0).start()
    serve(SERVE[0])
    wait_recv(l1)

    def total(buf):
        m = [get_packet(buf, j) for j in range(4)]
        ab, cd = compose(m[0], m[1]), compose(m[2], m[3])
        return (*compose(ab, cd), (m[0][2] * m[1][2]) * (m[2][2] * m[3][2]))

    put_packet(zbuf, zl, *total(ybuf))
    l2 = exchange(zbuf, zl, r_l2, 8, others_zl)
    start(l2)
    serve(SERVE[1])
    wait_recv(l2)
    put_packet(gbuf, zg, *total(zbuf))
    l3 = exchange(gbuf, zg, r_l3, 9, others_zg)
    for d in range(1, NG):
        @pl.when(zg + d < NG)
        def _(d=d):
            l3[d - 1].start()

    def before(buf, count, begin):
        ent[...] = jnp.concatenate(begin, axis=0)

        def step(j, _):
            p, u, _ = get_packet(buf, j)
            both = dot3(ent[...], unfold(p))
            ent[0:HEAD, :] = both[:HEAD]
            ent[HEAD:, :] = both[HEAD:] + u
            return 0

        lax.fori_loop(0, count, step, 0)
        return ent[0:HEAD, :], ent[HEAD:, :]

    ident = (fold_diag(jnp.ones((1, LANES), f32)), jnp.zeros((HEAD, LANES), f32))
    entry = before(ybuf, y, before(zbuf, zl, ident))
    for d in range(1, NX):
        wo_same(d).wait_recv()
        wo_relay(d).start()
    serve(SERVE[2])
    for d in range(1, NG):
        @pl.when(zg >= d)
        def _(d=d):
            l3[d - 1].wait_recv()

    def turn(j, s):
        p, u, _ = get_packet(gbuf, j)
        return dot3(s, unfold(p)) + u

    s_in = lax.fori_loop(0, zg, turn, jnp.zeros((HEAD, LANES), f32))
    s_in = dot3(s_in, unfold(entry[0])) + entry[1]

    first = lax.broadcasted_iota(jnp.int32, (steps, LANES), 1) < HEAD
    yy = dot3(q_s[...], unfold(s_in), NT) + y_s[...]
    yy = yy - per_head_sum(yy, first) * (1.0 / HEAD)
    spread = per_head_sum(yy * yy, first) * (1.0 / HEAD)
    r, k, v = (a[...].astype(f32) for a in (r_ref, k_ref, v_ref))
    own = per_head_sum(r * k * tw_ref[...], first) * v
    yy = yy * lax.rsqrt(spread + GROUP_EPS) * hg_ref[...] + own
    mixed[tp] = (yy * jax.nn.sigmoid(gate_ref[...].astype(f32))).astype(bf16)
    mx = [
        rcopy(mixed.at[tp], mixed.at[tp], send.at[10], r_mx.at[d], t)
        for d, t in enumerate(others_tp)
    ]
    start(mx)
    serve(SERVE[3])
    wait_bytes(wo.at[0 : NX * LANES, :], r_wo.at[NX - 1])
    res_copy.wait()
    wait_recv(mx)

    wide = 256

    def project(n, ss):
        cut = pl.ds(pl.multiple_of(n * wide, wide), wide)
        lhs = jnp.concatenate([mixed[j] for j in range(NTP)], axis=1)
        mix = jnp.dot(lhs, wo[:, cut], preferred_element_type=f32)
        mix = mix.astype(bf16).astype(f32)
        a = (resid[:, cut].astype(f32) + mix).astype(bf16).astype(f32)
        after[:, cut] = a
        return ss + jnp.sum(a * a, axis=-1, keepdims=True)

    ss = lax.fori_loop(0, model // wide, project, jnp.zeros((steps, 1), f32))
    factor = lax.rsqrt(ss * (1.0 / model) + NORM_EPS)

    def scale(n, _):
        cut = pl.ds(pl.multiple_of(n * wide, wide), wide)
        normed[:, cut] = (after[:, cut] * factor * gain_ref[:, cut]).astype(bf16)
        return 0

    lax.fori_loop(0, model // wide, scale, 0)
    serve(len(work))
    wait_bytes(wall.at[0 : NZ * depth, 0:ca], r_yf.at[0])

    lo = 0
    while lo < ff:
        n = min(wide, ff - lo)
        g = jnp.dot(normed[...], wall[:, lo : lo + n], preferred_element_type=f32)
        u = jnp.dot(normed[...], wall[:, ff + lo : ff + lo + n], preferred_element_type=f32)
        hid[:, lo : lo + n] = (g / (1.0 + jnp.exp(-g)) * u).astype(bf16)
        lo += n

    def down_part(n, _):
        cut = pl.ds(pl.multiple_of(n * wide, wide), wide)
        d = lax.dot_general(hid[...], wall[cut, ca:], NT, preferred_element_type=f32)
        for t in range(NTP):
            parts[t % NC, t // NC, :, cut] = d[t * own_rows : (t + 1) * own_rows].astype(bf16)
        return 0

    lax.fori_loop(0, model // wide, down_part, 0)

    pair = rcopy(parts.at[1 - c], pair_in, send.at[11], r_pair.at[0], partner)
    pair.start()
    pair.wait_recv()
    pair_sum[...] = (parts[c].astype(f32) + pair_in[...].astype(f32)).astype(bf16)
    fin = []
    for d in range(1, NX):
        xx = (x + d) % NX
        cp = rcopy(pair_sum.at[xx], last_in.at[d - 1], send.at[12], r_last.at[d - 1], dev(tt=xx * NC + c))
        cp.start()
        fin.append(cp)
    total_down = parts[c, x].astype(f32) + pair_in[x].astype(f32)
    for d in range(1, NX):
        fin[d - 1].wait_recv()
        total_down = total_down + last_in[d - 1].astype(f32)
    mine = after[pl.ds(pl.multiple_of(tp * own_rows, 8), own_rows), :]
    out_ref[...] = (mine + total_down).astype(bf16)

    wait_bytes(wall.at[0 : (2 * HOPS - 1) * depth, 0:ca], send.at[0])
    wait_bytes(wall.at[0 : (2 * HOPS - 1) * plane, ca:], send.at[1])
    wait_bytes(wall.at[0 : 2 * NZ * depth, 0:ca], send.at[2])
    wait_bytes(wall.at[0 : NZ * depth, 0:ca], send.at[3])
    wait_bytes(wall.at[0 : (NY - 1) * depth, ca:], send.at[4])
    wait_bytes(wo.at[0 : (NX - 1) * LANES, :], send.at[5])
    wait_bytes(wo.at[0 : NX * LANES, :], send.at[6])
    wait_bytes(ybuf.at[0:3], send.at[7])
    wait_bytes(zbuf.at[0:3], send.at[8])
    for d in range(1, NG):
        @pl.when(zg + d < NG)
        def _(d=d):
            l3[d - 1].wait_send()
    wait_bytes(mixed.at[0 : NTP - 1], send.at[10])
    wait_bytes(pair_in, send.at[11])
    wait_bytes(pair_sum.at[0 : NX - 1], send.at[12])


SERVE = (3, 6, 6, 3)


def layer(r, k, v, dw, lw, gate, tw, hg, wg, wu, wd, gain, wo, residual):
    f32, bf16 = jnp.float32, jnp.bfloat16
    steps = r.shape[0]
    depth, ff = wg.shape
    model = residual.shape[1]
    own_rows = steps // NTP
    vmem = pl.BlockSpec(memory_space=pltpu.VMEM)
    far = pl.BlockSpec(memory_space=pl.ANY)
    dma = pltpu.SemaphoreType.DMA
    return pl.pallas_call(
        layer_kernel,
        in_specs=[vmem] * 12 + [far] * 2,
        out_specs=vmem,
        out_shape=jax.ShapeDtypeStruct((own_rows, model), bf16),
        scratch_shapes=[
            pltpu.VMEM((model, 3 * ff), bf16),
            pltpu.VMEM((NTP * LANES, model), bf16),
            pltpu.VMEM((NTP, steps, LANES), bf16),
            pltpu.VMEM((steps, model), bf16),
            pltpu.VMEM((steps, model), f32),
            pltpu.VMEM((steps, model), bf16),
            pltpu.VMEM((steps, ff), bf16),
            pltpu.VMEM((NC, NX, own_rows, model), bf16),
            pltpu.VMEM((NX, own_rows, model), bf16),
            pltpu.VMEM((NX, own_rows, model), bf16),
            pltpu.VMEM((NX - 1, own_rows, model), bf16),
            pltpu.VMEM((NY, PACKET, LANES), bf16),
            pltpu.VMEM((NG, PACKET, LANES), bf16),
            pltpu.VMEM((NG, PACKET, LANES), bf16),
            pltpu.VMEM((steps, LANES), f32),
            pltpu.VMEM((steps, LANES), f32),
            pltpu.VMEM((LANES, LANES), f32),
            dma((13,)),
            dma((NX,)),
            dma((2, HOPS)),
            dma((2, HOPS)),
            dma((2, NZ)),
            dma((1,)),
            dma((NY - 1,)),
            dma((NY - 1,)),
            dma((NG - 1,)),
            dma((NG - 1,)),
            dma((NTP - 1,)),
            dma((1,)),
            dma((NX - 1,)),
            dma((2,)),
        ],
        compiler_params=pltpu.CompilerParams(
            collective_id=0, has_side_effects=True, vmem_limit_bytes=60 * 1024 * 1024
        ),
        cost_estimate=pl.CostEstimate(
            flops=3_000_000_000, bytes_accessed=8_000_000, transcendentals=1_000_000
        ),
        name="layer",
    )(r, k, v, dw, lw, gate, tw, hg, wg, wu, wd, gain, wo, residual)


def per_device(r, k, v, dw, lw, gate, tw, hg, w_out, residual, gain, w_gate, w_up, w_down):
    return layer(
        r, k, v, dw, lw, gate, tw.reshape(1, -1), hg.reshape(1, -1), w_gate, w_up, w_down,
        gain.reshape(1, -1), w_out, residual,
    )


def solution(mesh):
    split_both = P("sp", "tp")
    placed = (split_both,) * 6 + (
        P("tp", None),
        P("tp"),
        P("tp", None),
        P("sp", None),
        P(),
        split_both,
        split_both,
        P("tp", "sp"),
    )
    return jax.shard_map(
        per_device, mesh=mesh, in_specs=placed, out_specs=P(("sp", "tp"), None), check_vma=False
    )
```

```python
import functools

import jax
import jax.numpy as jnp
from jax import lax
from jax.experimental import pallas as pl
from jax.experimental.pallas import tpu as pltpu
from jax.sharding import PartitionSpec as P

HEAD = 64
LANES = 2 * HEAD
GROUP_EPS = 0.00064
NORM_EPS = 1e-06
NN = (((1,), (0,)), ((), ()))
NT = (((1,), (1,)), ((), ()))
TN = (((0,), (0,)), ((), ()))
NX, NY, NZ, NC = 4, 4, 16, 2
NTP = NX * NC
NG = 4
HOPS = NZ // 2
MESH = pl.DeviceIdType.MESH
PACKET = LANES + 16


def split(x):
    high = x.astype(jnp.bfloat16)
    return high, (x - high.astype(jnp.float32)).astype(jnp.bfloat16)


def dot1(a, b, dims=NN):
    return lax.dot_general(
        a.astype(jnp.bfloat16), b.astype(jnp.bfloat16), dims, preferred_element_type=jnp.float32
    )


def dot3(a, b, dims=NN):
    ah, al = a if isinstance(a, tuple) else split(a)
    bh, bl = b if isinstance(b, tuple) else split(b)
    d = functools.partial(
        lax.dot_general, dimension_numbers=dims, preferred_element_type=jnp.float32
    )
    return d(ah, bh) + (d(ah, bl) + d(al, bh))


def per_head_sum(x, first):
    s0 = jnp.sum(jnp.where(first, x, 0.0), axis=-1, keepdims=True)
    s1 = jnp.sum(jnp.where(first, 0.0, x), axis=-1, keepdims=True)
    return jnp.where(first, s0, s1)


def block_diag_mask():
    row = lax.broadcasted_iota(jnp.int32, (LANES, LANES), 0)
    col = lax.broadcasted_iota(jnp.int32, (LANES, LANES), 1)
    return row // HEAD == col // HEAD


def fold(full):
    kept = jnp.where(block_diag_mask(), full, 0.0)
    return kept[:HEAD] + kept[HEAD:]


def unfold(packed):
    return jnp.where(block_diag_mask(), jnp.concatenate([packed, packed], axis=0), 0.0)


def fold_diag(d):
    row = lax.broadcasted_iota(jnp.int32, (HEAD, LANES), 0)
    col = lax.broadcasted_iota(jnp.int32, (HEAD, LANES), 1)
    return jnp.where(col % HEAD == row, d, 0.0)


def compose(a, b):
    both = dot3(jnp.concatenate([a[0], a[1]], axis=0), unfold(b[0]))
    return both[:HEAD], both[HEAD:] + b[1]


def put_packet(ref, slot, prod, state, decay):
    high, low = split(decay)
    row = lax.broadcasted_iota(jnp.int32, (16, LANES), 0)
    high, low = high.astype(jnp.float32), low.astype(jnp.float32)
    tail = jnp.where(row == 0, high, jnp.where(row == 1, low, 0.0))
    ref[slot, :HEAD, :] = (prod - fold_diag(decay)).astype(jnp.bfloat16)
    ref[slot, HEAD:LANES, :] = state.astype(jnp.bfloat16)
    ref[slot, LANES:, :] = tail.astype(jnp.bfloat16)


def get_packet(ref, slot):
    f32 = jnp.float32
    tail = ref[slot, LANES:, :].astype(f32)
    decay = tail[0:1] + tail[1:2]
    prod = ref[slot, :HEAD, :].astype(f32) + fold_diag(decay)
    return prod, ref[slot, HEAD:LANES, :].astype(f32), decay


def local_part(r_ref, k_ref, v_ref, dw_ref, lw_ref, enter):
    steps = r_ref.shape[0]
    f32 = jnp.float32
    first = lax.broadcasted_iota(jnp.int32, (steps, LANES), 1) < HEAD
    row = lax.broadcasted_iota(jnp.int32, (steps, steps), 0)
    col = lax.broadcasted_iota(jnp.int32, (steps, steps), 1)
    r, k, v = (x[...].astype(f32) for x in (r_ref, k_ref, v_ref))
    log_decay = jax.nn.sigmoid(dw_ref[...]) * (-0.6065306597126334)
    ones = (row >= col).astype(jnp.bfloat16)
    h0 = log_decay.astype(jnp.bfloat16)
    rest = log_decay - h0.astype(f32)
    h1 = rest.astype(jnp.bfloat16)
    h2 = (rest - h1.astype(f32)).astype(jnp.bfloat16)
    total = dot1(ones, h0) + (dot1(ones, h1) + dot1(ones, h2))
    last = total[steps - 1 :, :]
    unit = k / jnp.maximum(jnp.sqrt(per_head_sum(k * k, first)), 1.0)
    insert = unit * jax.nn.sigmoid(lw_ref[...])
    undo = jnp.exp(-total)
    remaining = jnp.exp(last - total)
    a_bar = -unit * jnp.exp(total - log_decay)
    r_bar = r * jnp.exp(total)
    b_hat = insert * undo
    k_hat = k * undo
    right = split(jnp.concatenate([b_hat, k_hat], axis=0))
    left = jnp.concatenate([a_bar, r_bar], axis=0)
    first2 = jnp.concatenate([first, first], axis=0)
    grams = [
        dot3(jnp.where(first2 if h == 0 else ~first2, left, 0.0), right, NT) for h in (0, 1)
    ]
    enter()
    strict, incl = row > col, row >= col
    ab = [jnp.where(strict, g[:steps, :steps], 0.0) for g in grams]
    ak = [jnp.where(strict, g[:steps, steps:], 0.0) for g in grams]
    rb = [jnp.where(incl, g[steps:, :steps], 0.0) for g in grams]
    rk = [jnp.where(incl, g[steps:, steps:], 0.0) for g in grams]
    vb = v_ref[...]

    def times_v(m):
        mh, ml = split(m)
        return dot1(mh, vb) + dot1(ml, vb)

    seeds = [jnp.concatenate([a_bar, times_v(m)], axis=1) for m in ak]
    ab16 = [m.astype(jnp.bfloat16) for m in ab]
    eye = (row == col).astype(f32)
    size = 1
    inv = None
    while size < steps:
        joined = (
            (row // (2 * size) == col // (2 * size))
            & ((row // size) % 2 == 1)
            & ((col // size) % 2 == 0)
        )
        parts = [jnp.where(joined, m, jnp.zeros_like(m)) for m in ab16]
        if inv is None:
            inv = [eye + p.astype(f32) for p in parts]
        else:
            t16 = [t.astype(jnp.bfloat16) for t in inv]
            mid = [dot1(t, p) for t, p in zip(t16, parts)]
            inv = [t + dot1(m, tt) for t, m, tt in zip(inv, mid, t16)]
        size *= 2
    inv16 = [t.astype(jnp.bfloat16) for t in inv]
    absp = [split(m) for m in ab]
    sol = [dot1(t, s) for t, s in zip(inv16, seeds)]
    for _ in range(2):
        res = [s - x + dot3(m, x) for s, x, m in zip(seeds, sol, absp)]
        sol = [x + dot1(t, e) for x, t, e in zip(sol, inv16, res)]
    w = jnp.where(first, sol[0][:, :LANES], sol[1][:, :LANES])
    u = jnp.where(first, sol[0][:, LANES:], sol[1][:, LANES:])
    b_end = split(insert * remaining)
    decay = jnp.exp(last)
    prod = fold(dot3(w, b_end, TN)) + fold_diag(decay)
    kh, kl = split(k * remaining)
    state = fold(dot3(u, b_end, TN) + dot1(vb, kh, TN) + dot1(vb, kl, TN))

    def outputs():
        outs = [dot3(m, x) for m, x in zip(rb, sol)]
        own = [times_v(m) for m in rk]
        q = r_bar + jnp.where(first, outs[0][:, :LANES], outs[1][:, :LANES])
        y = jnp.where(first, outs[0][:, LANES:] + own[0], outs[1][:, LANES:] + own[1])
        return q, y

    return prod, state, decay, outputs


def layer_kernel(
    r_hbm, k_hbm, v_hbm, dw_hbm, lw_hbm, gate_hbm, tw_hbm, hg_hbm, gain_hbm, wg_hbm, wu_hbm, wd_hbm,
    wo_hbm, res_hbm,
    out_ref,
    wall, wo, mixed, resid, after, normed, hid, parts, pair_in, pair_sum, last_in,
    r_ref, k_ref, v_ref, dw_ref, lw_ref, gate_ref, tw_ref, hg_ref, gain_ref,
    ybuf, zbuf, gbuf, q_s, y_s, ent,
    send, r_wo, r_z, r_q, r_y0, r_ya, r_yb, r_l1, r_l2, r_l3, x_l3, r_l4, x_l4, r_mx, r_pair, r_last, loc,
):
    f32, bf16 = jnp.float32, jnp.bfloat16
    steps = r_ref.shape[0]
    depth, ff = wg_hbm.shape
    plane = NY * depth
    half = depth // 2
    ca = 2 * ff
    model = wo.shape[1]
    own_rows = out_ref.shape[0]
    sp, tp = lax.axis_index("sp"), lax.axis_index("tp")
    z, y = sp // NY, sp % NY
    x, c = tp // NC, tp % NC
    zg, zl = z // NG, z % NG

    def dev(zz=None, yy=None, tt=None):
        zz = z if zz is None else zz
        yy = y if yy is None else yy
        return (zz * NY + yy, tp if tt is None else tt)

    def rcopy(src, dst, s, r, device):
        return pltpu.make_async_remote_copy(
            src_ref=src, dst_ref=dst, send_sem=s, recv_sem=r, device_id=device, device_id_type=MESH
        )

    def wait_bytes(ref, sem):
        pltpu.make_async_copy(ref, ref, sem).wait()

    up, down = (z + 1) % NZ, (z + NZ - 1) % NZ
    others_y = [dev(yy=(y + d) % NY) for d in range(1, NY)]
    others_zl = [dev(zz=zg * NG + (zl + d) % NG) for d in range(1, NG)]
    others_zg = [dev(zz=((zg + d) % NG) * NG + zl) for d in range(1, NG)]
    others_tp = [dev(tt=(tp + d) % NTP) for d in range(1, NTP)]
    ring = [dev(zz=up), dev(zz=down)]

    barrier = pltpu.get_barrier_semaphore()
    greet = others_y + others_zl + others_zg + others_tp + ring
    for d in greet:
        pl.semaphore_signal(barrier, inc=1, device_id=d, device_id_type=MESH)

    my_row = pl.multiple_of(sp * depth, depth)
    wo_rows = lambda t: wo.at[pl.ds(pl.multiple_of(t * LANES, LANES), LANES), :]
    loads = [
        (dw_hbm, dw_ref), (k_hbm, k_ref), (lw_hbm, lw_ref), (r_hbm, r_ref), (v_hbm, v_ref),
        (wg_hbm, wall.at[pl.ds(my_row, depth), 0:ff]),
        (wu_hbm, wall.at[pl.ds(my_row, depth), ff:ca]),
        (wd_hbm, wall.at[pl.ds(my_row, depth), ca:]),
        (gate_hbm, gate_ref), (tw_hbm, tw_ref), (hg_hbm, hg_ref), (gain_hbm, gain_ref),
        (wo_hbm, wo_rows(tp)), (res_hbm, resid),
    ]
    loads = [pltpu.make_async_copy(a, b, loc.at[i]) for i, (a, b) in enumerate(loads)]
    for cp in loads:
        cp.start()

    def rows(zz, yy, lo=0, n=None):
        return pl.ds(pl.multiple_of(zz * plane + yy * depth + lo, half), depth if n is None else n)

    y2 = (y + 2) % NY
    lane = (y, y2)
    cols = (slice(0, ff), slice(ff, ca), slice(ca, 3 * ff))

    def block(zz, yy, part, lo=0, n=None):
        return wall.at[rows(zz, yy, lo, n), cols[part]]

    def ahead(s, dirn):
        return (z + NZ - s) % NZ if dirn == 0 else (z + s) % NZ

    def plane_of(i):
        return z if i == 0 else ahead((i + 1) // 2, (i - 1) % 2)

    def zstream(st, part, s):
        out = []
        for d in (0, 1):
            at = (0, depth) if s < HOPS - 1 else (half * d, half)
            ref = block(ahead(s, d), lane[st], part, *at)
            k = 3 * st + part
            out.append(rcopy(ref, ref, send.at[k], r_z.at[k, d, s], ring[d]))
        return out

    side = [dev(yy=(y + 1) % NY), dev(yy=(y + NY - 1) % NY)]

    def yside(part, i):
        ref = block(plane_of(i), y, part)
        sems = [r_ya.at[part]] * 2 if part < DOWN else [r_yb.at[d, i] for d in (0, 1)]
        if i == 0:
            sems = [r_y0.at[part, d] for d in (0, 1)]
        return [rcopy(ref, ref, send.at[6 + part], sems[d], side[d]) for d in (0, 1)]

    def across(part):
        out = []
        for d in (0, 1):
            ref = block(z, (y + NY - 1) % NY if d == 0 else (y + 1) % NY, part, half * d, half)
            out.append(rcopy(ref, ref, send.at[9 + part], r_q.at[part, d], side[d]))
        return out

    def start(copies):
        for cp in copies:
            cp.start()

    def wait_recv(copies):
        for cp in copies:
            cp.wait_recv()

    def exchange(buf, slot, sem, s, targets):
        return [
            rcopy(buf.at[slot], buf.at[slot], send.at[s], sem.at[d], t)
            for d, t in enumerate(targets)
        ]

    def wo_same(d):
        t = ((x + d) % NX) * NC + c
        return rcopy(wo_hbm, wo_rows(tp), send.at[12], r_wo.at[d - 1], dev(tt=t))

    partner = dev(tt=x * NC + 1 - c)

    def wo_relay(d):
        ref = wo_rows(((x + NX - d) % NX) * NC + c)
        return rcopy(ref, ref, send.at[13], r_wo.at[NX - 1], partner)

    def enter():
        for cp in loads[5:8]:
            cp.wait()
        with jax.named_scope("enter"):
            pl.semaphore_wait(barrier, len(greet))
        for part in range(3):
            start(zstream(0, part, 0))
            start(yside(part, 0))
        for d in range(1, NX):
            wo_same(d).start()

    def new_at(s):
        return [2 * s + 1, 2 * s + 2] if s < HOPS - 1 else [2 * s + 1]

    def relay(part):
        wait_recv(yside(part, 0))
        start(across(part))

    def q_open(part):
        wait_recv(across(part))
        start(zstream(1, part, 0))

    def p_step(part, s):
        wait_recv(zstream(0, part, s))
        if s < HOPS - 1:
            start(zstream(0, part, s + 1))
        for i in new_at(s):
            start(yside(part, i))

    def q_step(part, s):
        wait_recv(zstream(1, part, s))
        if s < HOPS - 1:
            start(zstream(1, part, s + 1))

    work = []

    def job(f, *a):
        work.append(functools.partial(f, *a))

    for part in range(DOWN):
        job(relay, part)
        job(p_step, part, 0)
    job(relay, DOWN)
    job(q_open, 0)
    job(q_open, 1)
    job(p_step, DOWN, 0)
    job(q_open, DOWN)
    for s in range(HOPS + LAG):
        for step in (p_step, q_step):
            for part in range(3):
                t = s - LAG if part == DOWN else s
                if 0 <= t < HOPS and (step is q_step or t > 0):
                    job(step, part, t)
    a_last = [f for f in work if f.args[0] < DOWN and f.func is q_step][-1]
    b_last = [f for f in work if f.args[0] == DOWN and f.func is q_step]

    def serve(n=None, until=None):
        while work and (n is None or n > 0) and (until is None or until in work):
            f = work.pop(0)
            n = None if n is None else n - 1
            with jax.named_scope("_".join([f.func.__name__] + [str(a) for a in f.args])):
                f()

    for cp in loads[:5]:
        cp.wait()
    with jax.named_scope("local"):
        prod, state, decay, outputs = local_part(r_ref, k_ref, v_ref, dw_ref, lw_ref, enter)
        put_packet(ybuf, y, prod, state, decay)
    l1 = exchange(ybuf, y, r_l1, 14, others_y)
    start(l1)
    with jax.named_scope("local_out"):
        q, y_own = outputs()
        q_s[...] = q
        y_s[...] = y_own
    for cp in loads[8:]:
        cp.wait()
    wo_relay(0).start()
    serve(SERVE[0])
    with jax.named_scope("wait_l1"):
        wait_recv(l1)

    def total(buf):
        m = [get_packet(buf, j) for j in range(4)]
        ab, cd = compose(m[0], m[1]), compose(m[2], m[3])
        return (*compose(ab, cd), (m[0][2] * m[1][2]) * (m[2][2] * m[3][2]))

    ident = (fold_diag(jnp.ones((1, LANES), f32)), jnp.zeros((HEAD, LANES), f32))

    def before(at, buf, count):
        ent[at] = jnp.concatenate(ident, axis=0)

        def step(j, _):
            p, u, _ = get_packet(buf, j)
            both = dot3(ent[at], unfold(p))
            ent[at, 0:HEAD, :] = both[:HEAD]
            ent[at, HEAD:, :] = both[HEAD:] + u
            return 0

        lax.fori_loop(0, count, step, 0)

    put_packet(zbuf, zl, *total(ybuf))
    l2 = exchange(zbuf, zl, r_l2, 15, others_zl)
    start(l2)
    with jax.named_scope("before_y"):
        before(0, ybuf, y)
    serve(SERVE[1])
    with jax.named_scope("wait_l2"):
        wait_recv(l2)
    put_packet(gbuf, zg, *total(zbuf))
    quarter = pl.ds(pl.multiple_of(y * (LANES // NY), LANES // NY), LANES // NY)

    def far(d):
        cuts = gbuf.at[zg, quarter, :], gbuf.at[zg, LANES:, :]
        return [
            rcopy(ref, ref, x_l3.at[d - 1, i], r_l3.at[d - 1, i], others_zg[d - 1])
            for i, ref in enumerate(cuts)
        ]

    def share(d):
        ref = gbuf.at[zg - d, quarter, :]
        return [
            rcopy(ref, ref, x_l4.at[d - 1, e], r_l4.at[d - 1, e], others_y[e])
            for e in range(NY - 1)
        ]

    for d in range(1, NG):
        @pl.when(zg + d < NG)
        def _(d=d):
            start(far(d))

    with jax.named_scope("before_z"):
        before(1, zbuf, zl)
    serve(SERVE[2])
    with jax.named_scope("wait_far"):
        for d in range(1, NG):
            @pl.when(zg >= d)
            def _(d=d):
                wait_recv(far(d))
                start(share(d))
    serve(SERVE[3])
    with jax.named_scope("relay"):
        for d in range(1, NX):
            wo_same(d).wait_recv()
            wo_relay(d).start()
    with jax.named_scope("wait_l3"):
        for d in range(1, NG):
            @pl.when(zg >= d)
            def _(d=d):
                wait_recv(share(d))

    def turn(j, s):
        p, u, _ = get_packet(gbuf, j)
        return dot3(s, unfold(p)) + u

    s_in = lax.fori_loop(0, zg, turn, jnp.zeros((HEAD, LANES), f32))
    for at in (1, 0):
        s_in = dot3(s_in, unfold(ent[at, 0:HEAD, :])) + ent[at, HEAD:, :]

    first = lax.broadcasted_iota(jnp.int32, (steps, LANES), 1) < HEAD
    yy = dot3(q_s[...], unfold(s_in), NT) + y_s[...]
    yy = yy - per_head_sum(yy, first) * (1.0 / HEAD)
    spread = per_head_sum(yy * yy, first) * (1.0 / HEAD)
    r, k, v = (a[...].astype(f32) for a in (r_ref, k_ref, v_ref))
    weight = jnp.concatenate([tw_ref[0:1, :], tw_ref[1:2, :]], axis=1)
    own = per_head_sum(r * k * weight, first) * v
    yy = yy * lax.rsqrt(spread + GROUP_EPS) * hg_ref[...] + own
    mixed[tp] = (yy * jax.nn.sigmoid(gate_ref[...].astype(f32))).astype(bf16)
    mx = [
        rcopy(mixed.at[tp], mixed.at[tp], send.at[17], r_mx.at[d], t)
        for d, t in enumerate(others_tp)
    ]
    start(mx)
    serve(SERVE[4])
    with jax.named_scope("wait_mixed"):
        wait_bytes(wo.at[0 : NX * LANES, :], r_wo.at[NX - 1])
        wait_recv(mx)

    wide = 512

    def project(n, ss):
        cut = pl.ds(pl.multiple_of(n * wide, wide), wide)
        lhs = jnp.concatenate([mixed[j] for j in range(NTP)], axis=1)
        mix = jnp.dot(lhs, wo[:, cut], preferred_element_type=f32)
        mix = mix.astype(bf16).astype(f32)
        a = (resid[:, cut].astype(f32) + mix).astype(bf16).astype(f32)
        after[:, cut] = a
        return ss + jnp.sum(a * a, axis=-1, keepdims=True)

    with jax.named_scope("project"):
        ss = lax.fori_loop(0, model // wide, project, jnp.zeros((steps, 1), f32))
    factor = lax.rsqrt(ss * (1.0 / model) + NORM_EPS)

    def scale(n, _):
        cut = pl.ds(pl.multiple_of(n * wide, wide), wide)
        normed[:, cut] = (after[:, cut] * factor * gain_ref[:, cut]).astype(bf16)
        return 0

    with jax.named_scope("scale"):
        lax.fori_loop(0, model // wide, scale, 0)
    serve(until=a_last)
    serve(1)
    with jax.named_scope("wait_gate_up"):
        for part in range(DOWN):
            wait_bytes(wall.at[0 : 2 * (NZ - 1) * depth, cols[part]], r_ya.at[part])

    serve(1)
    with jax.named_scope("gate_up"):
        lo = 0
        while lo < ff:
            n = min(256, ff - lo)
            g = jnp.dot(normed[...], wall[:, lo : lo + n], preferred_element_type=f32)
            u = jnp.dot(normed[...], wall[:, ff + lo : ff + lo + n], preferred_element_type=f32)
            hid[:, lo : lo + n] = (g / (1.0 + jnp.exp(-g)) * u).astype(bf16)
            lo += n

    serve(1)

    def down_planes(lo, hi):
        for i in range(lo, hi, 2):
            both = [wall[rows(plane_of(j), 0, 0, plane), ca:] for j in range(i, min(i + 2, hi))]
            w = both[0] if len(both) == 1 else jnp.concatenate(both, axis=0)
            d = lax.dot_general(hid[...], w, NT, preferred_element_type=f32)
            for t in range(NTP):
                own = d[t * own_rows : (t + 1) * own_rows].astype(bf16)
                for j in range(len(both)):
                    parts[t % NC, i + j, t // NC] = own[:, j * plane : (j + 1) * plane]

    def pair(g):
        lo, hi = GROUPS[g]
        return rcopy(
            parts.at[1 - c, lo:hi], pair_in.at[lo:hi], send.at[18], r_pair.at[g], partner
        )

    def across_x(g):
        lo, hi = GROUPS[g]
        out = []
        for d in range(1, NX):
            xx = (x + d) % NX
            out.append(
                rcopy(
                    pair_sum.at[xx, lo:hi], last_in.at[d - 1, lo:hi], send.at[19],
                    r_last.at[d - 1, g], dev(tt=xx * NC + c),
                )
            )
        return out

    def sum_pair(g):
        with jax.named_scope(f"pair_{g}"):
            pair(g).wait_recv()
        lo, hi = GROUPS[g]
        for xx in range(NX):
            both = parts[c, lo:hi, xx].astype(f32) + pair_in[lo:hi, xx].astype(f32)
            pair_sum[xx, lo:hi] = both.astype(bf16)
        start(across_x(g))

    for g, (lo, hi) in enumerate(GROUPS):
        if g == 2 or b_last[hi // 2 - 1] in work:
            serve()
        with jax.named_scope(f"wait_down_{g}"):
            for i in range(max(lo, 1), hi):
                wait_recv(yside(DOWN, i))
        with jax.named_scope(f"down_{g}"):
            down_planes(lo, hi)
        pair(g).start()
        if g > 0:
            sum_pair(g - 1)
    sum_pair(len(GROUPS) - 1)

    my_rows = pl.ds(pl.multiple_of(tp * own_rows, 8), own_rows)
    for g, (lo, hi) in enumerate(GROUPS):
        with jax.named_scope(f"last_{g}"):
            wait_recv(across_x(g))
        for i in range(lo, hi):
            to = pl.ds(pl.multiple_of(plane_of(i) * plane, plane), plane)
            t = parts[c, i, x].astype(f32) + pair_in[i, x].astype(f32)
            for d in range(1, NX):
                t = t + last_in[d - 1, i].astype(f32)
            out_ref[:, to] = after[my_rows, to] + t

    for k in range(6):
        wait_bytes(wall.at[0 : (2 * HOPS - 1) * depth, cols[k % 3]], send.at[k])
    for part in range(3):
        wait_bytes(wall.at[0 : 2 * NZ * depth, cols[part]], send.at[6 + part])
        wait_bytes(wall.at[0:depth, cols[part]], send.at[9 + part])
    wait_bytes(wo.at[0 : (NX - 1) * LANES, :], send.at[12])
    wait_bytes(wo.at[0 : NX * LANES, :], send.at[13])
    wait_bytes(ybuf.at[0:3], send.at[14])
    wait_bytes(zbuf.at[0:3], send.at[15])
    for d in range(1, NG):
        @pl.when(zg + d < NG)
        def _(d=d):
            for cp in far(d):
                cp.wait_send()
    for d in range(1, NG):
        @pl.when(zg >= d)
        def _(d=d):
            for cp in share(d):
                cp.wait_send()
    wait_bytes(mixed.at[0 : NTP - 1], send.at[17])
    wait_bytes(pair_in, send.at[18])
    wait_bytes(pair_sum.at[0 : NX - 1], send.at[19])


DOWN = 2
LAG = 2
GROUPS = ((0, 5), (5, 9), (9, 13), (13, 15), (15, 16))
VMEM_MB = 58
SERVE = (4, 5, 11, 6, 9)


def layer(r, k, v, dw, lw, gate, tw, hg, wg, wu, wd, gain, wo, residual):
    f32, bf16 = jnp.float32, jnp.bfloat16
    steps = r.shape[0]
    depth, ff = wg.shape
    model = residual.shape[1]
    own_rows = steps // NTP
    vmem = pl.BlockSpec(memory_space=pltpu.VMEM)
    dma = pltpu.SemaphoreType.DMA
    return pl.pallas_call(
        layer_kernel,
        in_specs=[pl.BlockSpec(memory_space=pltpu.HBM)] * 14,
        out_specs=vmem,
        out_shape=pltpu.VMEM((own_rows, model), f32),
        scratch_shapes=[
            pltpu.VMEM((model, 3 * ff), bf16),
            pltpu.VMEM((NTP * LANES, model), bf16),
            pltpu.VMEM((NTP, steps, LANES), bf16),
            pltpu.VMEM((steps, model), bf16),
            pltpu.VMEM((steps, model), f32),
            pltpu.VMEM((steps, model), bf16),
            pltpu.VMEM((steps, ff), bf16),
            pltpu.VMEM((NC, NZ, NX, own_rows, LANES), bf16),
            pltpu.VMEM((NZ, NX, own_rows, LANES), bf16),
            pltpu.VMEM((NX, NZ, own_rows, LANES), bf16),
            pltpu.VMEM((NX - 1, NZ, own_rows, LANES), bf16),
            *[pltpu.VMEM(a.shape, a.dtype) for a in (r, k, v, dw, lw, gate, tw, hg, gain)],
            pltpu.VMEM((NY, PACKET, LANES), bf16),
            pltpu.VMEM((NG, PACKET, LANES), bf16),
            pltpu.VMEM((NG, PACKET, LANES), bf16),
            pltpu.VMEM((steps, LANES), f32),
            pltpu.VMEM((steps, LANES), f32),
            pltpu.VMEM((2, LANES, LANES), f32),
            dma((20,)),
            dma((NX,)),
            dma((6, 2, HOPS)),
            dma((3, 2)),
            dma((3, 2)),
            dma((DOWN,)),
            dma((2, NZ)),
            dma((NY - 1,)),
            dma((NG - 1,)),
            dma((NG - 1, 2)),
            dma((NG - 1, 2)),
            dma((NG - 1, NY - 1)),
            dma((NG - 1, NY - 1)),
            dma((NTP - 1,)),
            dma((len(GROUPS),)),
            dma((NX - 1, len(GROUPS))),
            dma((14,)),
        ],
        compiler_params=pltpu.CompilerParams(
            collective_id=0, has_side_effects=True, vmem_limit_bytes=VMEM_MB * 1024 * 1024
        ),
        cost_estimate=pl.CostEstimate(
            flops=3_000_000_000, bytes_accessed=8_000_000, transcendentals=1_000_000
        ),
        name="layer",
    )(r, k, v, dw, lw, gate, tw, hg, gain, wg, wu, wd, wo, residual)


def per_device(r, k, v, dw, lw, gate, tw, hg, w_out, residual, gain, w_gate, w_up, w_down):
    return layer(
        r, k, v, dw, lw, gate, tw, hg.reshape(1, -1), w_gate, w_up, w_down.T,
        gain.reshape(1, -1), w_out, residual,
    ).astype(jnp.bfloat16)


def solution(mesh):
    split_both = P("sp", "tp")
    placed = (split_both,) * 6 + (
        P("tp", None),
        P("tp"),
        P("tp", None),
        P("sp", None),
        P(),
        split_both,
        split_both,
        P("tp", "sp"),
    )
    return jax.shard_map(
        per_device, mesh=mesh, in_specs=placed, out_specs=P(("sp", "tp"), None), check_vma=False
    )
```

```python
import functools

import jax
import jax.numpy as jnp
from jax import lax
from jax.experimental import pallas as pl
from jax.experimental.pallas import tpu as pltpu
from jax.sharding import PartitionSpec as P

HEAD = 64
LANES = 2 * HEAD
GROUP_EPS = 0.00064
NORM_EPS = 1e-06
NN = (((1,), (0,)), ((), ()))
NT = (((1,), (1,)), ((), ()))
TN = (((0,), (0,)), ((), ()))
NX, NY, NZ, NC = 4, 4, 16, 2
NTP = NX * NC
NG = 4
HOPS = NZ // 2
MESH = pl.DeviceIdType.MESH
PACKET = LANES + 16


def split(x):
    high = x.astype(jnp.bfloat16)
    return high, (x - high.astype(jnp.float32)).astype(jnp.bfloat16)


def dot1(a, b, dims=NN):
    return lax.dot_general(
        a.astype(jnp.bfloat16), b.astype(jnp.bfloat16), dims, preferred_element_type=jnp.float32
    )


def dot3(a, b, dims=NN):
    ah, al = a if isinstance(a, tuple) else split(a)
    bh, bl = b if isinstance(b, tuple) else split(b)
    d = functools.partial(
        lax.dot_general, dimension_numbers=dims, preferred_element_type=jnp.float32
    )
    return d(ah, bh) + (d(ah, bl) + d(al, bh))


def per_head_sum(x, first):
    s0 = jnp.sum(jnp.where(first, x, 0.0), axis=-1, keepdims=True)
    s1 = jnp.sum(jnp.where(first, 0.0, x), axis=-1, keepdims=True)
    return jnp.where(first, s0, s1)


def block_diag_mask():
    row = lax.broadcasted_iota(jnp.int32, (LANES, LANES), 0)
    col = lax.broadcasted_iota(jnp.int32, (LANES, LANES), 1)
    return row // HEAD == col // HEAD


def fold(full):
    kept = jnp.where(block_diag_mask(), full, 0.0)
    return kept[:HEAD] + kept[HEAD:]


def unfold(packed):
    return jnp.where(block_diag_mask(), jnp.concatenate([packed, packed], axis=0), 0.0)


def fold_diag(d):
    row = lax.broadcasted_iota(jnp.int32, (HEAD, LANES), 0)
    col = lax.broadcasted_iota(jnp.int32, (HEAD, LANES), 1)
    return jnp.where(col % HEAD == row, d, 0.0)


def compose(a, b):
    both = dot3(jnp.concatenate([a[0], a[1]], axis=0), unfold(b[0]))
    return both[:HEAD], both[HEAD:] + b[1]


def put_packet(ref, slot, prod, state, decay):
    high, low = split(decay)
    row = lax.broadcasted_iota(jnp.int32, (16, LANES), 0)
    high, low = high.astype(jnp.float32), low.astype(jnp.float32)
    tail = jnp.where(row == 0, high, jnp.where(row == 1, low, 0.0))
    ref[slot, :HEAD, :] = (prod - fold_diag(decay)).astype(jnp.bfloat16)
    ref[slot, HEAD:LANES, :] = state.astype(jnp.bfloat16)
    ref[slot, LANES:, :] = tail.astype(jnp.bfloat16)


def get_packet(ref, slot):
    f32 = jnp.float32
    tail = ref[slot, LANES:, :].astype(f32)
    decay = tail[0:1] + tail[1:2]
    prod = ref[slot, :HEAD, :].astype(f32) + fold_diag(decay)
    return prod, ref[slot, HEAD:LANES, :].astype(f32), decay


def local_part(r_ref, k_ref, v_ref, dw_ref, lw_ref, between):
    steps = r_ref.shape[0]
    f32 = jnp.float32
    first = lax.broadcasted_iota(jnp.int32, (steps, LANES), 1) < HEAD
    row = lax.broadcasted_iota(jnp.int32, (steps, steps), 0)
    col = lax.broadcasted_iota(jnp.int32, (steps, steps), 1)
    r, k, v = (x[...].astype(f32) for x in (r_ref, k_ref, v_ref))
    log_decay = jax.nn.sigmoid(dw_ref[...]) * (-0.6065306597126334)
    ones = (row >= col).astype(jnp.bfloat16)
    h0 = log_decay.astype(jnp.bfloat16)
    rest = log_decay - h0.astype(f32)
    h1 = rest.astype(jnp.bfloat16)
    h2 = (rest - h1.astype(f32)).astype(jnp.bfloat16)
    total = dot1(ones, h0) + (dot1(ones, h1) + dot1(ones, h2))
    last = total[steps - 1 :, :]
    unit = k / jnp.maximum(jnp.sqrt(per_head_sum(k * k, first)), 1.0)
    insert = unit * jax.nn.sigmoid(lw_ref[...])
    undo = jnp.exp(-total)
    remaining = jnp.exp(last - total)
    a_bar = -unit * jnp.exp(total - log_decay)
    r_bar = r * jnp.exp(total)
    b_hat = insert * undo
    k_hat = k * undo
    right = split(jnp.concatenate([b_hat, k_hat], axis=0))
    left = jnp.concatenate([a_bar, r_bar], axis=0)
    first2 = jnp.concatenate([first, first], axis=0)
    grams = [
        dot3(jnp.where(first2 if h == 0 else ~first2, left, 0.0), right, NT) for h in (0, 1)
    ]
    between()
    strict, incl = row > col, row >= col
    ab = [jnp.where(strict, g[:steps, :steps], 0.0) for g in grams]
    ak = [jnp.where(strict, g[:steps, steps:], 0.0) for g in grams]
    rb = [jnp.where(incl, g[steps:, :steps], 0.0) for g in grams]
    rk = [jnp.where(incl, g[steps:, steps:], 0.0) for g in grams]
    vb = v_ref[...]

    def times_v(m):
        mh, ml = split(m)
        return dot1(mh, vb) + dot1(ml, vb)

    seeds = [jnp.concatenate([a_bar, times_v(m)], axis=1) for m in ak]
    ab16 = [m.astype(jnp.bfloat16) for m in ab]
    eye = (row == col).astype(f32)
    size = 1
    inv = None
    while size < steps:
        joined = (
            (row // (2 * size) == col // (2 * size))
            & ((row // size) % 2 == 1)
            & ((col // size) % 2 == 0)
        )
        parts = [jnp.where(joined, m, jnp.zeros_like(m)) for m in ab16]
        if inv is None:
            inv = [eye + p.astype(f32) for p in parts]
        else:
            t16 = [t.astype(jnp.bfloat16) for t in inv]
            mid = [dot1(t, p) for t, p in zip(t16, parts)]
            inv = [t + dot1(m, tt) for t, m, tt in zip(inv, mid, t16)]
        size *= 2
    inv16 = [t.astype(jnp.bfloat16) for t in inv]
    absp = [split(m) for m in ab]
    sol = [dot1(t, s) for t, s in zip(inv16, seeds)]
    for _ in range(2):
        res = [s - x + dot3(m, x) for s, x, m in zip(seeds, sol, absp)]
        sol = [x + dot1(t, e) for x, t, e in zip(sol, inv16, res)]
    w = jnp.where(first, sol[0][:, :LANES], sol[1][:, :LANES])
    u = jnp.where(first, sol[0][:, LANES:], sol[1][:, LANES:])
    b_end = split(insert * remaining)
    decay = jnp.exp(last)
    prod = fold(dot3(w, b_end, TN)) + fold_diag(decay)
    kh, kl = split(k * remaining)
    state = fold(dot3(u, b_end, TN) + dot1(vb, kh, TN) + dot1(vb, kl, TN))

    def outputs():
        outs = [dot3(m, x) for m, x in zip(rb, sol)]
        own = [times_v(m) for m in rk]
        q = r_bar + jnp.where(first, outs[0][:, :LANES], outs[1][:, :LANES])
        y = jnp.where(first, outs[0][:, LANES:] + own[0], outs[1][:, LANES:] + own[1])
        return q, y

    return prod, state, decay, outputs


def layer_kernel(
    r_hbm, k_hbm, v_hbm, dw_hbm, lw_hbm, gate_hbm, tw_hbm, hg_hbm, gain_hbm, wg_hbm, wu_hbm, wd_hbm,
    wo_hbm, res_hbm,
    out_ref,
    wall, wo, mixed, resid, after, normed, hid, parts, pair_in, pair_sum, last_in,
    r_ref, k_ref, v_ref, dw_ref, lw_ref, gate_ref, tw_ref, hg_ref, gain_ref,
    ybuf, zbuf, gbuf, q_s, y_s, ent,
    send, r_wo, r_z, r_q, r_y0, r_ya, r_yb, r_l1, r_l2, r_l3, x_l3, r_l4, x_l4, r_mx, r_pair, r_last, loc,
):
    f32, bf16 = jnp.float32, jnp.bfloat16
    steps = r_ref.shape[0]
    depth, ff = wg_hbm.shape
    plane = NY * depth
    half = depth // 2
    ca = 2 * ff
    model = wo.shape[1]
    own_rows = out_ref.shape[0]
    sp, tp = lax.axis_index("sp"), lax.axis_index("tp")
    z, y = sp // NY, sp % NY
    x, c = tp // NC, tp % NC
    zg, zl = z // NG, z % NG

    def dev(zz=None, yy=None, tt=None):
        zz = z if zz is None else zz
        yy = y if yy is None else yy
        return (zz * NY + yy, tp if tt is None else tt)

    def rcopy(src, dst, s, r, device):
        return pltpu.make_async_remote_copy(
            src_ref=src, dst_ref=dst, send_sem=s, recv_sem=r, device_id=device, device_id_type=MESH
        )

    def wait_bytes(ref, sem):
        pltpu.make_async_copy(ref, ref, sem).wait()

    up, down = (z + 1) % NZ, (z + NZ - 1) % NZ
    others_y = [dev(yy=(y + d) % NY) for d in range(1, NY)]
    others_zl = [dev(zz=zg * NG + (zl + d) % NG) for d in range(1, NG)]
    others_zg = [dev(zz=((zg + d) % NG) * NG + zl) for d in range(1, NG)]
    others_tp = [dev(tt=(tp + d) % NTP) for d in range(1, NTP)]
    ring = [dev(zz=up), dev(zz=down)]

    barrier = pltpu.get_barrier_semaphore()
    greet = others_y + others_zl + others_zg + others_tp + ring
    for d in greet:
        pl.semaphore_signal(barrier, inc=1, device_id=d, device_id_type=MESH)

    my_row = pl.multiple_of(sp * depth, depth)
    wo_rows = lambda t: wo.at[pl.ds(pl.multiple_of(t * LANES, LANES), LANES), :]
    loads = [
        (wg_hbm, wall.at[pl.ds(my_row, depth), 0:ff]),
        (wu_hbm, wall.at[pl.ds(my_row, depth), ff:ca]),
        (wd_hbm, wall.at[pl.ds(my_row, depth), ca:]),
        (dw_hbm, dw_ref), (k_hbm, k_ref), (lw_hbm, lw_ref), (r_hbm, r_ref), (v_hbm, v_ref),
        (gate_hbm, gate_ref), (tw_hbm, tw_ref), (hg_hbm, hg_ref), (gain_hbm, gain_ref),
        (wo_hbm, wo_rows(tp)), (res_hbm, resid),
    ]
    loads = [pltpu.make_async_copy(a, b, loc.at[i]) for i, (a, b) in enumerate(loads)]
    for cp in loads[:8]:
        cp.start()

    def rows(zz, yy, lo=0, n=None):
        return pl.ds(pl.multiple_of(zz * plane + yy * depth + lo, half), depth if n is None else n)

    y2 = (y + 2) % NY
    lane = (y, y2)
    cols = (slice(0, ff), slice(ff, ca), slice(ca, 3 * ff))

    def block(zz, yy, part, lo=0, n=None):
        return wall.at[rows(zz, yy, lo, n), cols[part]]

    def ahead(s, dirn):
        return (z + NZ - s) % NZ if dirn == 0 else (z + s) % NZ

    def plane_of(i):
        return z if i == 0 else ahead((i + 1) // 2, (i - 1) % 2)

    def zstream(st, part, s):
        out = []
        for d in (0, 1):
            at = (0, depth) if s < HOPS - 1 else (half * d, half)
            ref = block(ahead(s, d), lane[st], part, *at)
            k = 3 * st + part
            out.append(rcopy(ref, ref, send.at[k], r_z.at[k, s], ring[d]))
        return out

    side = [dev(yy=(y + 1) % NY), dev(yy=(y + NY - 1) % NY)]

    def yside(part, i):
        ref = block(plane_of(i), y, part)
        group = [g for g, (lo, hi) in enumerate(GROUPS) if lo <= i < hi][0]
        sems = [r_ya.at[part] if part < DOWN else r_yb.at[group]] * 2
        if i == 0:
            sems = [r_y0.at[part]] * 2
        return [rcopy(ref, ref, send.at[6 + part], sems[d], side[d]) for d in (0, 1)]

    def across(part):
        out = []
        for d in (0, 1):
            ref = block(z, (y + NY - 1) % NY if d == 0 else (y + 1) % NY, part, half * d, half)
            out.append(rcopy(ref, ref, send.at[9 + part], r_q.at[part], side[d]))
        return out

    def start(copies):
        for cp in copies:
            cp.start()

    def wait_recv(copies):
        for cp in copies:
            cp.wait_recv()

    def exchange(buf, slot, sem, s, targets):
        return [
            rcopy(buf.at[slot], buf.at[slot], send.at[s], sem.at[0], t)
            for d, t in enumerate(targets)
        ]

    def wo_same(d):
        t = ((x + d) % NX) * NC + c
        return rcopy(wo_hbm, wo_rows(tp), send.at[12], r_wo.at[d - 1], dev(tt=t))

    partner = dev(tt=x * NC + 1 - c)

    def wo_relay(d):
        ref = wo_rows(((x + NX - d) % NX) * NC + c)
        return rcopy(ref, ref, send.at[13], r_wo.at[NX - 1], partner)

    def enter():
        for cp in loads[:3]:
            cp.wait()
        with jax.named_scope("enter"):
            pl.semaphore_wait(barrier, len(greet))
        for part in range(3):
            start(zstream(0, part, 0))
            start(yside(part, 0))
        for cp in loads[8:]:
            cp.start()
        for d in range(1, NX):
            wo_same(d).start()

    def new_at(s):
        return [2 * s + 1, 2 * s + 2] if s < HOPS - 1 else [2 * s + 1]

    def relay(part):
        wait_blocks(part, 2, r_y0.at[part])
        start(across(part))

    def wait_blocks(part, n, sem):
        wait_bytes(wall.at[0 : n * depth, cols[part]], sem)

    def q_open(part):
        wait_blocks(part, 1, r_q.at[part])
        start(zstream(1, part, 0))

    def p_step(part, s):
        wait_blocks(part, 2 if s < HOPS - 1 else 1, r_z.at[part, s])
        if s < HOPS - 1:
            start(zstream(0, part, s + 1))
        for i in new_at(s):
            start(yside(part, i))

    def q_step(part, s):
        wait_blocks(part, 2 if s < HOPS - 1 else 1, r_z.at[3 + part, s])
        if s < HOPS - 1:
            start(zstream(1, part, s + 1))

    work = []

    def job(f, *a):
        work.append(functools.partial(f, *a))

    for part in range(3):
        job(relay, part)
    for part in range(3):
        job(p_step, part, 0)
    job(q_open, 0)
    for s in range(1, HOPS + LAG + 1):
        for step, t in ((p_step, s), (q_step, s - 1)):
            for part in range(3):
                u = t - LAG if part == DOWN else t
                if (0 if step is q_step else 1) <= u < HOPS:
                    job(step, part, u)
                if s == 1 and step is p_step and part == 0:
                    job(q_open, 1)
                    job(q_open, DOWN)
    a_last = [f for f in work if f.args[0] < DOWN and f.func is q_step][-1]
    b_last = [f for f in work if f.args[0] == DOWN and f.func is q_step]

    def serve(n=None, until=None):
        while work and (n is None or n > 0) and (until is None or until in work):
            f = work.pop(0)
            n = None if n is None else n - 1
            with jax.named_scope("_".join([f.func.__name__] + [str(a) for a in f.args])):
                f()

    for cp in loads[3:8]:
        cp.wait()
    with jax.named_scope("local"):
        prod, state, decay, outputs = local_part(
            r_ref, k_ref, v_ref, dw_ref, lw_ref, enter
        )
        put_packet(ybuf, y, prod, state, decay)
    l1 = exchange(ybuf, y, r_l1, 14, others_y)
    start(l1)
    serve(SERVE[0])
    with jax.named_scope("local_out"):
        q, y_own = outputs()
        q_s[...] = q
        y_s[...] = y_own
    for cp in loads[8:]:
        cp.wait()
    wo_relay(0).start()
    serve(SERVE[1])
    with jax.named_scope("wait_l1"):
        wait_bytes(ybuf.at[0:3], r_l1.at[0])

    def total(buf):
        m = [get_packet(buf, j) for j in range(4)]
        ab, cd = compose(m[0], m[1]), compose(m[2], m[3])
        return (*compose(ab, cd), (m[0][2] * m[1][2]) * (m[2][2] * m[3][2]))

    ident = (fold_diag(jnp.ones((1, LANES), f32)), jnp.zeros((HEAD, LANES), f32))

    def before(at, buf, count):
        ent[at] = jnp.concatenate(ident, axis=0)

        def step(j, _):
            p, u, _ = get_packet(buf, j)
            both = dot3(ent[at], unfold(p))
            ent[at, 0:HEAD, :] = both[:HEAD]
            ent[at, HEAD:, :] = both[HEAD:] + u
            return 0

        lax.fori_loop(0, count, step, 0)

    put_packet(zbuf, zl, *total(ybuf))
    l2 = exchange(zbuf, zl, r_l2, 15, others_zl)
    start(l2)
    with jax.named_scope("before_y"):
        before(0, ybuf, y)
    serve(SERVE[2])
    with jax.named_scope("wait_l2"):
        wait_bytes(zbuf.at[0:3], r_l2.at[0])
    put_packet(gbuf, zg, *total(zbuf))
    quarter = pl.ds(pl.multiple_of(y * (LANES // NY), LANES // NY), LANES // NY)

    def far(d):
        cuts = gbuf.at[zg, quarter, :], gbuf.at[zg, LANES:, :]
        return [
            rcopy(ref, ref, x_l3.at[d - 1], r_l3.at[d - 1], others_zg[d - 1]) for ref in cuts
        ]

    def share(d):
        ref = gbuf.at[zg - d, quarter, :]
        return [
            rcopy(ref, ref, x_l4.at[d - 1], r_l4.at[d - 1], others_y[e])
            for e in range(NY - 1)
        ]

    for d in range(1, NG):
        @pl.when(zg + d < NG)
        def _(d=d):
            start(far(d))

    with jax.named_scope("before_z"):
        before(1, zbuf, zl)
    serve(SERVE[3])
    with jax.named_scope("wait_far"):
        for d in range(1, NG):
            @pl.when(zg >= d)
            def _(d=d):
                wait_bytes(gbuf.at[0, 0 : LANES // NY + 16, :], r_l3.at[d - 1])
                start(share(d))
    serve(SERVE[4])
    with jax.named_scope("relay"):
        for d in range(1, NX):
            wo_same(d).wait_recv()
            wo_relay(d).start()
    with jax.named_scope("wait_l3"):
        for d in range(1, NG):
            @pl.when(zg >= d)
            def _(d=d):
                wait_bytes(gbuf.at[0, 0 : LANES // NY * (NY - 1), :], r_l4.at[d - 1])

    def turn(j, s):
        p, u, _ = get_packet(gbuf, j)
        return dot3(s, unfold(p)) + u

    s_in = lax.fori_loop(0, zg, turn, jnp.zeros((HEAD, LANES), f32))
    for at in (1, 0):
        s_in = dot3(s_in, unfold(ent[at, 0:HEAD, :])) + ent[at, HEAD:, :]

    first = lax.broadcasted_iota(jnp.int32, (steps, LANES), 1) < HEAD
    yy = dot3(q_s[...], unfold(s_in), NT) + y_s[...]
    yy = yy - per_head_sum(yy, first) * (1.0 / HEAD)
    spread = per_head_sum(yy * yy, first) * (1.0 / HEAD)
    r, k, v = (a[...].astype(f32) for a in (r_ref, k_ref, v_ref))
    weight = jnp.concatenate([tw_ref[0:1, :], tw_ref[1:2, :]], axis=1)
    own = per_head_sum(r * k * weight, first) * v
    yy = yy * lax.rsqrt(spread + GROUP_EPS) * hg_ref[...] + own
    mixed[tp] = (yy * jax.nn.sigmoid(gate_ref[...].astype(f32))).astype(bf16)
    mx = [
        rcopy(mixed.at[tp], mixed.at[tp], send.at[17], r_mx.at[0], t)
        for d, t in enumerate(others_tp)
    ]
    start(mx)
    serve(SERVE[5])
    with jax.named_scope("wait_mixed"):
        wait_bytes(wo.at[0 : NX * LANES, :], r_wo.at[NX - 1])
        wait_bytes(mixed.at[0 : NTP - 1], r_mx.at[0])

    wide = 512

    def project(n, ss):
        cut = pl.ds(pl.multiple_of(n * wide, wide), wide)
        lhs = jnp.concatenate([mixed[j] for j in range(NTP)], axis=1)
        mix = jnp.dot(lhs, wo[:, cut], preferred_element_type=f32)
        mix = mix.astype(bf16).astype(f32)
        a = (resid[:, cut].astype(f32) + mix).astype(bf16).astype(f32)
        after[:, cut] = a
        return ss + jnp.sum(a * a, axis=-1, keepdims=True)

    with jax.named_scope("project"):
        ss = lax.fori_loop(0, model // wide, project, jnp.zeros((steps, 1), f32))
    factor = lax.rsqrt(ss * (1.0 / model) + NORM_EPS)

    def scale(n, _):
        cut = pl.ds(pl.multiple_of(n * wide, wide), wide)
        normed[:, cut] = (after[:, cut] * factor * gain_ref[:, cut]).astype(bf16)
        return 0

    with jax.named_scope("scale"):
        lax.fori_loop(0, model // wide, scale, 0)
    serve(until=a_last)
    serve(TAIL[0])
    with jax.named_scope("wait_gate_up"):
        for part in range(DOWN):
            wait_bytes(wall.at[0 : 2 * (NZ - 1) * depth, cols[part]], r_ya.at[part])

    with jax.named_scope("gate_up"):
        lo = 0
        while lo < ff:
            n = min(256, ff - lo)
            g = jnp.dot(normed[...], wall[:, lo : lo + n], preferred_element_type=f32)
            u = jnp.dot(normed[...], wall[:, ff + lo : ff + lo + n], preferred_element_type=f32)
            hid[:, lo : lo + n] = (g / (1.0 + jnp.exp(-g)) * u).astype(bf16)
            lo += n

    serve(TAIL[1])

    def down_planes(lo, hi):
        for i in range(lo, hi, 2):
            both = [wall[rows(plane_of(j), 0, 0, plane), ca:] for j in range(i, min(i + 2, hi))]
            w = both[0] if len(both) == 1 else jnp.concatenate(both, axis=0)
            d = lax.dot_general(hid[...], w, NT, preferred_element_type=f32)
            for t in range(NTP):
                own = d[t * own_rows : (t + 1) * own_rows].astype(bf16)
                for j in range(len(both)):
                    parts[t % NC, i + j, t // NC] = own[:, j * plane : (j + 1) * plane]

    def pair(g):
        lo, hi = GROUPS[g]
        return rcopy(
            parts.at[1 - c, lo:hi], pair_in.at[lo:hi], send.at[18], r_pair.at[g], partner
        )

    def across_x(g):
        lo, hi = GROUPS[g]
        out = []
        for d in range(1, NX):
            xx = (x + d) % NX
            out.append(
                rcopy(
                    pair_sum.at[xx, lo:hi], last_in.at[d - 1, lo:hi], send.at[19],
                    r_last.at[g], dev(tt=xx * NC + c),
                )
            )
        return out

    def sum_pair(g):
        with jax.named_scope(f"pair_{g}"):
            pair(g).wait_recv()
        lo, hi = GROUPS[g]
        for xx in range(NX):
            both = parts[c, lo:hi, xx].astype(f32) + pair_in[lo:hi, xx].astype(f32)
            pair_sum[xx, lo:hi] = both.astype(bf16)
        start(across_x(g))

    for g, (lo, hi) in enumerate(GROUPS):
        if b_last[hi // 2 - 1] in work:
            serve(until=b_last[hi // 2 - 1])
        with jax.named_scope(f"wait_down_{g}"):
            wait_blocks(DOWN, 2 * (hi - max(lo, 1)), r_yb.at[g])
        with jax.named_scope(f"down_{g}"):
            down_planes(lo, hi)
        pair(g).start()
        if g > 0:
            sum_pair(g - 1)
    sum_pair(len(GROUPS) - 1)

    my_rows = pl.ds(pl.multiple_of(tp * own_rows, 8), own_rows)
    for g, (lo, hi) in enumerate(GROUPS):
        with jax.named_scope(f"last_{g}"):
            wait_bytes(last_in.at[:, lo:hi], r_last.at[g])
        for i in range(lo, hi):
            to = pl.ds(pl.multiple_of(plane_of(i) * plane, plane), plane)
            t = parts[c, i, x].astype(f32) + pair_in[i, x].astype(f32)
            for d in range(1, NX):
                t = t + last_in[d - 1, i].astype(f32)
            out_ref[:, to] = after[my_rows, to] + t

    drain = jax.named_scope("drain")
    drain.__enter__()
    for k in range(6):
        wait_bytes(wall.at[0 : (2 * HOPS - 1) * depth, cols[k % 3]], send.at[k])
    for part in range(3):
        wait_bytes(wall.at[0 : 2 * NZ * depth, cols[part]], send.at[6 + part])
        wait_bytes(wall.at[0:depth, cols[part]], send.at[9 + part])
    wait_bytes(wo.at[0 : (NX - 1) * LANES, :], send.at[12])
    wait_bytes(wo.at[0 : NX * LANES, :], send.at[13])
    wait_bytes(ybuf.at[0:3], send.at[14])
    wait_bytes(zbuf.at[0:3], send.at[15])
    for d in range(1, NG):
        @pl.when(zg + d < NG)
        def _(d=d):
            wait_bytes(gbuf.at[0, 0 : LANES // NY + 16, :], x_l3.at[d - 1])
    for d in range(1, NG):
        @pl.when(zg >= d)
        def _(d=d):
            wait_bytes(gbuf.at[0, 0 : LANES // NY * (NY - 1), :], x_l4.at[d - 1])
    wait_bytes(mixed.at[0 : NTP - 1], send.at[17])
    wait_bytes(pair_in, send.at[18])
    wait_bytes(pair_sum.at[0 : NX - 1], send.at[19])
    drain.__exit__(None, None, None)


DOWN = 2
LAG = 1
GROUPS = ((0, 5), (5, 9), (9, 13), (13, 15), (15, 16))
VMEM_MB = 58
SERVE = (6, 1, 6, 9, 6, 9)
TAIL = (0, 1)


def layer(r, k, v, dw, lw, gate, tw, hg, wg, wu, wd, gain, wo, residual):
    f32, bf16 = jnp.float32, jnp.bfloat16
    steps = r.shape[0]
    depth, ff = wg.shape
    model = residual.shape[1]
    own_rows = steps // NTP
    vmem = pl.BlockSpec(memory_space=pltpu.VMEM)
    dma = pltpu.SemaphoreType.DMA
    return pl.pallas_call(
        layer_kernel,
        in_specs=[pl.BlockSpec(memory_space=pltpu.HBM)] * 14,
        out_specs=vmem,
        out_shape=pltpu.VMEM((own_rows, model), f32),
        scratch_shapes=[
            pltpu.VMEM((model, 3 * ff), bf16),
            pltpu.VMEM((NTP * LANES, model), bf16),
            pltpu.VMEM((NTP, steps, LANES), bf16),
            pltpu.VMEM((steps, model), bf16),
            pltpu.VMEM((steps, model), f32),
            pltpu.VMEM((steps, model), bf16),
            pltpu.VMEM((steps, ff), bf16),
            pltpu.VMEM((NC, NZ, NX, own_rows, LANES), bf16),
            pltpu.VMEM((NZ, NX, own_rows, LANES), bf16),
            pltpu.VMEM((NX, NZ, own_rows, LANES), bf16),
            pltpu.VMEM((NX - 1, NZ, own_rows, LANES), bf16),
            *[pltpu.VMEM(a.shape, a.dtype) for a in (r, k, v, dw, lw, gate, tw, hg, gain)],
            pltpu.VMEM((NY, PACKET, LANES), bf16),
            pltpu.VMEM((NG, PACKET, LANES), bf16),
            pltpu.VMEM((NG, PACKET, LANES), bf16),
            pltpu.VMEM((steps, LANES), f32),
            pltpu.VMEM((steps, LANES), f32),
            pltpu.VMEM((2, LANES, LANES), f32),
            dma((20,)),
            dma((NX,)),
            dma((6, HOPS)),
            dma((3,)),
            dma((3,)),
            dma((DOWN,)),
            dma((len(GROUPS),)),
            dma((1,)),
            dma((1,)),
            dma((NG - 1,)),
            dma((NG - 1,)),
            dma((NG - 1,)),
            dma((NG - 1,)),
            dma((1,)),
            dma((len(GROUPS),)),
            dma((len(GROUPS),)),
            dma((14,)),
        ],
        compiler_params=pltpu.CompilerParams(
            collective_id=0, has_side_effects=True, vmem_limit_bytes=VMEM_MB * 1024 * 1024
        ),
        cost_estimate=pl.CostEstimate(
            flops=3_000_000_000, bytes_accessed=8_000_000, transcendentals=1_000_000
        ),
        name="layer",
    )(r, k, v, dw, lw, gate, tw, hg, gain, wg, wu, wd, wo, residual)


def per_device(r, k, v, dw, lw, gate, tw, hg, w_out, residual, gain, w_gate, w_up, w_down):
    return layer(
        r, k, v, dw, lw, gate, tw, hg.reshape(1, -1), w_gate, w_up, w_down.T,
        gain.reshape(1, -1), w_out, residual,
    ).astype(jnp.bfloat16)


def solution(mesh):
    split_both = P("sp", "tp")
    placed = (split_both,) * 6 + (
        P("tp", None),
        P("tp"),
        P("tp", None),
        P("sp", None),
        P(),
        split_both,
        split_both,
        P("tp", "sp"),
    )
    return jax.shard_map(
        per_device, mesh=mesh, in_specs=placed, out_specs=P(("sp", "tp"), None), check_vma=False
    )
```

```python
import functools

import jax
import jax.numpy as jnp
from jax import lax
from jax.experimental import pallas as pl
from jax.experimental.pallas import tpu as pltpu
from jax.sharding import PartitionSpec as P

HEAD = 64
LANES = 2 * HEAD
GROUP_EPS = 0.00064
NORM_EPS = 1e-06
NN = (((1,), (0,)), ((), ()))
NT = (((1,), (1,)), ((), ()))
TN = (((0,), (0,)), ((), ()))
NX, NY, NZ, NC = 4, 4, 16, 2
NTP = NX * NC
NG = 4
HOPS = NZ // 2
MESH = pl.DeviceIdType.MESH
PACKET = LANES + 16


def split(x):
    high = x.astype(jnp.bfloat16)
    return high, (x - high.astype(jnp.float32)).astype(jnp.bfloat16)


def dot1(a, b, dims=NN):
    return lax.dot_general(
        a.astype(jnp.bfloat16), b.astype(jnp.bfloat16), dims, preferred_element_type=jnp.float32
    )


def dot3(a, b, dims=NN):
    ah, al = a if isinstance(a, tuple) else split(a)
    bh, bl = b if isinstance(b, tuple) else split(b)
    d = functools.partial(
        lax.dot_general, dimension_numbers=dims, preferred_element_type=jnp.float32
    )
    return d(ah, bh) + (d(ah, bl) + d(al, bh))


def per_head_sum(x, first):
    s0 = jnp.sum(jnp.where(first, x, 0.0), axis=-1, keepdims=True)
    s1 = jnp.sum(jnp.where(first, 0.0, x), axis=-1, keepdims=True)
    return jnp.where(first, s0, s1)


def block_diag_mask():
    row = lax.broadcasted_iota(jnp.int32, (LANES, LANES), 0)
    col = lax.broadcasted_iota(jnp.int32, (LANES, LANES), 1)
    return row // HEAD == col // HEAD


def fold(full):
    kept = jnp.where(block_diag_mask(), full, 0.0)
    return kept[:HEAD] + kept[HEAD:]


def unfold(packed):
    return jnp.where(block_diag_mask(), jnp.concatenate([packed, packed], axis=0), 0.0)


def fold_diag(d):
    row = lax.broadcasted_iota(jnp.int32, (HEAD, LANES), 0)
    col = lax.broadcasted_iota(jnp.int32, (HEAD, LANES), 1)
    return jnp.where(col % HEAD == row, d, 0.0)


def compose(a, b):
    both = dot3(jnp.concatenate([a[0], a[1]], axis=0), unfold(b[0]))
    return both[:HEAD], both[HEAD:] + b[1]


def put_packet(ref, slot, prod, state, decay):
    high, low = split(decay)
    row = lax.broadcasted_iota(jnp.int32, (16, LANES), 0)
    high, low = high.astype(jnp.float32), low.astype(jnp.float32)
    tail = jnp.where(row == 0, high, jnp.where(row == 1, low, 0.0))
    ref[slot, :HEAD, :] = (prod - fold_diag(decay)).astype(jnp.bfloat16)
    ref[slot, HEAD:LANES, :] = state.astype(jnp.bfloat16)
    ref[slot, LANES:, :] = tail.astype(jnp.bfloat16)


def get_packet(ref, slot):
    f32 = jnp.float32
    tail = ref[slot, LANES:, :].astype(f32)
    decay = tail[0:1] + tail[1:2]
    prod = ref[slot, :HEAD, :].astype(f32) + fold_diag(decay)
    return prod, ref[slot, HEAD:LANES, :].astype(f32), decay


def local_part(r_ref, k_ref, v_ref, dw_ref, lw_ref, between):
    steps = r_ref.shape[0]
    f32 = jnp.float32
    first = lax.broadcasted_iota(jnp.int32, (steps, LANES), 1) < HEAD
    row = lax.broadcasted_iota(jnp.int32, (steps, steps), 0)
    col = lax.broadcasted_iota(jnp.int32, (steps, steps), 1)
    r, k, v = (x[...].astype(f32) for x in (r_ref, k_ref, v_ref))
    log_decay = jax.nn.sigmoid(dw_ref[...]) * (-0.6065306597126334)
    ones = (row >= col).astype(jnp.bfloat16)
    h0 = log_decay.astype(jnp.bfloat16)
    rest = log_decay - h0.astype(f32)
    h1 = rest.astype(jnp.bfloat16)
    h2 = (rest - h1.astype(f32)).astype(jnp.bfloat16)
    total = dot1(ones, h0) + (dot1(ones, h1) + dot1(ones, h2))
    last = total[steps - 1 :, :]
    unit = k / jnp.maximum(jnp.sqrt(per_head_sum(k * k, first)), 1.0)
    insert = unit * jax.nn.sigmoid(lw_ref[...])
    undo = jnp.exp(-total)
    remaining = jnp.exp(last - total)
    a_bar = -unit * jnp.exp(total - log_decay)
    r_bar = r * jnp.exp(total)
    b_hat = insert * undo
    k_hat = k * undo
    right = split(jnp.concatenate([b_hat, k_hat], axis=0))
    left = jnp.concatenate([a_bar, r_bar], axis=0)
    first2 = jnp.concatenate([first, first], axis=0)
    grams = [
        dot3(jnp.where(first2 if h == 0 else ~first2, left, 0.0), right, NT) for h in (0, 1)
    ]
    strict, incl = row > col, row >= col
    ab = [jnp.where(strict, g[:steps, :steps], 0.0) for g in grams]
    ak = [jnp.where(strict, g[:steps, steps:], 0.0) for g in grams]
    rb = [jnp.where(incl, g[steps:, :steps], 0.0) for g in grams]
    rk = [jnp.where(incl, g[steps:, steps:], 0.0) for g in grams]
    vb = v_ref[...]

    def times_v(m):
        mh, ml = split(m)
        return dot1(mh, vb) + dot1(ml, vb)

    seeds = [jnp.concatenate([a_bar, times_v(m)], axis=1) for m in ak]
    ab16 = [m.astype(jnp.bfloat16) for m in ab]
    eye = (row == col).astype(f32)
    size = 1
    inv = None
    while size < steps:
        joined = (
            (row // (2 * size) == col // (2 * size))
            & ((row // size) % 2 == 1)
            & ((col // size) % 2 == 0)
        )
        parts = [jnp.where(joined, m, jnp.zeros_like(m)) for m in ab16]
        if inv is None:
            inv = [eye + p.astype(f32) for p in parts]
        else:
            t16 = [t.astype(jnp.bfloat16) for t in inv]
            mid = [dot1(t, p) for t, p in zip(t16, parts)]
            inv = [t + dot1(m, tt) for t, m, tt in zip(inv, mid, t16)]
        size *= 2
    between()
    inv16 = [t.astype(jnp.bfloat16) for t in inv]
    absp = [split(m) for m in ab]
    sol = [dot1(t, s) for t, s in zip(inv16, seeds)]
    for _ in range(2):
        res = [s - x + dot3(m, x) for s, x, m in zip(seeds, sol, absp)]
        sol = [x + dot1(t, e) for x, t, e in zip(sol, inv16, res)]
    w = jnp.where(first, sol[0][:, :LANES], sol[1][:, :LANES])
    u = jnp.where(first, sol[0][:, LANES:], sol[1][:, LANES:])
    b_end = split(insert * remaining)
    decay = jnp.exp(last)
    prod = fold(dot3(w, b_end, TN)) + fold_diag(decay)
    kh, kl = split(k * remaining)
    state = fold(dot3(u, b_end, TN) + dot1(vb, kh, TN) + dot1(vb, kl, TN))

    def outputs():
        outs = [dot3(m, x) for m, x in zip(rb, sol)]
        own = [times_v(m) for m in rk]
        q = r_bar + jnp.where(first, outs[0][:, :LANES], outs[1][:, :LANES])
        y = jnp.where(first, outs[0][:, LANES:] + own[0], outs[1][:, LANES:] + own[1])
        return q, y

    return prod, state, decay, outputs


def layer_kernel(
    r_hbm, k_hbm, v_hbm, dw_hbm, lw_hbm, gate_hbm, tw_hbm, hg_hbm, gain_hbm, wg_hbm, wu_hbm, wd_hbm,
    wo_hbm, res_hbm,
    out_ref,
    wall, wo, mixed, resid, after, normed, hid, parts, pair_in, pair_sum, last_in,
    r_ref, k_ref, v_ref, dw_ref, lw_ref, gate_ref, tw_ref, hg_ref, gain_ref,
    ybuf, zbuf, gbuf, q_s, y_s, ent,
    send, r_wo, r_z, r_q, r_y0, r_ya, r_yb, r_l1, r_l2, r_l3, x_l3, r_l4, x_l4, r_mx, r_pair, r_last, loc, ok,
):
    f32, bf16 = jnp.float32, jnp.bfloat16
    steps = r_ref.shape[0]
    depth, ff = wg_hbm.shape
    plane = NY * depth
    half = depth // 2
    ca = 2 * ff
    model = wo.shape[1]
    own_rows = out_ref.shape[0]
    sp, tp = lax.axis_index("sp"), lax.axis_index("tp")
    z, y = sp // NY, sp % NY
    x, c = tp // NC, tp % NC
    zg, zl = z // NG, z % NG

    def dev(zz=None, yy=None, tt=None):
        zz = z if zz is None else zz
        yy = y if yy is None else yy
        return (zz * NY + yy, tp if tt is None else tt)

    def rcopy(src, dst, s, r, device):
        return pltpu.make_async_remote_copy(
            src_ref=src, dst_ref=dst, send_sem=s, recv_sem=r, device_id=device, device_id_type=MESH
        )

    def wait_bytes(ref, sem):
        pltpu.make_async_copy(ref, ref, sem).wait()

    up, down = (z + 1) % NZ, (z + NZ - 1) % NZ
    others_y = [dev(yy=(y + d) % NY) for d in range(1, NY)]
    others_zl = [dev(zz=zg * NG + (zl + d) % NG) for d in range(1, NG)]
    others_zg = [dev(zz=((zg + d) % NG) * NG + zl) for d in range(1, NG)]
    others_tp = [dev(tt=(tp + d) % NTP) for d in range(1, NTP)]
    ring = [dev(zz=up), dev(zz=down)]

    barrier = pltpu.get_barrier_semaphore()
    greet = others_y + others_tp + ring
    for d in greet:
        pl.semaphore_signal(barrier, inc=1, device_id=d, device_id_type=MESH)

    my_row = pl.multiple_of(sp * depth, depth)
    wo_rows = lambda t: wo.at[pl.ds(pl.multiple_of(t * LANES, LANES), LANES), :]
    loads = [
        (wg_hbm, wall.at[pl.ds(my_row, depth), 0:ff]),
        (wu_hbm, wall.at[pl.ds(my_row, depth), ff:ca]),
        (wd_hbm, wall.at[pl.ds(my_row, depth), ca:]),
        (dw_hbm, dw_ref), (k_hbm, k_ref), (lw_hbm, lw_ref), (r_hbm, r_ref), (v_hbm, v_ref),
        (gate_hbm, gate_ref), (tw_hbm, tw_ref), (hg_hbm, hg_ref), (gain_hbm, gain_ref),
        (wo_hbm, wo_rows(tp)), (res_hbm, resid),
    ]
    loads = [pltpu.make_async_copy(a, b, loc.at[i]) for i, (a, b) in enumerate(loads)]
    for cp in loads[:8]:
        cp.start()

    def rows(zz, yy, lo=0, n=None):
        return pl.ds(pl.multiple_of(zz * plane + yy * depth + lo, half), depth if n is None else n)

    y2 = (y + 2) % NY
    lane = (y, y2)
    cols = (slice(0, ff), slice(ff, ca), slice(ca, 3 * ff))

    def block(zz, yy, part, lo=0, n=None):
        return wall.at[rows(zz, yy, lo, n), cols[part]]

    def ahead(s, dirn):
        return (z + NZ - s) % NZ if dirn == 0 else (z + s) % NZ

    def plane_of(i):
        return z if i == 0 else ahead((i + 1) // 2, (i - 1) % 2)

    def zstream(st, part, s):
        out = []
        for d in (0, 1):
            at = (0, depth) if s < HOPS - 1 else (half * d, half)
            ref = block(ahead(s, d), lane[st], part, *at)
            k = 3 * st + part
            out.append(rcopy(ref, ref, send.at[k], r_z.at[k, s], ring[d]))
        return out

    side = [dev(yy=(y + 1) % NY), dev(yy=(y + NY - 1) % NY)]

    def yside(part, i):
        ref = block(plane_of(i), y, part)
        group = [g for g, (lo, hi) in enumerate(GROUPS) if lo <= i < hi][0]
        sems = [r_ya.at[part] if part < DOWN else r_yb.at[group]] * 2
        if i == 0:
            sems = [r_y0.at[part]] * 2
        return [rcopy(ref, ref, send.at[6 + part], sems[d], side[d]) for d in (0, 1)]

    def across(part):
        out = []
        for d in (0, 1):
            ref = block(z, (y + NY - 1) % NY if d == 0 else (y + 1) % NY, part, half * d, half)
            out.append(rcopy(ref, ref, send.at[9 + part], r_q.at[part], side[d]))
        return out

    def start(copies):
        for cp in copies:
            cp.start()

    def wait_recv(copies):
        for cp in copies:
            cp.wait_recv()

    def exchange(buf, slot, sem, s, targets):
        return [
            rcopy(buf.at[slot], buf.at[slot], send.at[s], sem.at[0], t)
            for d, t in enumerate(targets)
        ]

    def wo_same(d):
        t = ((x + d) % NX) * NC + c
        return rcopy(wo_hbm, wo_rows(tp), send.at[12], r_wo.at[d - 1], dev(tt=t))

    partner = dev(tt=x * NC + 1 - c)

    def wo_relay(d):
        ref = wo_rows(((x + NX - d) % NX) * NC + c)
        return rcopy(ref, ref, send.at[13], r_wo.at[NX - 1], partner)

    def tell(i):
        for zz in (z + 2**i, z + NZ - 2**i):
            pl.semaphore_signal(ok.at[i], inc=1, device_id=dev(zz=zz % NZ), device_id_type=MESH)

    def heard(i):
        pl.semaphore_wait(ok.at[i], 2)

    def enter():
        for cp in loads[:3]:
            cp.wait()
        with jax.named_scope("enter"):
            pl.semaphore_wait(barrier, len(greet))
        tell(0)
        for part in range(3):
            start(zstream(0, part, 0))
            start(yside(part, 0))
        for cp in loads[8:]:
            cp.start()
        for d in range(1, NX):
            wo_same(d).start()

    def new_at(s):
        return [2 * s + 1, 2 * s + 2] if s < HOPS - 1 else [2 * s + 1]

    def relay(part):
        wait_blocks(part, 2, r_y0.at[part])
        start(across(part))

    def wait_blocks(part, n, sem):
        wait_bytes(wall.at[0 : n * depth, cols[part]], sem)

    def q_open(part):
        wait_blocks(part, 1, r_q.at[part])
        start(zstream(1, part, 0))

    def p_step(part, s):
        wait_blocks(part, 2 if s < HOPS - 1 else 1, r_z.at[part, s])
        if s < HOPS - 1:
            start(zstream(0, part, s + 1))
        for i in new_at(s):
            start(yside(part, i))

    def q_step(part, s):
        wait_blocks(part, 2 if s < HOPS - 1 else 1, r_z.at[3 + part, s])
        if s < HOPS - 1:
            start(zstream(1, part, s + 1))

    work = []

    def job(f, *a):
        work.append(functools.partial(f, *a))

    for part in range(3):
        job(relay, part)
    for part in range(3):
        job(p_step, part, 0)
    job(q_open, 0)
    for s in range(1, HOPS + LAG + 1):
        for step, t in ((p_step, s), (q_step, s - 1)):
            for part in range(3):
                u = t - LAG if part == DOWN else t
                if (0 if step is q_step else 1) <= u < HOPS:
                    job(step, part, u)
                if s == 1 and step is p_step and part == 0:
                    job(q_open, 1)
                    job(q_open, DOWN)
    a_last = [f for f in work if f.args[0] < DOWN and f.func is q_step][-1]
    b_last = [f for f in work if f.args[0] == DOWN and f.func is q_step]

    def serve(n=None, until=None):
        while work and (n is None or n > 0) and (until is None or until in work):
            f = work.pop(0)
            n = None if n is None else n - 1
            with jax.named_scope("_".join([f.func.__name__] + [str(a) for a in f.args])):
                f()

    enter()
    for cp in loads[3:8]:
        cp.wait()
    with jax.named_scope("local"):
        prod, state, decay, outputs = local_part(
            r_ref, k_ref, v_ref, dw_ref, lw_ref, lambda: serve(MID)
        )
        put_packet(ybuf, y, prod, state, decay)
    l1 = exchange(ybuf, y, r_l1, 14, others_y)
    start(l1)
    heard(0)
    tell(1)
    serve(SERVE[0])
    with jax.named_scope("local_out"):
        q, y_own = outputs()
        q_s[...] = q
        y_s[...] = y_own
    for cp in loads[8:]:
        cp.wait()
    wo_relay(0).start()
    serve(SERVE[1])
    with jax.named_scope("wait_l1"):
        wait_bytes(ybuf.at[0:3], r_l1.at[0])

    def total(buf):
        m = [get_packet(buf, j) for j in range(4)]
        ab, cd = compose(m[0], m[1]), compose(m[2], m[3])
        return (*compose(ab, cd), (m[0][2] * m[1][2]) * (m[2][2] * m[3][2]))

    ident = (fold_diag(jnp.ones((1, LANES), f32)), jnp.zeros((HEAD, LANES), f32))

    def before(at, buf, count):
        ent[at] = jnp.concatenate(ident, axis=0)

        def step(j, _):
            p, u, _ = get_packet(buf, j)
            both = dot3(ent[at], unfold(p))
            ent[at, 0:HEAD, :] = both[:HEAD]
            ent[at, HEAD:, :] = both[HEAD:] + u
            return 0

        lax.fori_loop(0, count, step, 0)

    put_packet(zbuf, zl, *total(ybuf))
    heard(1)
    tell(2)
    l2 = exchange(zbuf, zl, r_l2, 15, others_zl)
    start(l2)
    with jax.named_scope("before_y"):
        before(0, ybuf, y)
    serve(SERVE[2])
    with jax.named_scope("wait_l2"):
        wait_bytes(zbuf.at[0:3], r_l2.at[0])
    put_packet(gbuf, zg, *total(zbuf))
    quarter = pl.ds(pl.multiple_of(y * (LANES // NY), LANES // NY), LANES // NY)

    def far(d):
        cuts = gbuf.at[zg, quarter, :], gbuf.at[zg, LANES:, :]
        return [
            rcopy(ref, ref, x_l3.at[d - 1], r_l3.at[d - 1], others_zg[d - 1]) for ref in cuts
        ]

    def share(d):
        ref = gbuf.at[zg - d, quarter, :]
        return [
            rcopy(ref, ref, x_l4.at[d - 1], r_l4.at[d - 1], others_y[e])
            for e in range(NY - 1)
        ]

    heard(2)
    for d in range(1, NG):
        @pl.when(zg + d < NG)
        def _(d=d):
            start(far(d))

    with jax.named_scope("before_z"):
        before(1, zbuf, zl)
    serve(SERVE[3])
    with jax.named_scope("wait_far"):
        for d in range(1, NG):
            @pl.when(zg >= d)
            def _(d=d):
                wait_bytes(gbuf.at[0, 0 : LANES // NY + 16, :], r_l3.at[d - 1])
                start(share(d))
    serve(SERVE[4])
    with jax.named_scope("relay"):
        for d in range(1, NX):
            wo_same(d).wait_recv()
            wo_relay(d).start()
    with jax.named_scope("wait_l3"):
        for d in range(1, NG):
            @pl.when(zg >= d)
            def _(d=d):
                wait_bytes(gbuf.at[0, 0 : LANES // NY * (NY - 1), :], r_l4.at[d - 1])

    def turn(j, s):
        p, u, _ = get_packet(gbuf, j)
        return dot3(s, unfold(p)) + u

    s_in = lax.fori_loop(0, zg, turn, jnp.zeros((HEAD, LANES), f32))
    for at in (1, 0):
        s_in = dot3(s_in, unfold(ent[at, 0:HEAD, :])) + ent[at, HEAD:, :]

    first = lax.broadcasted_iota(jnp.int32, (steps, LANES), 1) < HEAD
    yy = dot3(q_s[...], unfold(s_in), NT) + y_s[...]
    yy = yy - per_head_sum(yy, first) * (1.0 / HEAD)
    spread = per_head_sum(yy * yy, first) * (1.0 / HEAD)
    r, k, v = (a[...].astype(f32) for a in (r_ref, k_ref, v_ref))
    weight = jnp.concatenate([tw_ref[0:1, :], tw_ref[1:2, :]], axis=1)
    own = per_head_sum(r * k * weight, first) * v
    yy = yy * lax.rsqrt(spread + GROUP_EPS) * hg_ref[...] + own
    mixed[tp] = (yy * jax.nn.sigmoid(gate_ref[...].astype(f32))).astype(bf16)
    mx = [
        rcopy(mixed.at[tp], mixed.at[tp], send.at[17], r_mx.at[0], t)
        for d, t in enumerate(others_tp)
    ]
    start(mx)
    serve(SERVE[5])
    with jax.named_scope("wait_mixed"):
        wait_bytes(wo.at[0 : NX * LANES, :], r_wo.at[NX - 1])
        wait_bytes(mixed.at[0 : NTP - 1], r_mx.at[0])

    wide = 512

    def project(n, ss):
        cut = pl.ds(pl.multiple_of(n * wide, wide), wide)
        lhs = jnp.concatenate([mixed[j] for j in range(NTP)], axis=1)
        mix = jnp.dot(lhs, wo[:, cut], preferred_element_type=f32)
        mix = mix.astype(bf16).astype(f32)
        a = (resid[:, cut].astype(f32) + mix).astype(bf16).astype(f32)
        after[:, cut] = a
        return ss + jnp.sum(a * a, axis=-1, keepdims=True)

    with jax.named_scope("project"):
        ss = lax.fori_loop(0, model // wide, project, jnp.zeros((steps, 1), f32))
    factor = lax.rsqrt(ss * (1.0 / model) + NORM_EPS)

    def scale(n, _):
        cut = pl.ds(pl.multiple_of(n * wide, wide), wide)
        normed[:, cut] = (after[:, cut] * factor * gain_ref[:, cut]).astype(bf16)
        return 0

    with jax.named_scope("scale"):
        lax.fori_loop(0, model // wide, scale, 0)
    serve(until=a_last)
    serve(TAIL[0])
    with jax.named_scope("wait_gate_up"):
        for part in range(DOWN):
            wait_bytes(wall.at[0 : 2 * (NZ - 1) * depth, cols[part]], r_ya.at[part])

    with jax.named_scope("gate_up"):
        lo = 0
        while lo < ff:
            n = min(256, ff - lo)
            g = jnp.dot(normed[...], wall[:, lo : lo + n], preferred_element_type=f32)
            u = jnp.dot(normed[...], wall[:, ff + lo : ff + lo + n], preferred_element_type=f32)
            hid[:, lo : lo + n] = (g / (1.0 + jnp.exp(-g)) * u).astype(bf16)
            lo += n

    serve(TAIL[1])

    def down_planes(lo, hi):
        for i in range(lo, hi, 2):
            both = [wall[rows(plane_of(j), 0, 0, plane), ca:] for j in range(i, min(i + 2, hi))]
            w = both[0] if len(both) == 1 else jnp.concatenate(both, axis=0)
            d = lax.dot_general(hid[...], w, NT, preferred_element_type=f32)
            for t in range(NTP):
                own = d[t * own_rows : (t + 1) * own_rows].astype(bf16)
                for j in range(len(both)):
                    parts[t % NC, i + j, t // NC] = own[:, j * plane : (j + 1) * plane]

    def pair(g):
        lo, hi = GROUPS[g]
        return rcopy(
            parts.at[1 - c, lo:hi], pair_in.at[lo:hi], send.at[18], r_pair.at[g], partner
        )

    def across_x(g):
        lo, hi = GROUPS[g]
        out = []
        for d in range(1, NX):
            xx = (x + d) % NX
            out.append(
                rcopy(
                    pair_sum.at[xx, lo:hi], last_in.at[d - 1, lo:hi], send.at[19],
                    r_last.at[g], dev(tt=xx * NC + c),
                )
            )
        return out

    def sum_pair(g):
        with jax.named_scope(f"pair_{g}"):
            pair(g).wait_recv()
        lo, hi = GROUPS[g]
        for xx in range(NX):
            both = parts[c, lo:hi, xx].astype(f32) + pair_in[lo:hi, xx].astype(f32)
            pair_sum[xx, lo:hi] = both.astype(bf16)
        start(across_x(g))

    for g, (lo, hi) in enumerate(GROUPS):
        if b_last[hi // 2 - 1] in work:
            serve(until=b_last[hi // 2 - 1])
        with jax.named_scope(f"wait_down_{g}"):
            wait_blocks(DOWN, 2 * (hi - max(lo, 1)), r_yb.at[g])
        with jax.named_scope(f"down_{g}"):
            down_planes(lo, hi)
        pair(g).start()
        if g > 0:
            sum_pair(g - 1)
    sum_pair(len(GROUPS) - 1)

    my_rows = pl.ds(pl.multiple_of(tp * own_rows, 8), own_rows)
    for g, (lo, hi) in enumerate(GROUPS):
        with jax.named_scope(f"last_{g}"):
            wait_bytes(last_in.at[:, lo:hi], r_last.at[g])
        for i in range(lo, hi):
            to = pl.ds(pl.multiple_of(plane_of(i) * plane, plane), plane)
            t = parts[c, i, x].astype(f32) + pair_in[i, x].astype(f32)
            for d in range(1, NX):
                t = t + last_in[d - 1, i].astype(f32)
            out_ref[:, to] = after[my_rows, to] + t

    drain = jax.named_scope("drain")
    drain.__enter__()
    for k in range(6):
        wait_bytes(wall.at[0 : (2 * HOPS - 1) * depth, cols[k % 3]], send.at[k])
    for part in range(3):
        wait_bytes(wall.at[0 : 2 * NZ * depth, cols[part]], send.at[6 + part])
        wait_bytes(wall.at[0:depth, cols[part]], send.at[9 + part])
    wait_bytes(wo.at[0 : (NX - 1) * LANES, :], send.at[12])
    wait_bytes(wo.at[0 : NX * LANES, :], send.at[13])
    wait_bytes(ybuf.at[0:3], send.at[14])
    wait_bytes(zbuf.at[0:3], send.at[15])
    for d in range(1, NG):
        @pl.when(zg + d < NG)
        def _(d=d):
            wait_bytes(gbuf.at[0, 0 : LANES // NY + 16, :], x_l3.at[d - 1])
    for d in range(1, NG):
        @pl.when(zg >= d)
        def _(d=d):
            wait_bytes(gbuf.at[0, 0 : LANES // NY * (NY - 1), :], x_l4.at[d - 1])
    wait_bytes(mixed.at[0 : NTP - 1], send.at[17])
    wait_bytes(pair_in, send.at[18])
    wait_bytes(pair_sum.at[0 : NX - 1], send.at[19])
    drain.__exit__(None, None, None)


DOWN = 2
LAG = 1
GROUPS = ((0, 5), (5, 9), (9, 13), (13, 15), (15, 16))
VMEM_MB = 58
MID = 1
SERVE = (5, 4, 3, 9, 6, 9)
TAIL = (0, 1)


def layer(r, k, v, dw, lw, gate, tw, hg, wg, wu, wd, gain, wo, residual):
    f32, bf16 = jnp.float32, jnp.bfloat16
    steps = r.shape[0]
    depth, ff = wg.shape
    model = residual.shape[1]
    own_rows = steps // NTP
    vmem = pl.BlockSpec(memory_space=pltpu.VMEM)
    dma = pltpu.SemaphoreType.DMA
    return pl.pallas_call(
        layer_kernel,
        in_specs=[pl.BlockSpec(memory_space=pltpu.HBM)] * 14,
        out_specs=vmem,
        out_shape=pltpu.VMEM((own_rows, model), f32),
        scratch_shapes=[
            pltpu.VMEM((model, 3 * ff), bf16),
            pltpu.VMEM((NTP * LANES, model), bf16),
            pltpu.VMEM((NTP, steps, LANES), bf16),
            pltpu.VMEM((steps, model), bf16),
            pltpu.VMEM((steps, model), f32),
            pltpu.VMEM((steps, model), bf16),
            pltpu.VMEM((steps, ff), bf16),
            pltpu.VMEM((NC, NZ, NX, own_rows, LANES), bf16),
            pltpu.VMEM((NZ, NX, own_rows, LANES), bf16),
            pltpu.VMEM((NX, NZ, own_rows, LANES), bf16),
            pltpu.VMEM((NX - 1, NZ, own_rows, LANES), bf16),
            *[pltpu.VMEM(a.shape, a.dtype) for a in (r, k, v, dw, lw, gate, tw, hg, gain)],
            pltpu.VMEM((NY, PACKET, LANES), bf16),
            pltpu.VMEM((NG, PACKET, LANES), bf16),
            pltpu.VMEM((NG, PACKET, LANES), bf16),
            pltpu.VMEM((steps, LANES), f32),
            pltpu.VMEM((steps, LANES), f32),
            pltpu.VMEM((2, LANES, LANES), f32),
            dma((20,)),
            dma((NX,)),
            dma((6, HOPS)),
            dma((3,)),
            dma((3,)),
            dma((DOWN,)),
            dma((len(GROUPS),)),
            dma((1,)),
            dma((1,)),
            dma((NG - 1,)),
            dma((NG - 1,)),
            dma((NG - 1,)),
            dma((NG - 1,)),
            dma((1,)),
            dma((len(GROUPS),)),
            dma((len(GROUPS),)),
            dma((14,)),
            pltpu.SemaphoreType.REGULAR((3,)),
        ],
        compiler_params=pltpu.CompilerParams(
            collective_id=0, has_side_effects=True, vmem_limit_bytes=VMEM_MB * 1024 * 1024
        ),
        cost_estimate=pl.CostEstimate(
            flops=3_000_000_000, bytes_accessed=8_000_000, transcendentals=1_000_000
        ),
        name="layer",
    )(r, k, v, dw, lw, gate, tw, hg, gain, wg, wu, wd, wo, residual)


def per_device(r, k, v, dw, lw, gate, tw, hg, w_out, residual, gain, w_gate, w_up, w_down):
    return layer(
        r, k, v, dw, lw, gate, tw, hg.reshape(1, -1), w_gate, w_up, w_down.T,
        gain.reshape(1, -1), w_out, residual,
    ).astype(jnp.bfloat16)


def solution(mesh):
    split_both = P("sp", "tp")
    placed = (split_both,) * 6 + (
        P("tp", None),
        P("tp"),
        P("tp", None),
        P("sp", None),
        P(),
        split_both,
        split_both,
        P("tp", "sp"),
    )
    return jax.shard_map(
        per_device, mesh=mesh, in_specs=placed, out_specs=P(("sp", "tp"), None), check_vma=False
    )
```

```python
import functools

import jax
import jax.numpy as jnp
from jax import lax
from jax.experimental import pallas as pl
from jax.experimental.pallas import tpu as pltpu
from jax.sharding import PartitionSpec as P

HEAD = 64
LANES = 2 * HEAD
GROUP_EPS = 0.00064
NORM_EPS = 1e-06
NN = (((1,), (0,)), ((), ()))
NT = (((1,), (1,)), ((), ()))
TN = (((0,), (0,)), ((), ()))
NX, NY, NZ, NC = 4, 4, 16, 2
NTP = NX * NC
NG = 4
HOPS = NZ // 2
MESH = pl.DeviceIdType.MESH
PACKET = LANES + 16


def split(x):
    high = x.astype(jnp.bfloat16)
    return high, (x - high.astype(jnp.float32)).astype(jnp.bfloat16)


def dot1(a, b, dims=NN):
    return lax.dot_general(
        a.astype(jnp.bfloat16), b.astype(jnp.bfloat16), dims, preferred_element_type=jnp.float32
    )


def dot3(a, b, dims=NN):
    ah, al = a if isinstance(a, tuple) else split(a)
    bh, bl = b if isinstance(b, tuple) else split(b)
    d = functools.partial(
        lax.dot_general, dimension_numbers=dims, preferred_element_type=jnp.float32
    )
    return d(ah, bh) + (d(ah, bl) + d(al, bh))


def per_head_sum(x, first):
    s0 = jnp.sum(jnp.where(first, x, 0.0), axis=-1, keepdims=True)
    s1 = jnp.sum(jnp.where(first, 0.0, x), axis=-1, keepdims=True)
    return jnp.where(first, s0, s1)


def block_diag_mask():
    row = lax.broadcasted_iota(jnp.int32, (LANES, LANES), 0)
    col = lax.broadcasted_iota(jnp.int32, (LANES, LANES), 1)
    return row // HEAD == col // HEAD


def fold(full):
    kept = jnp.where(block_diag_mask(), full, 0.0)
    return kept[:HEAD] + kept[HEAD:]


def unfold(packed):
    return jnp.where(block_diag_mask(), jnp.concatenate([packed, packed], axis=0), 0.0)


def fold_diag(d):
    row = lax.broadcasted_iota(jnp.int32, (HEAD, LANES), 0)
    col = lax.broadcasted_iota(jnp.int32, (HEAD, LANES), 1)
    return jnp.where(col % HEAD == row, d, 0.0)


def compose(a, b):
    both = dot3(jnp.concatenate([a[0], a[1]], axis=0), unfold(b[0]))
    return both[:HEAD], both[HEAD:] + b[1]


def put_packet(ref, slot, prod, state, decay):
    high, low = split(decay)
    row = lax.broadcasted_iota(jnp.int32, (16, LANES), 0)
    high, low = high.astype(jnp.float32), low.astype(jnp.float32)
    tail = jnp.where(row == 0, high, jnp.where(row == 1, low, 0.0))
    ref[slot, :HEAD, :] = (prod - fold_diag(decay)).astype(jnp.bfloat16)
    ref[slot, HEAD:LANES, :] = state.astype(jnp.bfloat16)
    ref[slot, LANES:, :] = tail.astype(jnp.bfloat16)


def get_packet(ref, slot):
    f32 = jnp.float32
    tail = ref[slot, LANES:, :].astype(f32)
    decay = tail[0:1] + tail[1:2]
    prod = ref[slot, :HEAD, :].astype(f32) + fold_diag(decay)
    return prod, ref[slot, HEAD:LANES, :].astype(f32), decay


def local_part(r_ref, k_ref, v_ref, dw_ref, lw_ref, between):
    steps = r_ref.shape[0]
    f32 = jnp.float32
    first = lax.broadcasted_iota(jnp.int32, (steps, LANES), 1) < HEAD
    row = lax.broadcasted_iota(jnp.int32, (steps, steps), 0)
    col = lax.broadcasted_iota(jnp.int32, (steps, steps), 1)
    r, k, v = (x[...].astype(f32) for x in (r_ref, k_ref, v_ref))
    log_decay = jax.nn.sigmoid(dw_ref[...]) * (-0.6065306597126334)
    ones = (row >= col).astype(jnp.bfloat16)
    h0 = log_decay.astype(jnp.bfloat16)
    rest = log_decay - h0.astype(f32)
    h1 = rest.astype(jnp.bfloat16)
    h2 = (rest - h1.astype(f32)).astype(jnp.bfloat16)
    total = dot1(ones, h0) + (dot1(ones, h1) + dot1(ones, h2))
    last = total[steps - 1 :, :]
    unit = k / jnp.maximum(jnp.sqrt(per_head_sum(k * k, first)), 1.0)
    insert = unit * jax.nn.sigmoid(lw_ref[...])
    undo = jnp.exp(-total)
    remaining = jnp.exp(last - total)
    a_bar = -unit * jnp.exp(total - log_decay)
    r_bar = r * jnp.exp(total)
    b_hat = insert * undo
    k_hat = k * undo
    right = split(jnp.concatenate([b_hat, k_hat], axis=0))
    left = jnp.concatenate([a_bar, r_bar], axis=0)
    first2 = jnp.concatenate([first, first], axis=0)
    grams = [
        dot3(jnp.where(first2 if h == 0 else ~first2, left, 0.0), right, NT) for h in (0, 1)
    ]
    strict, incl = row > col, row >= col
    ab = [jnp.where(strict, g[:steps, :steps], 0.0) for g in grams]
    ak = [jnp.where(strict, g[:steps, steps:], 0.0) for g in grams]
    rb = [jnp.where(incl, g[steps:, :steps], 0.0) for g in grams]
    rk = [jnp.where(incl, g[steps:, steps:], 0.0) for g in grams]
    vb = v_ref[...]

    def times_v(m):
        mh, ml = split(m)
        return dot1(mh, vb) + dot1(ml, vb)

    seeds = [jnp.concatenate([a_bar, times_v(m)], axis=1) for m in ak]
    ab16 = [m.astype(jnp.bfloat16) for m in ab]
    eye = (row == col).astype(f32)
    size = 1
    inv = None
    while size < steps:
        joined = (
            (row // (2 * size) == col // (2 * size))
            & ((row // size) % 2 == 1)
            & ((col // size) % 2 == 0)
        )
        parts = [jnp.where(joined, m, jnp.zeros_like(m)) for m in ab16]
        if inv is None:
            inv = [eye + p.astype(f32) for p in parts]
        else:
            t16 = [t.astype(jnp.bfloat16) for t in inv]
            mid = [dot1(t, p) for t, p in zip(t16, parts)]
            inv = [t + dot1(m, tt) for t, m, tt in zip(inv, mid, t16)]
        size *= 2
    between()
    inv16 = [t.astype(jnp.bfloat16) for t in inv]
    absp = [split(m) for m in ab]
    sol = [dot1(t, s) for t, s in zip(inv16, seeds)]
    for _ in range(2):
        res = [s - x + dot3(m, x) for s, x, m in zip(seeds, sol, absp)]
        sol = [x + dot1(t, e) for x, t, e in zip(sol, inv16, res)]
    w = jnp.where(first, sol[0][:, :LANES], sol[1][:, :LANES])
    u = jnp.where(first, sol[0][:, LANES:], sol[1][:, LANES:])
    b_end = split(insert * remaining)
    decay = jnp.exp(last)
    prod = fold(dot3(w, b_end, TN)) + fold_diag(decay)
    kh, kl = split(k * remaining)
    state = fold(dot3(u, b_end, TN) + dot1(vb, kh, TN) + dot1(vb, kl, TN))

    def outputs():
        outs = [dot3(m, x) for m, x in zip(rb, sol)]
        own = [times_v(m) for m in rk]
        q = r_bar + jnp.where(first, outs[0][:, :LANES], outs[1][:, :LANES])
        y = jnp.where(first, outs[0][:, LANES:] + own[0], outs[1][:, LANES:] + own[1])
        return q, y

    return prod, state, decay, outputs


def layer_kernel(
    r_hbm, k_hbm, v_hbm, dw_hbm, lw_hbm, gate_hbm, tw_hbm, hg_hbm, gain_hbm, wg_hbm, wu_hbm, wd_hbm,
    wo_hbm, res_hbm,
    out_ref,
    wall, wo, mixed, resid, after, normed, hid, parts, pair_in, pair_sum, last_in,
    r_ref, k_ref, v_ref, dw_ref, lw_ref, gate_ref, tw_ref, hg_ref, gain_ref,
    ybuf, zbuf, gbuf, q_s, y_s, ent, sums, acc,
    send, r_wo, r_z, r_q, r_y0, r_ya, r_yb, r_l1, r_l2, r_l3, x_l3, r_l4, x_l4, r_mx, r_pair, r_last, loc, ok,
):
    f32, bf16 = jnp.float32, jnp.bfloat16
    steps = r_ref.shape[0]
    depth, ff = wg_hbm.shape
    plane = NY * depth
    half = depth // 2
    ca = 2 * ff
    model = wo.shape[1]
    own_rows = out_ref.shape[0]
    sp, tp = lax.axis_index("sp"), lax.axis_index("tp")
    z, y = sp // NY, sp % NY
    x, c = tp // NC, tp % NC
    zg, zl = z // NG, z % NG

    def dev(zz=None, yy=None, tt=None):
        zz = z if zz is None else zz
        yy = y if yy is None else yy
        return (zz * NY + yy, tp if tt is None else tt)

    def rcopy(src, dst, s, r, device):
        return pltpu.make_async_remote_copy(
            src_ref=src, dst_ref=dst, send_sem=s, recv_sem=r, device_id=device, device_id_type=MESH
        )

    def wait_bytes(ref, sem):
        pltpu.make_async_copy(ref, ref, sem).wait()

    up, down = (z + 1) % NZ, (z + NZ - 1) % NZ
    others_y = [dev(yy=(y + d) % NY) for d in range(1, NY)]
    others_zl = [dev(zz=zg * NG + (zl + d) % NG) for d in range(1, NG)]
    others_zg = [dev(zz=((zg + d) % NG) * NG + zl) for d in range(1, NG)]
    others_tp = [dev(tt=(tp + d) % NTP) for d in range(1, NTP)]
    ring = [dev(zz=up), dev(zz=down)]

    barrier = pltpu.get_barrier_semaphore()
    greet = others_y + others_tp + ring
    for d in greet:
        pl.semaphore_signal(barrier, inc=1, device_id=d, device_id_type=MESH)

    my_row = pl.multiple_of(sp * depth, depth)
    wo_rows = lambda t: wo.at[pl.ds(pl.multiple_of(t * LANES, LANES), LANES), :]
    loads = [
        (wg_hbm, wall.at[pl.ds(my_row, depth), 0:ff]),
        (wu_hbm, wall.at[pl.ds(my_row, depth), ff:ca]),
        (wd_hbm, wall.at[pl.ds(my_row, depth), ca:]),
        (dw_hbm, dw_ref), (k_hbm, k_ref), (lw_hbm, lw_ref), (r_hbm, r_ref), (v_hbm, v_ref),
        (gate_hbm, gate_ref), (tw_hbm, tw_ref), (hg_hbm, hg_ref), (gain_hbm, gain_ref),
        (wo_hbm, wo_rows(tp)), (res_hbm, resid),
    ]
    loads = [pltpu.make_async_copy(a, b, loc.at[i]) for i, (a, b) in enumerate(loads)]
    for cp in loads[:8]:
        cp.start()

    def rows(zz, yy, lo=0, n=None):
        return pl.ds(pl.multiple_of(zz * plane + yy * depth + lo, half), depth if n is None else n)

    y2 = (y + 2) % NY
    lane = (y, y2)
    cols = (slice(0, ff), slice(ff, ca), slice(ca, 3 * ff))

    def block(zz, yy, part, lo=0, n=None):
        return wall.at[rows(zz, yy, lo, n), cols[part]]

    def ahead(s, dirn):
        return (z + NZ - s) % NZ if dirn == 0 else (z + s) % NZ

    def plane_of(i):
        return z if i == 0 else ahead((i + 1) // 2, (i - 1) % 2)

    def zstream(st, part, s):
        out = []
        for d in (0, 1):
            at = (0, depth) if s < HOPS - 1 else (half * d, half)
            ref = block(ahead(s, d), lane[st], part, *at)
            k = 3 * st + part
            out.append(rcopy(ref, ref, send.at[0], r_z.at[k, s], ring[d]))
        return out

    side = [dev(yy=(y + 1) % NY), dev(yy=(y + NY - 1) % NY)]

    def yside(part, i):
        ref = block(plane_of(i), y, part)
        group = [g for g, (lo, hi) in enumerate(GROUPS) if lo <= i < hi][0]
        sems = [r_ya.at[2 * part + (i >= EARLY)] if part < DOWN else r_yb.at[group]] * 2
        if i == 0:
            sems = [r_y0.at[part]] * 2
        return [rcopy(ref, ref, send.at[0], sems[d], side[d]) for d in (0, 1)]

    def across(part):
        out = []
        for d in (0, 1):
            ref = block(z, (y + NY - 1) % NY if d == 0 else (y + 1) % NY, part, half * d, half)
            out.append(rcopy(ref, ref, send.at[0], r_q.at[part], side[d]))
        return out

    def start(copies):
        for cp in copies:
            cp.start()

    def wait_recv(copies):
        for cp in copies:
            cp.wait_recv()

    def exchange(buf, slot, sem, s, targets):
        return [
            rcopy(buf.at[slot], buf.at[slot], send.at[s], sem.at[0], t)
            for d, t in enumerate(targets)
        ]

    def wo_same(d):
        t = ((x + d) % NX) * NC + c
        return rcopy(wo_hbm, wo_rows(tp), send.at[1], r_wo.at[d - 1], dev(tt=t))

    partner = dev(tt=x * NC + 1 - c)

    def wo_relay(d):
        ref = wo_rows(((x + NX - d) % NX) * NC + c)
        return rcopy(ref, ref, send.at[1], r_wo.at[NX - 1], partner)

    def tell(i):
        for zz in (z + 2**i, z + NZ - 2**i):
            pl.semaphore_signal(ok.at[i], inc=1, device_id=dev(zz=zz % NZ), device_id_type=MESH)

    def heard(i):
        pl.semaphore_wait(ok.at[i], 2)

    def enter():
        for cp in loads[:3]:
            cp.wait()
        with jax.named_scope("enter"):
            pl.semaphore_wait(barrier, len(greet))
        tell(0)
        for part in range(3):
            start(zstream(0, part, 0))
            start(yside(part, 0))
        for cp in loads[8:]:
            cp.start()
        for d in range(1, NX):
            wo_same(d).start()

    def new_at(s):
        return [2 * s + 1, 2 * s + 2] if s < HOPS - 1 else [2 * s + 1]

    def relay(part):
        wait_blocks(part, 2, r_y0.at[part])
        start(across(part))

    def wait_blocks(part, n, sem):
        wait_bytes(wall.at[0 : n * depth, cols[part]], sem)

    def q_open(part):
        wait_blocks(part, 1, r_q.at[part])
        start(zstream(1, part, 0))

    def p_step(part, s):
        wait_blocks(part, 2 if s < HOPS - 1 else 1, r_z.at[part, s])
        if s < HOPS - 1:
            start(zstream(0, part, s + 1))
        for i in new_at(s):
            start(yside(part, i))

    def q_step(part, s):
        wait_blocks(part, 2 if s < HOPS - 1 else 1, r_z.at[3 + part, s])
        if s < HOPS - 1:
            start(zstream(1, part, s + 1))

    work = []

    def job(f, *a):
        work.append(functools.partial(f, *a))

    for part in range(3):
        job(relay, part)
    for part in range(3):
        job(p_step, part, 0)
    job(q_open, 0)
    for s in range(1, HOPS + LAG + 1):
        for step, t in ((p_step, s), (q_step, s - 1)):
            for part in range(3):
                u = t - LAG if part == DOWN else t
                if (0 if step is q_step else 1) <= u < HOPS:
                    job(step, part, u)
                if s == 1 and step is p_step and part == 0:
                    job(q_open, 1)
                    job(q_open, DOWN)
    a_last = [f for f in work if f.args[0] < DOWN and f.func is q_step][-1]
    early = [f for f in work if f.func is q_step and f.args == (1, (EARLY - 2) // 2)][0]
    b_last = [f for f in work if f.args[0] == DOWN and f.func is q_step]

    def serve(n=None, until=None):
        while work and (n is None or n > 0) and (until is None or until in work):
            f = work.pop(0)
            n = None if n is None else n - 1
            with jax.named_scope("_".join([f.func.__name__] + [str(a) for a in f.args])):
                f()

    enter()
    for cp in loads[3:8]:
        cp.wait()
    with jax.named_scope("local"):
        prod, state, decay, outputs = local_part(
            r_ref, k_ref, v_ref, dw_ref, lw_ref, lambda: serve(MID)
        )
        put_packet(ybuf, y, prod, state, decay)
    l1 = exchange(ybuf, y, r_l1, 2, others_y)
    start(l1)
    heard(0)
    tell(1)
    serve(SERVE[0])
    with jax.named_scope("local_out"):
        q, y_own = outputs()
        q_s[...] = q
        y_s[...] = y_own
    for cp in loads[8:]:
        cp.wait()
    wo_relay(0).start()
    serve(SERVE[1])
    with jax.named_scope("wait_l1"):
        wait_bytes(ybuf.at[0:3], r_l1.at[0])

    def total(buf):
        m = [get_packet(buf, j) for j in range(4)]
        ab, cd = compose(m[0], m[1]), compose(m[2], m[3])
        return (*compose(ab, cd), (m[0][2] * m[1][2]) * (m[2][2] * m[3][2]))

    ident = (fold_diag(jnp.ones((1, LANES), f32)), jnp.zeros((HEAD, LANES), f32))

    def before(at, buf, count):
        ent[at] = jnp.concatenate(ident, axis=0)

        def step(j, _):
            p, u, _ = get_packet(buf, j)
            both = dot3(ent[at], unfold(p))
            ent[at, 0:HEAD, :] = both[:HEAD]
            ent[at, HEAD:, :] = both[HEAD:] + u
            return 0

        lax.fori_loop(0, count, step, 0)

    put_packet(zbuf, zl, *total(ybuf))
    heard(1)
    tell(2)
    l2 = exchange(zbuf, zl, r_l2, 3, others_zl)
    start(l2)
    with jax.named_scope("before_y"):
        before(0, ybuf, y)
    serve(SERVE[2])
    with jax.named_scope("wait_l2"):
        wait_bytes(zbuf.at[0:3], r_l2.at[0])
    put_packet(gbuf, zg, *total(zbuf))
    quarter = pl.ds(pl.multiple_of(y * (LANES // NY), LANES // NY), LANES // NY)

    def far(d):
        cuts = gbuf.at[zg, quarter, :], gbuf.at[zg, LANES:, :]
        return [
            rcopy(ref, ref, x_l3.at[d - 1], r_l3.at[d - 1], others_zg[d - 1]) for ref in cuts
        ]

    def share(d):
        ref = gbuf.at[zg - d, quarter, :]
        return [
            rcopy(ref, ref, x_l4.at[d - 1], r_l4.at[d - 1], others_y[e])
            for e in range(NY - 1)
        ]

    heard(2)
    for d in range(1, NG):
        @pl.when(zg + d < NG)
        def _(d=d):
            start(far(d))

    with jax.named_scope("before_z"):
        before(1, zbuf, zl)
    serve(SERVE[3])
    with jax.named_scope("wait_far"):
        for d in range(1, NG):
            @pl.when(zg >= d)
            def _(d=d):
                wait_bytes(gbuf.at[0, 0 : LANES // NY + 16, :], r_l3.at[d - 1])
                start(share(d))
    serve(SERVE[4])
    with jax.named_scope("relay"):
        for d in range(1, NX):
            wo_same(d).wait_recv()
            wo_relay(d).start()
    with jax.named_scope("wait_l3"):
        for d in range(1, NG):
            @pl.when(zg >= d)
            def _(d=d):
                wait_bytes(gbuf.at[0, 0 : LANES // NY * (NY - 1), :], r_l4.at[d - 1])

    def turn(j, s):
        p, u, _ = get_packet(gbuf, j)
        return dot3(s, unfold(p)) + u

    s_in = lax.fori_loop(0, zg, turn, jnp.zeros((HEAD, LANES), f32))
    for at in (1, 0):
        s_in = dot3(s_in, unfold(ent[at, 0:HEAD, :])) + ent[at, HEAD:, :]

    first = lax.broadcasted_iota(jnp.int32, (steps, LANES), 1) < HEAD
    yy = dot3(q_s[...], unfold(s_in), NT) + y_s[...]
    yy = yy - per_head_sum(yy, first) * (1.0 / HEAD)
    spread = per_head_sum(yy * yy, first) * (1.0 / HEAD)
    r, k, v = (a[...].astype(f32) for a in (r_ref, k_ref, v_ref))
    weight = jnp.concatenate([tw_ref[0:1, :], tw_ref[1:2, :]], axis=1)
    own = per_head_sum(r * k * weight, first) * v
    yy = yy * lax.rsqrt(spread + GROUP_EPS) * hg_ref[...] + own
    mixed[tp] = (yy * jax.nn.sigmoid(gate_ref[...].astype(f32))).astype(bf16)
    mx = [
        rcopy(mixed.at[tp], mixed.at[tp], send.at[4], r_mx.at[0], t)
        for d, t in enumerate(others_tp)
    ]
    start(mx)
    serve(SERVE[5])
    with jax.named_scope("wait_mixed"):
        wait_bytes(wo.at[0 : NX * LANES, :], r_wo.at[NX - 1])
        wait_bytes(mixed.at[0 : NTP - 1], r_mx.at[0])

    wide = 512

    def project(n, ss):
        cut = slice(n * wide, (n + 1) * wide)
        lhs = jnp.concatenate([mixed[j] for j in range(NTP)], axis=1)
        mix = jnp.dot(lhs, wo[:, cut], preferred_element_type=f32)
        mix = mix.astype(bf16).astype(f32)
        a = (resid[:, cut].astype(f32) + mix).astype(bf16).astype(f32)
        after[:, cut] = a
        return ss + jnp.sum(a * a, axis=-1, keepdims=True)

    ss = jnp.zeros((steps, 1), f32)
    for n in range(model // wide):
        with jax.named_scope("project"):
            ss = project(n, ss)
            sums[...] = ss
        serve(1)
        ss = sums[...]
    factor = lax.rsqrt(ss * (1.0 / model) + NORM_EPS)

    def scale(n, _):
        cut = pl.ds(pl.multiple_of(n * wide, wide), wide)
        normed[:, cut] = (after[:, cut] * factor * gain_ref[:, cut]).astype(bf16)
        return 0

    with jax.named_scope("scale"):
        lax.fori_loop(0, model // wide, scale, 0)
    def planes(lo, hi, part, at, n):
        total = None
        for i in range(lo, hi, 2):
            pair = [plane_of(i), plane_of(i + 1)]
            a = [normed[:, pl.ds(pl.multiple_of(p * plane, plane), plane)] for p in pair]
            w = [wall[rows(p, 0, 0, plane), part * ff + at : part * ff + at + n] for p in pair]
            d = jnp.dot(
                jnp.concatenate(a, axis=1), jnp.concatenate(w, axis=0), preferred_element_type=f32
            )
            total = d if total is None else total + d
        return total

    chunks = [(at, min(256, ff - at)) for at in range(0, ff, 256)]
    serve(until=early)
    with jax.named_scope("wait_early"):
        for part in range(DOWN):
            wait_blocks(part, 2 * (EARLY - 1), r_ya.at[2 * part])
    for at, n in chunks:
        for part in range(DOWN):
            with jax.named_scope("early"):
                acc[:, part * ff + at : part * ff + at + n] = planes(0, EARLY, part, at, n)
            serve(1)
    serve(until=a_last)
    serve(TAIL[0])
    with jax.named_scope("wait_gate_up"):
        for part in range(DOWN):
            wait_blocks(part, 2 * (NZ - EARLY), r_ya.at[2 * part + 1])

    with jax.named_scope("gate_up"):
        for at, n in chunks:
            g, u = (
                acc[:, part * ff + at : part * ff + at + n] + planes(EARLY, NZ, part, at, n)
                for part in range(DOWN)
            )
            hid[:, at : at + n] = (g / (1.0 + jnp.exp(-g)) * u).astype(bf16)

    serve(TAIL[1])

    def down_planes(lo, hi):
        for i in range(lo, hi, 2):
            both = [wall[rows(plane_of(j), 0, 0, plane), ca:] for j in range(i, min(i + 2, hi))]
            w = both[0] if len(both) == 1 else jnp.concatenate(both, axis=0)
            d = lax.dot_general(hid[...], w, NT, preferred_element_type=f32)
            for t in range(NTP):
                own = d[t * own_rows : (t + 1) * own_rows].astype(bf16)
                for j in range(len(both)):
                    parts[t % NC, i + j, t // NC] = own[:, j * plane : (j + 1) * plane]

    def pair(g):
        lo, hi = GROUPS[g]
        return rcopy(
            parts.at[1 - c, lo:hi], pair_in.at[lo:hi], send.at[5], r_pair.at[g], partner
        )

    def across_x(g):
        lo, hi = GROUPS[g]
        out = []
        for d in range(1, NX):
            xx = (x + d) % NX
            out.append(
                rcopy(
                    pair_sum.at[xx, lo:hi], last_in.at[d - 1, lo:hi], send.at[6],
                    r_last.at[g], dev(tt=xx * NC + c),
                )
            )
        return out

    def sum_pair(g):
        with jax.named_scope(f"pair_{g}"):
            pair(g).wait_recv()
        lo, hi = GROUPS[g]
        for xx in range(NX):
            both = parts[c, lo:hi, xx].astype(f32) + pair_in[lo:hi, xx].astype(f32)
            pair_sum[xx, lo:hi] = both.astype(bf16)
        start(across_x(g))

    for g, (lo, hi) in enumerate(GROUPS):
        if b_last[hi // 2 - 1] in work:
            serve(until=b_last[hi // 2 - 1])
        with jax.named_scope(f"wait_down_{g}"):
            wait_blocks(DOWN, 2 * (hi - max(lo, 1)), r_yb.at[g])
        with jax.named_scope(f"down_{g}"):
            down_planes(lo, hi)
        pair(g).start()
        if g > 0:
            sum_pair(g - 1)
    sum_pair(len(GROUPS) - 1)

    my_rows = pl.ds(pl.multiple_of(tp * own_rows, 8), own_rows)
    for g, (lo, hi) in enumerate(GROUPS):
        with jax.named_scope(f"last_{g}"):
            wait_bytes(last_in.at[:, lo:hi], r_last.at[g])
        for i in range(lo, hi):
            to = pl.ds(pl.multiple_of(plane_of(i) * plane, plane), plane)
            t = parts[c, i, x].astype(f32) + pair_in[i, x].astype(f32)
            for d in range(1, NX):
                t = t + last_in[d - 1, i].astype(f32)
            out_ref[:, to] = after[my_rows, to] + t

    drain = jax.named_scope("drain")
    drain.__enter__()
    wait_bytes(wall.at[0 : (2 * (2 * HOPS - 1) + 2 * NZ + 1) * depth, :], send.at[0])
    wait_bytes(wo.at[0 : (2 * NX - 1) * LANES, :], send.at[1])
    wait_bytes(ybuf.at[0:3], send.at[2])
    wait_bytes(zbuf.at[0:3], send.at[3])
    for d in range(1, NG):
        @pl.when(zg + d < NG)
        def _(d=d):
            wait_bytes(gbuf.at[0, 0 : LANES // NY + 16, :], x_l3.at[d - 1])
    for d in range(1, NG):
        @pl.when(zg >= d)
        def _(d=d):
            wait_bytes(gbuf.at[0, 0 : LANES // NY * (NY - 1), :], x_l4.at[d - 1])
    wait_bytes(mixed.at[0 : NTP - 1], send.at[4])
    wait_bytes(pair_in, send.at[5])
    wait_bytes(pair_sum.at[0 : NX - 1], send.at[6])
    drain.__exit__(None, None, None)


DOWN = 2
EARLY = 12
LAG = 1
GROUPS = ((0, 5), (5, 9), (9, 13), (13, 15), (15, 16))
VMEM_MB = 58
MID = 1
SERVE = (5, 4, 5, 7, 8, 10)
TAIL = (0, 1)


def layer(r, k, v, dw, lw, gate, tw, hg, wg, wu, wd, gain, wo, residual):
    f32, bf16 = jnp.float32, jnp.bfloat16
    steps = r.shape[0]
    depth, ff = wg.shape
    model = residual.shape[1]
    own_rows = steps // NTP
    vmem = pl.BlockSpec(memory_space=pltpu.VMEM)
    dma = pltpu.SemaphoreType.DMA
    return pl.pallas_call(
        layer_kernel,
        in_specs=[pl.BlockSpec(memory_space=pltpu.HBM)] * 14,
        out_specs=vmem,
        out_shape=pltpu.VMEM((own_rows, model), f32),
        scratch_shapes=[
            pltpu.VMEM((model, 3 * ff), bf16),
            pltpu.VMEM((NTP * LANES, model), bf16),
            pltpu.VMEM((NTP, steps, LANES), bf16),
            pltpu.VMEM((steps, model), bf16),
            pltpu.VMEM((steps, model), f32),
            pltpu.VMEM((steps, model), bf16),
            pltpu.VMEM((steps, ff), bf16),
            pltpu.VMEM((NC, NZ, NX, own_rows, LANES), bf16),
            pltpu.VMEM((NZ, NX, own_rows, LANES), bf16),
            pltpu.VMEM((NX, NZ, own_rows, LANES), bf16),
            pltpu.VMEM((NX - 1, NZ, own_rows, LANES), bf16),
            *[pltpu.VMEM(a.shape, a.dtype) for a in (r, k, v, dw, lw, gate, tw, hg, gain)],
            pltpu.VMEM((NY, PACKET, LANES), bf16),
            pltpu.VMEM((NG, PACKET, LANES), bf16),
            pltpu.VMEM((NG, PACKET, LANES), bf16),
            pltpu.VMEM((steps, LANES), f32),
            pltpu.VMEM((steps, LANES), f32),
            pltpu.VMEM((2, LANES, LANES), f32),
            pltpu.VMEM((steps, 1), f32),
            pltpu.VMEM((steps, 2 * ff), f32),
            dma((7,)),
            dma((NX,)),
            dma((6, HOPS)),
            dma((3,)),
            dma((3,)),
            dma((2 * DOWN,)),
            dma((len(GROUPS),)),
            dma((1,)),
            dma((1,)),
            dma((NG - 1,)),
            dma((NG - 1,)),
            dma((NG - 1,)),
            dma((NG - 1,)),
            dma((1,)),
            dma((len(GROUPS),)),
            dma((len(GROUPS),)),
            dma((14,)),
            pltpu.SemaphoreType.REGULAR((3,)),
        ],
        compiler_params=pltpu.CompilerParams(
            collective_id=0, has_side_effects=True, vmem_limit_bytes=VMEM_MB * 1024 * 1024
        ),
        cost_estimate=pl.CostEstimate(
            flops=3_000_000_000, bytes_accessed=8_000_000, transcendentals=1_000_000
        ),
        name="layer",
    )(r, k, v, dw, lw, gate, tw, hg, gain, wg, wu, wd, wo, residual)


def per_device(r, k, v, dw, lw, gate, tw, hg, w_out, residual, gain, w_gate, w_up, w_down):
    return layer(
        r, k, v, dw, lw, gate, tw, hg.reshape(1, -1), w_gate, w_up, w_down.T,
        gain.reshape(1, -1), w_out, residual,
    ).astype(jnp.bfloat16)


def solution(mesh):
    split_both = P("sp", "tp")
    placed = (split_both,) * 6 + (
        P("tp", None),
        P("tp"),
        P("tp", None),
        P("sp", None),
        P(),
        split_both,
        split_both,
        P("tp", "sp"),
    )
    return jax.shard_map(
        per_device, mesh=mesh, in_specs=placed, out_specs=P(("sp", "tp"), None), check_vma=False
    )
```

```python
import functools

import jax
import jax.numpy as jnp
from jax import lax
from jax.experimental import pallas as pl
from jax.experimental.pallas import tpu as pltpu
from jax.sharding import PartitionSpec as P

HEAD = 64
LANES = 2 * HEAD
GROUP_EPS = 0.00064
NORM_EPS = 1e-06
NN = (((1,), (0,)), ((), ()))
NT = (((1,), (1,)), ((), ()))
TN = (((0,), (0,)), ((), ()))
NX, NY, NZ, NC = 4, 4, 16, 2
NTP = NX * NC
NG = 4
HOPS = NZ // 2
MESH = pl.DeviceIdType.MESH
PACKET = LANES + 16


def split(x):
    high = x.astype(jnp.bfloat16)
    return high, (x - high.astype(jnp.float32)).astype(jnp.bfloat16)


def dot1(a, b, dims=NN):
    return lax.dot_general(
        a.astype(jnp.bfloat16), b.astype(jnp.bfloat16), dims, preferred_element_type=jnp.float32
    )


def dot3(a, b, dims=NN):
    ah, al = a if isinstance(a, tuple) else split(a)
    bh, bl = b if isinstance(b, tuple) else split(b)
    d = functools.partial(
        lax.dot_general, dimension_numbers=dims, preferred_element_type=jnp.float32
    )
    return d(ah, bh) + (d(ah, bl) + d(al, bh))


def per_head_sum(x, first):
    s0 = jnp.sum(jnp.where(first, x, 0.0), axis=-1, keepdims=True)
    s1 = jnp.sum(jnp.where(first, 0.0, x), axis=-1, keepdims=True)
    return jnp.where(first, s0, s1)


def block_diag_mask():
    row = lax.broadcasted_iota(jnp.int32, (LANES, LANES), 0)
    col = lax.broadcasted_iota(jnp.int32, (LANES, LANES), 1)
    return row // HEAD == col // HEAD


def fold(full):
    kept = jnp.where(block_diag_mask(), full, 0.0)
    return kept[:HEAD] + kept[HEAD:]


def unfold(packed):
    return jnp.where(block_diag_mask(), jnp.concatenate([packed, packed], axis=0), 0.0)


def fold_diag(d):
    row = lax.broadcasted_iota(jnp.int32, (HEAD, LANES), 0)
    col = lax.broadcasted_iota(jnp.int32, (HEAD, LANES), 1)
    return jnp.where(col % HEAD == row, d, 0.0)


def compose(a, b):
    both = dot3(jnp.concatenate([a[0], a[1]], axis=0), unfold(b[0]))
    return both[:HEAD], both[HEAD:] + b[1]


def put_packet(ref, slot, prod, state, decay):
    high, low = split(decay)
    row = lax.broadcasted_iota(jnp.int32, (16, LANES), 0)
    high, low = high.astype(jnp.float32), low.astype(jnp.float32)
    tail = jnp.where(row == 0, high, jnp.where(row == 1, low, 0.0))
    ref[slot, :HEAD, :] = (prod - fold_diag(decay)).astype(jnp.bfloat16)
    ref[slot, HEAD:LANES, :] = state.astype(jnp.bfloat16)
    ref[slot, LANES:, :] = tail.astype(jnp.bfloat16)


def get_packet(ref, slot):
    f32 = jnp.float32
    tail = ref[slot, LANES:, :].astype(f32)
    decay = tail[0:1] + tail[1:2]
    prod = ref[slot, :HEAD, :].astype(f32) + fold_diag(decay)
    return prod, ref[slot, HEAD:LANES, :].astype(f32), decay


def local_part(r_ref, k_ref, v_ref, dw_ref, lw_ref, between):
    steps = r_ref.shape[0]
    f32 = jnp.float32
    first = lax.broadcasted_iota(jnp.int32, (steps, LANES), 1) < HEAD
    row = lax.broadcasted_iota(jnp.int32, (steps, steps), 0)
    col = lax.broadcasted_iota(jnp.int32, (steps, steps), 1)
    r, k, v = (x[...].astype(f32) for x in (r_ref, k_ref, v_ref))
    log_decay = jax.nn.sigmoid(dw_ref[...]) * (-0.6065306597126334)
    ones = (row >= col).astype(jnp.bfloat16)
    h0 = log_decay.astype(jnp.bfloat16)
    rest = log_decay - h0.astype(f32)
    h1 = rest.astype(jnp.bfloat16)
    h2 = (rest - h1.astype(f32)).astype(jnp.bfloat16)
    total = dot1(ones, h0) + (dot1(ones, h1) + dot1(ones, h2))
    last = total[steps - 1 :, :]
    unit = k / jnp.maximum(jnp.sqrt(per_head_sum(k * k, first)), 1.0)
    insert = unit * jax.nn.sigmoid(lw_ref[...])
    undo = jnp.exp(-total)
    remaining = jnp.exp(last - total)
    a_bar = -unit * jnp.exp(total - log_decay)
    r_bar = r * jnp.exp(total)
    b_hat = insert * undo
    k_hat = k * undo
    right = split(jnp.concatenate([b_hat, k_hat], axis=0))
    left = jnp.concatenate([a_bar, r_bar], axis=0)
    first2 = jnp.concatenate([first, first], axis=0)
    grams = [
        dot3(jnp.where(first2 if h == 0 else ~first2, left, 0.0), right, NT) for h in (0, 1)
    ]
    strict, incl = row > col, row >= col
    ab = [jnp.where(strict, g[:steps, :steps], 0.0) for g in grams]
    ak = [jnp.where(strict, g[:steps, steps:], 0.0) for g in grams]
    rb = [jnp.where(incl, g[steps:, :steps], 0.0) for g in grams]
    rk = [jnp.where(incl, g[steps:, steps:], 0.0) for g in grams]
    vb = v_ref[...]

    def times_v(m):
        mh, ml = split(m)
        return dot1(mh, vb) + dot1(ml, vb)

    seeds = [jnp.concatenate([a_bar, times_v(m)], axis=1) for m in ak]
    ab16 = [m.astype(jnp.bfloat16) for m in ab]
    eye = (row == col).astype(f32)
    size = 1
    inv = None
    while size < steps:
        joined = (
            (row // (2 * size) == col // (2 * size))
            & ((row // size) % 2 == 1)
            & ((col // size) % 2 == 0)
        )
        parts = [jnp.where(joined, m, jnp.zeros_like(m)) for m in ab16]
        if inv is None:
            inv = [eye + p.astype(f32) for p in parts]
        else:
            t16 = [t.astype(jnp.bfloat16) for t in inv]
            mid = [dot1(t, p) for t, p in zip(t16, parts)]
            inv = [t + dot1(m, tt) for t, m, tt in zip(inv, mid, t16)]
        size *= 2
    between()
    inv16 = [t.astype(jnp.bfloat16) for t in inv]
    absp = [split(m) for m in ab]
    sol = [dot1(t, s) for t, s in zip(inv16, seeds)]
    for _ in range(2):
        res = [s - x + dot3(m, x) for s, x, m in zip(seeds, sol, absp)]
        sol = [x + dot1(t, e) for x, t, e in zip(sol, inv16, res)]
    w = jnp.where(first, sol[0][:, :LANES], sol[1][:, :LANES])
    u = jnp.where(first, sol[0][:, LANES:], sol[1][:, LANES:])
    b_end = split(insert * remaining)
    decay = jnp.exp(last)
    prod = fold(dot3(w, b_end, TN)) + fold_diag(decay)
    kh, kl = split(k * remaining)
    state = fold(dot3(u, b_end, TN) + dot1(vb, kh, TN) + dot1(vb, kl, TN))

    def outputs():
        outs = [dot3(m, x) for m, x in zip(rb, sol)]
        own = [times_v(m) for m in rk]
        q = r_bar + jnp.where(first, outs[0][:, :LANES], outs[1][:, :LANES])
        y = jnp.where(first, outs[0][:, LANES:] + own[0], outs[1][:, LANES:] + own[1])
        return q, y

    return prod, state, decay, outputs


def layer_kernel(
    r_hbm, k_hbm, v_hbm, dw_hbm, lw_hbm, gate_hbm, tw_hbm, hg_hbm, gain_hbm, wg_hbm, wu_hbm, wd_hbm,
    wo_hbm, res_hbm,
    out_ref,
    wall, wo, mixed, resid, after, normed, hid, parts, pair_in, pair_sum, last_in,
    r_ref, k_ref, v_ref, dw_ref, lw_ref, gate_ref, tw_ref, hg_ref, gain_ref,
    ybuf, zbuf, gbuf, q_s, y_s, ent, sums, acc,
    send, r_wo, r_z, r_q, r_y0, r_ya, r_yb, r_l1, r_l2, r_l3, x_l3, r_l4, x_l4, r_mx, r_pair, r_last, loc, ok,
):
    f32, bf16 = jnp.float32, jnp.bfloat16
    steps = r_ref.shape[0]
    depth, ff = wg_hbm.shape
    plane = NY * depth
    half = depth // 2
    ca = 2 * ff
    model = wo.shape[1]
    own_rows = out_ref.shape[0]
    sp, tp = lax.axis_index("sp"), lax.axis_index("tp")
    z, y = sp // NY, sp % NY
    x, c = tp // NC, tp % NC
    zg, zl = z // NG, z % NG

    def dev(zz=None, yy=None, tt=None):
        zz = z if zz is None else zz
        yy = y if yy is None else yy
        return (zz * NY + yy, tp if tt is None else tt)

    def rcopy(src, dst, s, r, device):
        return pltpu.make_async_remote_copy(
            src_ref=src, dst_ref=dst, send_sem=s, recv_sem=r, device_id=device, device_id_type=MESH
        )

    def wait_bytes(ref, sem):
        pltpu.make_async_copy(ref, ref, sem).wait()

    up, down = (z + 1) % NZ, (z + NZ - 1) % NZ
    others_y = [dev(yy=(y + d) % NY) for d in range(1, NY)]
    others_zl = [dev(zz=zg * NG + (zl + d) % NG) for d in range(1, NG)]
    others_zg = [dev(zz=((zg + d) % NG) * NG + zl) for d in range(1, NG)]
    others_tp = [dev(tt=(tp + d) % NTP) for d in range(1, NTP)]
    ring = [dev(zz=up), dev(zz=down)]

    barrier = pltpu.get_barrier_semaphore()
    greet = others_y + others_tp + ring
    for d in greet:
        pl.semaphore_signal(barrier, inc=1, device_id=d, device_id_type=MESH)

    my_row = pl.multiple_of(sp * depth, depth)
    wo_rows = lambda t: wo.at[pl.ds(pl.multiple_of(t * LANES, LANES), LANES), :]
    loads = [
        (wg_hbm, wall.at[pl.ds(my_row, depth), 0:ff]),
        (wu_hbm, wall.at[pl.ds(my_row, depth), ff:ca]),
        (wd_hbm, wall.at[pl.ds(my_row, depth), ca:]),
        (dw_hbm, dw_ref), (k_hbm, k_ref), (lw_hbm, lw_ref), (r_hbm, r_ref), (v_hbm, v_ref),
        (gate_hbm, gate_ref), (tw_hbm, tw_ref), (hg_hbm, hg_ref), (gain_hbm, gain_ref),
        (wo_hbm, wo_rows(tp)), (res_hbm, resid),
    ]
    loads = [pltpu.make_async_copy(a, b, loc.at[i]) for i, (a, b) in enumerate(loads)]
    for cp in loads[:8]:
        cp.start()

    def rows(zz, yy, lo=0, n=None):
        return pl.ds(pl.multiple_of(zz * plane + yy * depth + lo, half), depth if n is None else n)

    y2 = (y + 2) % NY
    lane = (y, y2)
    cols = (slice(0, ff), slice(ff, ca), slice(ca, 3 * ff))

    def block(zz, yy, part, lo=0, n=None):
        return wall.at[rows(zz, yy, lo, n), cols[part]]

    def ahead(s, dirn):
        return (z + NZ - s) % NZ if dirn == 0 else (z + s) % NZ

    def plane_of(i):
        return z if i == 0 else ahead((i + 1) // 2, (i - 1) % 2)

    def zstream(st, part, s):
        out = []
        for d in (0, 1):
            at = (0, depth) if s < HOPS - 1 else (half * d, half)
            ref = block(ahead(s, d), lane[st], part, *at)
            k = 3 * st + part
            out.append(rcopy(ref, ref, send.at[0], r_z.at[k, s], ring[d]))
        return out

    side = [dev(yy=(y + 1) % NY), dev(yy=(y + NY - 1) % NY)]

    def yside(part, i):
        ref = block(plane_of(i), y, part)
        group = [g for g, (lo, hi) in enumerate(GROUPS) if lo <= i < hi][0]
        sems = [r_ya.at[2 * part + (i >= EARLY)] if part < DOWN else r_yb.at[group]] * 2
        if i == 0:
            sems = [r_y0.at[part]] * 2
        return [rcopy(ref, ref, send.at[0], sems[d], side[d]) for d in (0, 1)]

    def across(part):
        out = []
        for d in (0, 1):
            ref = block(z, (y + NY - 1) % NY if d == 0 else (y + 1) % NY, part, half * d, half)
            out.append(rcopy(ref, ref, send.at[0], r_q.at[part], side[d]))
        return out

    def start(copies):
        for cp in copies:
            cp.start()

    def wait_recv(copies):
        for cp in copies:
            cp.wait_recv()

    def exchange(buf, slot, sem, s, targets):
        return [
            rcopy(buf.at[slot], buf.at[slot], send.at[s], sem.at[0], t)
            for d, t in enumerate(targets)
        ]

    def wo_same(d):
        t = ((x + d) % NX) * NC + c
        return rcopy(wo_hbm, wo_rows(tp), send.at[1], r_wo.at[d - 1], dev(tt=t))

    partner = dev(tt=x * NC + 1 - c)

    def wo_relay(d):
        ref = wo_rows(((x + NX - d) % NX) * NC + c)
        return rcopy(ref, ref, send.at[1], r_wo.at[NX - 1], partner)

    def tell(i):
        for zz in (z + 2**i, z + NZ - 2**i):
            pl.semaphore_signal(ok.at[i], inc=1, device_id=dev(zz=zz % NZ), device_id_type=MESH)

    def heard(i):
        pl.semaphore_wait(ok.at[i], 2)

    def enter():
        for cp in loads[:3]:
            cp.wait()
        with jax.named_scope("enter"):
            pl.semaphore_wait(barrier, len(greet))
        tell(0)
        for part in range(3):
            start(zstream(0, part, 0))
            start(yside(part, 0))
        for cp in loads[8:]:
            cp.start()
        for d in range(1, NX):
            wo_same(d).start()

    def new_at(s):
        return [2 * s + 1, 2 * s + 2] if s < HOPS - 1 else [2 * s + 1]

    def relay(part):
        wait_blocks(part, 2, r_y0.at[part])
        start(across(part))

    def wait_blocks(part, n, sem):
        wait_bytes(wall.at[0 : n * depth, cols[part]], sem)

    def q_open(part):
        wait_blocks(part, 1, r_q.at[part])
        start(zstream(1, part, 0))

    def p_step(part, s):
        wait_blocks(part, 2 if s < HOPS - 1 else 1, r_z.at[part, s])
        if s < HOPS - 1:
            start(zstream(0, part, s + 1))
        for i in new_at(s):
            start(yside(part, i))

    def q_step(part, s):
        wait_blocks(part, 2 if s < HOPS - 1 else 1, r_z.at[3 + part, s])
        if s < HOPS - 1:
            start(zstream(1, part, s + 1))

    work = []

    def job(f, *a):
        work.append(functools.partial(f, *a))

    for part in range(3):
        job(relay, part)
    for part in range(3):
        job(p_step, part, 0)
    job(q_open, 0)
    for s in range(1, HOPS + LAG + 1):
        for step, t in ((p_step, s), (q_step, s - 1)):
            for part in range(3):
                u = t - LAG if part == DOWN else t
                if (0 if step is q_step else 1) <= u < HOPS:
                    job(step, part, u)
                if s == 1 and step is p_step and part < DOWN:
                    job(q_open, part + 1)
    a_last = [f for f in work if f.args[0] < DOWN and f.func is q_step][-1]
    early = [f for f in work if f.func is q_step and f.args == (1, (EARLY - 2) // 2)][0]
    b_last = [f for f in work if f.args[0] == DOWN and f.func is q_step]

    def serve(n=None, until=None):
        while work and (n is None or n > 0) and (until is None or until in work):
            f = work.pop(0)
            n = None if n is None else n - 1
            with jax.named_scope("_".join([f.func.__name__] + [str(a) for a in f.args])):
                f()

    enter()
    for cp in loads[3:8]:
        cp.wait()
    with jax.named_scope("local"):
        prod, state, decay, outputs = local_part(
            r_ref, k_ref, v_ref, dw_ref, lw_ref, lambda: serve(MID)
        )
        put_packet(ybuf, y, prod, state, decay)
    l1 = exchange(ybuf, y, r_l1, 2, others_y)
    start(l1)
    heard(0)
    tell(1)
    serve(SERVE[0])
    with jax.named_scope("local_out"):
        q, y_own = outputs()
        q_s[...] = q
        y_s[...] = y_own
    for cp in loads[8:]:
        cp.wait()
    wo_relay(0).start()
    serve(SERVE[1])
    with jax.named_scope("wait_l1"):
        wait_bytes(ybuf.at[0:3], r_l1.at[0])

    def total(buf):
        m = [get_packet(buf, j) for j in range(4)]
        ab, cd = compose(m[0], m[1]), compose(m[2], m[3])
        return (*compose(ab, cd), (m[0][2] * m[1][2]) * (m[2][2] * m[3][2]))

    ident = (fold_diag(jnp.ones((1, LANES), f32)), jnp.zeros((HEAD, LANES), f32))

    def before(at, buf, count):
        ent[at] = jnp.concatenate(ident, axis=0)

        def step(j, _):
            p, u, _ = get_packet(buf, j)
            both = dot3(ent[at], unfold(p))
            ent[at, 0:HEAD, :] = both[:HEAD]
            ent[at, HEAD:, :] = both[HEAD:] + u
            return 0

        lax.fori_loop(0, count, step, 0)

    put_packet(zbuf, zl, *total(ybuf))
    heard(1)
    tell(2)
    l2 = exchange(zbuf, zl, r_l2, 3, others_zl)
    start(l2)
    with jax.named_scope("before_y"):
        before(0, ybuf, y)
    serve(SERVE[2])
    with jax.named_scope("wait_l2"):
        wait_bytes(zbuf.at[0:3], r_l2.at[0])
    put_packet(gbuf, zg, *total(zbuf))
    quarter = pl.ds(pl.multiple_of(y * (LANES // NY), LANES // NY), LANES // NY)

    def far(d):
        cuts = gbuf.at[zg, quarter, :], gbuf.at[zg, LANES:, :]
        return [
            rcopy(ref, ref, x_l3.at[d - 1], r_l3.at[d - 1], others_zg[d - 1]) for ref in cuts
        ]

    def share(d):
        ref = gbuf.at[zg - d, quarter, :]
        return [
            rcopy(ref, ref, x_l4.at[d - 1], r_l4.at[d - 1], others_y[e])
            for e in range(NY - 1)
        ]

    heard(2)
    for d in range(1, NG):
        @pl.when(zg + d < NG)
        def _(d=d):
            start(far(d))

    with jax.named_scope("before_z"):
        before(1, zbuf, zl)
    serve(SERVE[3])
    with jax.named_scope("wait_far"):
        for d in range(1, NG):
            @pl.when(zg >= d)
            def _(d=d):
                wait_bytes(gbuf.at[0, 0 : LANES // NY + 16, :], r_l3.at[d - 1])
                start(share(d))
    serve(SERVE[4])
    with jax.named_scope("relay"):
        for d in range(1, NX):
            wo_same(d).wait_recv()
            wo_relay(d).start()
    with jax.named_scope("wait_l3"):
        for d in range(1, NG):
            @pl.when(zg >= d)
            def _(d=d):
                wait_bytes(gbuf.at[0, 0 : LANES // NY * (NY - 1), :], r_l4.at[d - 1])

    def turn(j, s):
        p, u, _ = get_packet(gbuf, j)
        return dot3(s, unfold(p)) + u

    s_in = lax.fori_loop(0, zg, turn, jnp.zeros((HEAD, LANES), f32))
    for at in (1, 0):
        s_in = dot3(s_in, unfold(ent[at, 0:HEAD, :])) + ent[at, HEAD:, :]

    first = lax.broadcasted_iota(jnp.int32, (steps, LANES), 1) < HEAD
    yy = dot3(q_s[...], unfold(s_in), NT) + y_s[...]
    yy = yy - per_head_sum(yy, first) * (1.0 / HEAD)
    spread = per_head_sum(yy * yy, first) * (1.0 / HEAD)
    r, k, v = (a[...].astype(f32) for a in (r_ref, k_ref, v_ref))
    weight = jnp.concatenate([tw_ref[0:1, :], tw_ref[1:2, :]], axis=1)
    own = per_head_sum(r * k * weight, first) * v
    yy = yy * lax.rsqrt(spread + GROUP_EPS) * hg_ref[...] + own
    mixed[tp] = (yy * jax.nn.sigmoid(gate_ref[...].astype(f32))).astype(bf16)
    mx = [
        rcopy(mixed.at[tp], mixed.at[tp], send.at[4], r_mx.at[0], t)
        for d, t in enumerate(others_tp)
    ]
    start(mx)
    serve(SERVE[5])
    with jax.named_scope("wait_mixed"):
        wait_bytes(wo.at[0 : NX * LANES, :], r_wo.at[NX - 1])
        wait_bytes(mixed.at[0 : NTP - 1], r_mx.at[0])

    wide = 512

    def project(n, ss):
        cut = slice(n * wide, (n + 1) * wide)
        lhs = jnp.concatenate([mixed[j] for j in range(NTP)], axis=1)
        mix = jnp.dot(lhs, wo[:, cut], preferred_element_type=f32)
        mix = mix.astype(bf16).astype(f32)
        a = (resid[:, cut].astype(f32) + mix).astype(bf16).astype(f32)
        after[:, cut] = a
        return ss + jnp.sum(a * a, axis=-1, keepdims=True)

    ss = jnp.zeros((steps, 1), f32)
    for n in range(model // wide):
        with jax.named_scope("project"):
            ss = project(n, ss)
            sums[...] = ss
        serve(1)
        ss = sums[...]
    factor = lax.rsqrt(ss * (1.0 / model) + NORM_EPS)

    def scale(n, _):
        cut = pl.ds(pl.multiple_of(n * wide, wide), wide)
        normed[:, cut] = (after[:, cut] * factor * gain_ref[:, cut]).astype(bf16)
        return 0

    with jax.named_scope("scale"):
        lax.fori_loop(0, model // wide, scale, 0)
    def planes(lo, hi, part, at, n):
        total = None
        for i in range(lo, hi, 2):
            pair = [plane_of(i), plane_of(i + 1)]
            a = [normed[:, pl.ds(pl.multiple_of(p * plane, plane), plane)] for p in pair]
            w = [wall[rows(p, 0, 0, plane), part * ff + at : part * ff + at + n] for p in pair]
            d = jnp.dot(
                jnp.concatenate(a, axis=1), jnp.concatenate(w, axis=0), preferred_element_type=f32
            )
            total = d if total is None else total + d
        return total

    chunks = [(at, min(256, ff - at)) for at in range(0, ff, 256)]
    serve(until=early)
    with jax.named_scope("wait_early"):
        for part in range(DOWN):
            wait_blocks(part, 2 * (EARLY - 1), r_ya.at[2 * part])
    for at, n in chunks:
        for part in range(DOWN):
            with jax.named_scope("early"):
                acc[:, part * ff + at : part * ff + at + n] = planes(0, EARLY, part, at, n)
            serve(1)
    serve(until=a_last)
    serve(TAIL[0])
    with jax.named_scope("wait_gate_up"):
        for part in range(DOWN):
            wait_blocks(part, 2 * (NZ - EARLY), r_ya.at[2 * part + 1])

    with jax.named_scope("gate_up"):
        for at, n in chunks:
            g, u = (
                acc[:, part * ff + at : part * ff + at + n] + planes(EARLY, NZ, part, at, n)
                for part in range(DOWN)
            )
            hid[:, at : at + n] = (g / (1.0 + jnp.exp(-g)) * u).astype(bf16)

    serve(TAIL[1])

    def down_planes(lo, hi):
        for i in range(lo, hi, 2):
            both = [wall[rows(plane_of(j), 0, 0, plane), ca:] for j in range(i, min(i + 2, hi))]
            w = both[0] if len(both) == 1 else jnp.concatenate(both, axis=0)
            d = lax.dot_general(hid[...], w, NT, preferred_element_type=f32)
            for t in range(NTP):
                own = d[t * own_rows : (t + 1) * own_rows].astype(bf16)
                for j in range(len(both)):
                    parts[t % NC, i + j, t // NC] = own[:, j * plane : (j + 1) * plane]

    def pair(g):
        lo, hi = GROUPS[g]
        return rcopy(
            parts.at[1 - c, lo:hi], pair_in.at[lo:hi], send.at[5], r_pair.at[g], partner
        )

    def across_x(g):
        lo, hi = GROUPS[g]
        out = []
        for d in range(1, NX):
            xx = (x + d) % NX
            out.append(
                rcopy(
                    pair_sum.at[xx, lo:hi], last_in.at[d - 1, lo:hi], send.at[6],
                    r_last.at[g], dev(tt=xx * NC + c),
                )
            )
        return out

    def sum_pair(g):
        with jax.named_scope(f"pair_{g}"):
            pair(g).wait_recv()
        lo, hi = GROUPS[g]
        for xx in range(NX):
            both = parts[c, lo:hi, xx].astype(f32) + pair_in[lo:hi, xx].astype(f32)
            pair_sum[xx, lo:hi] = both.astype(bf16)
        start(across_x(g))

    for g, (lo, hi) in enumerate(GROUPS):
        if b_last[hi // 2 - 1] in work:
            serve(until=b_last[hi // 2 - 1])
        with jax.named_scope(f"wait_down_{g}"):
            wait_blocks(DOWN, 2 * (hi - max(lo, 1)), r_yb.at[g])
        with jax.named_scope(f"down_{g}"):
            down_planes(lo, hi)
        pair(g).start()
        if g > 0:
            sum_pair(g - 1)
    sum_pair(len(GROUPS) - 1)

    my_rows = pl.ds(pl.multiple_of(tp * own_rows, 8), own_rows)
    for g, (lo, hi) in enumerate(GROUPS):
        with jax.named_scope(f"last_{g}"):
            wait_bytes(last_in.at[:, lo:hi], r_last.at[g])
        for i in range(lo, hi):
            to = pl.ds(pl.multiple_of(plane_of(i) * plane, plane), plane)
            t = parts[c, i, x].astype(f32) + pair_in[i, x].astype(f32)
            for d in range(1, NX):
                t = t + last_in[d - 1, i].astype(f32)
            out_ref[:, to] = after[my_rows, to] + t

    drain = jax.named_scope("drain")
    drain.__enter__()
    wait_bytes(wall.at[0 : (2 * (2 * HOPS - 1) + 2 * NZ + 1) * depth, :], send.at[0])
    wait_bytes(wo.at[0 : (2 * NX - 1) * LANES, :], send.at[1])
    wait_bytes(ybuf.at[0:3], send.at[2])
    wait_bytes(zbuf.at[0:3], send.at[3])
    for d in range(1, NG):
        @pl.when(zg + d < NG)
        def _(d=d):
            wait_bytes(gbuf.at[0, 0 : LANES // NY + 16, :], x_l3.at[d - 1])
    for d in range(1, NG):
        @pl.when(zg >= d)
        def _(d=d):
            wait_bytes(gbuf.at[0, 0 : LANES // NY * (NY - 1), :], x_l4.at[d - 1])
    wait_bytes(mixed.at[0 : NTP - 1], send.at[4])
    wait_bytes(pair_in, send.at[5])
    wait_bytes(pair_sum.at[0 : NX - 1], send.at[6])
    drain.__exit__(None, None, None)


DOWN = 2
EARLY = 12
LAG = 1
GROUPS = ((0, 5), (5, 9), (9, 13), (13, 15), (15, 16))
VMEM_MB = 58
MID = 1
SERVE = (5, 5, 4, 7, 8, 10)
TAIL = (0, 1)


def layer(r, k, v, dw, lw, gate, tw, hg, wg, wu, wd, gain, wo, residual):
    f32, bf16 = jnp.float32, jnp.bfloat16
    steps = r.shape[0]
    depth, ff = wg.shape
    model = residual.shape[1]
    own_rows = steps // NTP
    vmem = pl.BlockSpec(memory_space=pltpu.VMEM)
    dma = pltpu.SemaphoreType.DMA
    return pl.pallas_call(
        layer_kernel,
        in_specs=[pl.BlockSpec(memory_space=pltpu.HBM)] * 14,
        out_specs=vmem,
        out_shape=pltpu.VMEM((own_rows, model), f32),
        scratch_shapes=[
            pltpu.VMEM((model, 3 * ff), bf16),
            pltpu.VMEM((NTP * LANES, model), bf16),
            pltpu.VMEM((NTP, steps, LANES), bf16),
            pltpu.VMEM((steps, model), bf16),
            pltpu.VMEM((steps, model), f32),
            pltpu.VMEM((steps, model), bf16),
            pltpu.VMEM((steps, ff), bf16),
            pltpu.VMEM((NC, NZ, NX, own_rows, LANES), bf16),
            pltpu.VMEM((NZ, NX, own_rows, LANES), bf16),
            pltpu.VMEM((NX, NZ, own_rows, LANES), bf16),
            pltpu.VMEM((NX - 1, NZ, own_rows, LANES), bf16),
            *[pltpu.VMEM(a.shape, a.dtype) for a in (r, k, v, dw, lw, gate, tw, hg, gain)],
            pltpu.VMEM((NY, PACKET, LANES), bf16),
            pltpu.VMEM((NG, PACKET, LANES), bf16),
            pltpu.VMEM((NG, PACKET, LANES), bf16),
            pltpu.VMEM((steps, LANES), f32),
            pltpu.VMEM((steps, LANES), f32),
            pltpu.VMEM((2, LANES, LANES), f32),
            pltpu.VMEM((steps, 1), f32),
            pltpu.VMEM((steps, 2 * ff), f32),
            dma((7,)),
            dma((NX,)),
            dma((6, HOPS)),
            dma((3,)),
            dma((3,)),
            dma((2 * DOWN,)),
            dma((len(GROUPS),)),
            dma((1,)),
            dma((1,)),
            dma((NG - 1,)),
            dma((NG - 1,)),
            dma((NG - 1,)),
            dma((NG - 1,)),
            dma((1,)),
            dma((len(GROUPS),)),
            dma((len(GROUPS),)),
            dma((14,)),
            pltpu.SemaphoreType.REGULAR((3,)),
        ],
        compiler_params=pltpu.CompilerParams(
            collective_id=0, has_side_effects=True, vmem_limit_bytes=VMEM_MB * 1024 * 1024
        ),
        cost_estimate=pl.CostEstimate(
            flops=3_000_000_000, bytes_accessed=8_000_000, transcendentals=1_000_000
        ),
        name="layer",
    )(r, k, v, dw, lw, gate, tw, hg, gain, wg, wu, wd, wo, residual)


def per_device(r, k, v, dw, lw, gate, tw, hg, w_out, residual, gain, w_gate, w_up, w_down):
    return layer(
        r, k, v, dw, lw, gate, tw, hg.reshape(1, -1), w_gate, w_up, w_down.T,
        gain.reshape(1, -1), w_out, residual,
    ).astype(jnp.bfloat16)


def solution(mesh):
    split_both = P("sp", "tp")
    placed = (split_both,) * 6 + (
        P("tp", None),
        P("tp"),
        P("tp", None),
        P("sp", None),
        P(),
        split_both,
        split_both,
        P("tp", "sp"),
    )
    return jax.shard_map(
        per_device, mesh=mesh, in_specs=placed, out_specs=P(("sp", "tp"), None), check_vma=False
    )
```

```python
import functools

import jax
import jax.numpy as jnp
from jax import lax
from jax.experimental import pallas as pl
from jax.experimental.pallas import tpu as pltpu
from jax.sharding import PartitionSpec as P

HEAD = 64
LANES = 2 * HEAD
GROUP_EPS = 0.00064
NORM_EPS = 1e-06
NN = (((1,), (0,)), ((), ()))
NT = (((1,), (1,)), ((), ()))
TN = (((0,), (0,)), ((), ()))
NX, NY, NZ, NC = 4, 4, 16, 2
NTP = NX * NC
NG = 4
HOPS = NZ // 2
MESH = pl.DeviceIdType.MESH
PACKET = LANES + 16


def split(x):
    high = x.astype(jnp.bfloat16)
    return high, (x - high.astype(jnp.float32)).astype(jnp.bfloat16)


def dot1(a, b, dims=NN):
    return lax.dot_general(
        a.astype(jnp.bfloat16), b.astype(jnp.bfloat16), dims, preferred_element_type=jnp.float32
    )


def dot3(a, b, dims=NN):
    ah, al = a if isinstance(a, tuple) else split(a)
    bh, bl = b if isinstance(b, tuple) else split(b)
    d = functools.partial(
        lax.dot_general, dimension_numbers=dims, preferred_element_type=jnp.float32
    )
    return d(ah, bh) + (d(ah, bl) + d(al, bh))


def per_head_sum(x, first):
    s0 = jnp.sum(jnp.where(first, x, 0.0), axis=-1, keepdims=True)
    s1 = jnp.sum(jnp.where(first, 0.0, x), axis=-1, keepdims=True)
    return jnp.where(first, s0, s1)


def block_diag_mask():
    row = lax.broadcasted_iota(jnp.int32, (LANES, LANES), 0)
    col = lax.broadcasted_iota(jnp.int32, (LANES, LANES), 1)
    return row // HEAD == col // HEAD


def fold(full):
    kept = jnp.where(block_diag_mask(), full, 0.0)
    return kept[:HEAD] + kept[HEAD:]


def unfold(packed):
    return jnp.where(block_diag_mask(), jnp.concatenate([packed, packed], axis=0), 0.0)


def fold_diag(d):
    row = lax.broadcasted_iota(jnp.int32, (HEAD, LANES), 0)
    col = lax.broadcasted_iota(jnp.int32, (HEAD, LANES), 1)
    return jnp.where(col % HEAD == row, d, 0.0)


def compose(a, b):
    both = dot3(jnp.concatenate([a[0], a[1]], axis=0), unfold(b[0]))
    return both[:HEAD], both[HEAD:] + b[1]


def put_packet(ref, slot, prod, state, decay):
    high, low = split(decay)
    row = lax.broadcasted_iota(jnp.int32, (16, LANES), 0)
    high, low = high.astype(jnp.float32), low.astype(jnp.float32)
    tail = jnp.where(row == 0, high, jnp.where(row == 1, low, 0.0))
    ref[slot, :HEAD, :] = (prod - fold_diag(decay)).astype(jnp.bfloat16)
    ref[slot, HEAD:LANES, :] = state.astype(jnp.bfloat16)
    ref[slot, LANES:, :] = tail.astype(jnp.bfloat16)


def get_packet(ref, slot):
    f32 = jnp.float32
    tail = ref[slot, LANES:, :].astype(f32)
    decay = tail[0:1] + tail[1:2]
    prod = ref[slot, :HEAD, :].astype(f32) + fold_diag(decay)
    return prod, ref[slot, HEAD:LANES, :].astype(f32), decay


def local_part(r_ref, k_ref, v_ref, dw_ref, lw_ref, between):
    steps = r_ref.shape[0]
    f32 = jnp.float32
    first = lax.broadcasted_iota(jnp.int32, (steps, LANES), 1) < HEAD
    row = lax.broadcasted_iota(jnp.int32, (steps, steps), 0)
    col = lax.broadcasted_iota(jnp.int32, (steps, steps), 1)
    r, k, v = (x[...].astype(f32) for x in (r_ref, k_ref, v_ref))
    log_decay = jax.nn.sigmoid(dw_ref[...]) * (-0.6065306597126334)
    ones = (row >= col).astype(jnp.bfloat16)
    h0 = log_decay.astype(jnp.bfloat16)
    rest = log_decay - h0.astype(f32)
    h1 = rest.astype(jnp.bfloat16)
    h2 = (rest - h1.astype(f32)).astype(jnp.bfloat16)
    total = dot1(ones, h0) + (dot1(ones, h1) + dot1(ones, h2))
    last = total[steps - 1 :, :]
    unit = k / jnp.maximum(jnp.sqrt(per_head_sum(k * k, first)), 1.0)
    insert = unit * jax.nn.sigmoid(lw_ref[...])
    undo = jnp.exp(-total)
    remaining = jnp.exp(last - total)
    a_bar = -unit * jnp.exp(total - log_decay)
    r_bar = r * jnp.exp(total)
    b_hat = insert * undo
    k_hat = k * undo
    right = split(jnp.concatenate([b_hat, k_hat], axis=0))
    left = jnp.concatenate([a_bar, r_bar], axis=0)
    first2 = jnp.concatenate([first, first], axis=0)
    grams = [
        dot3(jnp.where(first2 if h == 0 else ~first2, left, 0.0), right, NT) for h in (0, 1)
    ]
    strict, incl = row > col, row >= col
    ab = [jnp.where(strict, g[:steps, :steps], 0.0) for g in grams]
    ak = [jnp.where(strict, g[:steps, steps:], 0.0) for g in grams]
    rb = [jnp.where(incl, g[steps:, :steps], 0.0) for g in grams]
    rk = [jnp.where(incl, g[steps:, steps:], 0.0) for g in grams]
    vb = v_ref[...]

    def times_v(m):
        mh, ml = split(m)
        return dot1(mh, vb) + dot1(ml, vb)

    seeds = [jnp.concatenate([a_bar, times_v(m)], axis=1) for m in ak]
    ab16 = [m.astype(jnp.bfloat16) for m in ab]
    eye = (row == col).astype(f32)
    size = 1
    inv = None
    while size < steps:
        joined = (
            (row // (2 * size) == col // (2 * size))
            & ((row // size) % 2 == 1)
            & ((col // size) % 2 == 0)
        )
        parts = [jnp.where(joined, m, jnp.zeros_like(m)) for m in ab16]
        if inv is None:
            inv = [eye + p.astype(f32) for p in parts]
        else:
            t16 = [t.astype(jnp.bfloat16) for t in inv]
            mid = [dot1(t, p) for t, p in zip(t16, parts)]
            inv = [t + dot1(m, tt) for t, m, tt in zip(inv, mid, t16)]
        size *= 2
    between()
    inv16 = [t.astype(jnp.bfloat16) for t in inv]
    absp = [split(m) for m in ab]
    sol = [dot1(t, s) for t, s in zip(inv16, seeds)]
    for _ in range(2):
        res = [s - x + dot3(m, x) for s, x, m in zip(seeds, sol, absp)]
        sol = [x + dot1(t, e) for x, t, e in zip(sol, inv16, res)]
    w = jnp.where(first, sol[0][:, :LANES], sol[1][:, :LANES])
    u = jnp.where(first, sol[0][:, LANES:], sol[1][:, LANES:])
    b_end = split(insert * remaining)
    decay = jnp.exp(last)
    prod = fold(dot3(w, b_end, TN)) + fold_diag(decay)
    kh, kl = split(k * remaining)
    state = fold(dot3(u, b_end, TN) + dot1(vb, kh, TN) + dot1(vb, kl, TN))

    def outputs():
        outs = [dot3(m, x) for m, x in zip(rb, sol)]
        own = [times_v(m) for m in rk]
        q = r_bar + jnp.where(first, outs[0][:, :LANES], outs[1][:, :LANES])
        y = jnp.where(first, outs[0][:, LANES:] + own[0], outs[1][:, LANES:] + own[1])
        return q, y

    return prod, state, decay, outputs


def layer_kernel(
    r_hbm, k_hbm, v_hbm, dw_hbm, lw_hbm, gate_hbm, tw_hbm, hg_hbm, gain_hbm, wg_hbm, wu_hbm, wd_hbm,
    wo_hbm, res_hbm,
    out_ref,
    wall, wo, mixed, resid, after, normed, hid, parts, pair_in, pair_sum, last_in,
    r_ref, k_ref, v_ref, dw_ref, lw_ref, gate_ref, tw_ref, hg_ref, gain_ref,
    ybuf, zbuf, gbuf, q_s, y_s, ent, sums, acc,
    send, r_wo, r_z, r_q, r_y0, r_ya, r_yb, r_l1, r_l2, r_l3, x_l3, r_l4, x_l4, r_mx, r_pair, r_last, loc, ok,
):
    f32, bf16 = jnp.float32, jnp.bfloat16
    steps = r_ref.shape[0]
    depth, ff = wg_hbm.shape
    plane = NY * depth
    half = depth // 2
    ca = 2 * ff
    model = wo.shape[1]
    own_rows = out_ref.shape[0]
    sp, tp = lax.axis_index("sp"), lax.axis_index("tp")
    z, y = sp // NY, sp % NY
    x, c = tp // NC, tp % NC
    zg, zl = z // NG, z % NG

    def dev(zz=None, yy=None, tt=None):
        zz = z if zz is None else zz
        yy = y if yy is None else yy
        return (zz * NY + yy, tp if tt is None else tt)

    def rcopy(src, dst, s, r, device):
        return pltpu.make_async_remote_copy(
            src_ref=src, dst_ref=dst, send_sem=s, recv_sem=r, device_id=device, device_id_type=MESH
        )

    def wait_bytes(ref, sem):
        pltpu.make_async_copy(ref, ref, sem).wait()

    up, down = (z + 1) % NZ, (z + NZ - 1) % NZ
    others_y = [dev(yy=(y + d) % NY) for d in range(1, NY)]
    others_zl = [dev(zz=zg * NG + (zl + d) % NG) for d in range(1, NG)]
    others_zg = [dev(zz=((zg + d) % NG) * NG + zl) for d in range(1, NG)]
    others_tp = [dev(tt=(tp + d) % NTP) for d in range(1, NTP)]
    ring = [dev(zz=up), dev(zz=down)]

    barrier = pltpu.get_barrier_semaphore()
    greet = others_y + others_tp + ring
    for d in greet:
        pl.semaphore_signal(barrier, inc=1, device_id=d, device_id_type=MESH)

    my_row = pl.multiple_of(sp * depth, depth)
    wo_rows = lambda t: wo.at[pl.ds(pl.multiple_of(t * LANES, LANES), LANES), :]
    loads = [
        (wg_hbm, wall.at[pl.ds(my_row, depth), 0:ff]),
        (wu_hbm, wall.at[pl.ds(my_row, depth), ff:ca]),
        (wd_hbm, wall.at[pl.ds(my_row, depth), ca:]),
        (dw_hbm, dw_ref), (k_hbm, k_ref), (lw_hbm, lw_ref), (r_hbm, r_ref), (v_hbm, v_ref),
        (gate_hbm, gate_ref), (tw_hbm, tw_ref), (hg_hbm, hg_ref), (gain_hbm, gain_ref),
        (wo_hbm, wo_rows(tp)), (res_hbm, resid),
    ]
    loads = [pltpu.make_async_copy(a, b, loc.at[i]) for i, (a, b) in enumerate(loads)]
    for cp in loads[:8]:
        cp.start()

    def rows(zz, yy, lo=0, n=None):
        return pl.ds(pl.multiple_of(zz * plane + yy * depth + lo, half), depth if n is None else n)

    y2 = (y + 2) % NY
    lane = (y, y2)
    cols = (slice(0, ff), slice(ff, ca), slice(ca, 3 * ff))

    def block(zz, yy, part, lo=0, n=None):
        return wall.at[rows(zz, yy, lo, n), cols[part]]

    def ahead(s, dirn):
        return (z + NZ - s) % NZ if dirn == 0 else (z + s) % NZ

    def plane_of(i):
        return z if i == 0 else ahead((i + 1) // 2, (i - 1) % 2)

    def zstream(st, part, s):
        out = []
        for d in (0, 1):
            at = (0, depth) if s < HOPS - 1 else (half * d, half)
            ref = block(ahead(s, d), lane[st], part, *at)
            k = 3 * st + part
            out.append(rcopy(ref, ref, send.at[0], r_z.at[k, s], ring[d]))
        return out

    side = [dev(yy=(y + 1) % NY), dev(yy=(y + NY - 1) % NY)]

    def yside(part, i):
        ref = block(plane_of(i), y, part)
        group = [g for g, (lo, hi) in enumerate(GROUPS) if lo <= i < hi][0]
        sems = [r_ya.at[2 * part + (i >= EARLY)] if part < DOWN else r_yb.at[group]] * 2
        if i == 0:
            sems = [r_y0.at[part]] * 2
        return [rcopy(ref, ref, send.at[0], sems[d], side[d]) for d in (0, 1)]

    def across(part):
        out = []
        for d in (0, 1):
            ref = block(z, (y + NY - 1) % NY if d == 0 else (y + 1) % NY, part, half * d, half)
            out.append(rcopy(ref, ref, send.at[0], r_q.at[part], side[d]))
        return out

    def start(copies):
        for cp in copies:
            cp.start()

    def wait_recv(copies):
        for cp in copies:
            cp.wait_recv()

    def exchange(buf, slot, sem, s, targets):
        return [
            rcopy(buf.at[slot], buf.at[slot], send.at[s], sem.at[0], t)
            for d, t in enumerate(targets)
        ]

    def wo_same(d):
        t = ((x + d) % NX) * NC + c
        return rcopy(wo_hbm, wo_rows(tp), send.at[1], r_wo.at[d - 1], dev(tt=t))

    partner = dev(tt=x * NC + 1 - c)

    def wo_relay(d):
        ref = wo_rows(((x + NX - d) % NX) * NC + c)
        return rcopy(ref, ref, send.at[1], r_wo.at[NX - 1], partner)

    def tell(i):
        for zz in (z + 2**i, z + NZ - 2**i):
            pl.semaphore_signal(ok.at[i], inc=1, device_id=dev(zz=zz % NZ), device_id_type=MESH)

    def heard(i):
        pl.semaphore_wait(ok.at[i], 2)

    def enter():
        for cp in loads[:3]:
            cp.wait()
        with jax.named_scope("enter"):
            pl.semaphore_wait(barrier, len(greet))
        tell(0)
        for part in range(3):
            start(zstream(0, part, 0))
            start(yside(part, 0))
        for cp in loads[8:]:
            cp.start()
        for d in range(1, NX):
            wo_same(d).start()

    def new_at(s):
        return [2 * s + 1, 2 * s + 2] if s < HOPS - 1 else [2 * s + 1]

    def relay(part):
        wait_blocks(part, 2, r_y0.at[part])
        start(across(part))

    def wait_blocks(part, n, sem):
        wait_bytes(wall.at[0 : n * depth, cols[part]], sem)

    def q_open(part):
        wait_blocks(part, 1, r_q.at[part])
        start(zstream(1, part, 0))

    def p_step(part, s):
        wait_blocks(part, 2 if s < HOPS - 1 else 1, r_z.at[part, s])
        if s < HOPS - 1:
            start(zstream(0, part, s + 1))
        for i in new_at(s):
            start(yside(part, i))

    def q_step(part, s):
        wait_blocks(part, 2 if s < HOPS - 1 else 1, r_z.at[3 + part, s])
        if s < HOPS - 1:
            start(zstream(1, part, s + 1))

    work = []

    def job(f, *a):
        work.append(functools.partial(f, *a))

    for part in range(3):
        job(relay, part)
    for part in range(3):
        job(p_step, part, 0)
    job(q_open, 0)
    for s in range(1, HOPS + LAG + 1):
        for step, t in ((p_step, s), (q_step, s - 1)):
            for part in range(3):
                u = t - LAG if part == DOWN else t
                if (0 if step is q_step else 1) <= u < HOPS:
                    job(step, part, u)
                if s == 1 and step is p_step and part < DOWN:
                    job(q_open, part + 1)
    a_last = [f for f in work if f.args[0] < DOWN and f.func is q_step][-1]
    early = [f for f in work if f.func is q_step and f.args == (1, (EARLY - 2) // 2)][0]
    b_last = [f for f in work if f.args[0] == DOWN and f.func is q_step]

    def serve(n=None, until=None):
        while work and (n is None or n > 0) and (until is None or until in work):
            f = work.pop(0)
            n = None if n is None else n - 1
            with jax.named_scope("_".join([f.func.__name__] + [str(a) for a in f.args])):
                f()

    enter()
    for cp in loads[3:8]:
        cp.wait()
    with jax.named_scope("local"):
        prod, state, decay, outputs = local_part(
            r_ref, k_ref, v_ref, dw_ref, lw_ref, lambda: serve(MID)
        )
        put_packet(ybuf, y, prod, state, decay)
    l1 = exchange(ybuf, y, r_l1, 2, others_y)
    start(l1)
    heard(0)
    tell(1)
    serve(SERVE[0])
    with jax.named_scope("local_out"):
        q, y_own = outputs()
        q_s[...] = q
        y_s[...] = y_own
    for cp in loads[8:]:
        cp.wait()
    wo_relay(0).start()
    serve(SERVE[1])
    with jax.named_scope("wait_l1"):
        wait_bytes(ybuf.at[0:3], r_l1.at[0])

    def total(buf):
        m = [get_packet(buf, j) for j in range(4)]
        ab, cd = compose(m[0], m[1]), compose(m[2], m[3])
        return (*compose(ab, cd), (m[0][2] * m[1][2]) * (m[2][2] * m[3][2]))

    ident = (fold_diag(jnp.ones((1, LANES), f32)), jnp.zeros((HEAD, LANES), f32))

    def before(at, buf, count):
        ent[at] = jnp.concatenate(ident, axis=0)

        def step(j, _):
            p, u, _ = get_packet(buf, j)
            both = dot3(ent[at], unfold(p))
            ent[at, 0:HEAD, :] = both[:HEAD]
            ent[at, HEAD:, :] = both[HEAD:] + u
            return 0

        lax.fori_loop(0, count, step, 0)

    put_packet(zbuf, zl, *total(ybuf))
    heard(1)
    tell(2)
    l2 = exchange(zbuf, zl, r_l2, 3, others_zl)
    start(l2)
    with jax.named_scope("before_y"):
        before(0, ybuf, y)
    serve(SERVE[2])
    with jax.named_scope("wait_l2"):
        wait_bytes(zbuf.at[0:3], r_l2.at[0])
    put_packet(gbuf, zg, *total(zbuf))
    quarter = pl.ds(pl.multiple_of(y * (LANES // NY), LANES // NY), LANES // NY)

    def far(d):
        cuts = gbuf.at[zg, quarter, :], gbuf.at[zg, LANES:, :]
        return [
            rcopy(ref, ref, x_l3.at[d - 1], r_l3.at[d - 1], others_zg[d - 1]) for ref in cuts
        ]

    def share(d):
        ref = gbuf.at[zg - d, quarter, :]
        return [
            rcopy(ref, ref, x_l4.at[d - 1], r_l4.at[d - 1], others_y[e])
            for e in range(NY - 1)
        ]

    heard(2)
    for d in range(1, NG):
        @pl.when(zg + d < NG)
        def _(d=d):
            start(far(d))

    with jax.named_scope("before_z"):
        before(1, zbuf, zl)
    serve(SERVE[3])
    with jax.named_scope("wait_far"):
        for d in range(1, NG):
            @pl.when(zg >= d)
            def _(d=d):
                wait_bytes(gbuf.at[0, 0 : LANES // NY + 16, :], r_l3.at[d - 1])
                start(share(d))
    serve(SERVE[4])
    with jax.named_scope("relay"):
        for d in range(1, NX):
            wo_same(d).wait_recv()
            wo_relay(d).start()
    with jax.named_scope("wait_l3"):
        for d in range(1, NG):
            @pl.when(zg >= d)
            def _(d=d):
                wait_bytes(gbuf.at[0, 0 : LANES // NY * (NY - 1), :], r_l4.at[d - 1])

    def turn(j, s):
        p, u, _ = get_packet(gbuf, j)
        return dot3(s, unfold(p)) + u

    s_in = lax.fori_loop(0, zg, turn, jnp.zeros((HEAD, LANES), f32))
    for at in (1, 0):
        s_in = dot3(s_in, unfold(ent[at, 0:HEAD, :])) + ent[at, HEAD:, :]

    first = lax.broadcasted_iota(jnp.int32, (steps, LANES), 1) < HEAD
    yy = dot3(q_s[...], unfold(s_in), NT) + y_s[...]
    yy = yy - per_head_sum(yy, first) * (1.0 / HEAD)
    spread = per_head_sum(yy * yy, first) * (1.0 / HEAD)
    r, k, v = (a[...].astype(f32) for a in (r_ref, k_ref, v_ref))
    weight = jnp.concatenate([tw_ref[0:1, :], tw_ref[1:2, :]], axis=1)
    own = per_head_sum(r * k * weight, first) * v
    yy = yy * lax.rsqrt(spread + GROUP_EPS) * hg_ref[...] + own
    mixed[tp] = (yy * jax.nn.sigmoid(gate_ref[...].astype(f32))).astype(bf16)
    mx = [
        rcopy(mixed.at[tp], mixed.at[tp], send.at[4], r_mx.at[0], t)
        for d, t in enumerate(others_tp)
    ]
    start(mx)
    serve(SERVE[5])
    with jax.named_scope("wait_mixed"):
        wait_bytes(wo.at[0 : NX * LANES, :], r_wo.at[NX - 1])
        wait_bytes(mixed.at[0 : NTP - 1], r_mx.at[0])

    wide = 512

    def project(n, ss):
        cut = slice(n * wide, (n + 1) * wide)
        lhs = jnp.concatenate([mixed[j] for j in range(NTP)], axis=1)
        mix = jnp.dot(lhs, wo[:, cut], preferred_element_type=f32)
        mix = mix.astype(bf16).astype(f32)
        a = (resid[:, cut].astype(f32) + mix).astype(bf16).astype(f32)
        after[:, cut] = a
        return ss + jnp.sum(a * a, axis=-1, keepdims=True)

    ss = jnp.zeros((steps, 1), f32)
    for n in range(model // wide):
        with jax.named_scope("project"):
            ss = project(n, ss)
            sums[...] = ss
        serve(1)
        ss = sums[...]
    factor = lax.rsqrt(ss * (1.0 / model) + NORM_EPS)

    def scale(n, _):
        cut = pl.ds(pl.multiple_of(n * wide, wide), wide)
        normed[:, cut] = (after[:, cut] * factor * gain_ref[:, cut]).astype(bf16)
        return 0

    with jax.named_scope("scale"):
        lax.fori_loop(0, model // wide, scale, 0)
    def planes(lo, hi, part, at, n):
        total = None
        for i in range(lo, hi, 2):
            pair = [plane_of(i), plane_of(i + 1)]
            a = [normed[:, pl.ds(pl.multiple_of(p * plane, plane), plane)] for p in pair]
            w = [wall[rows(p, 0, 0, plane), part * ff + at : part * ff + at + n] for p in pair]
            d = jnp.dot(
                jnp.concatenate(a, axis=1), jnp.concatenate(w, axis=0), preferred_element_type=f32
            )
            total = d if total is None else total + d
        return total

    chunks = [(at, min(256, ff - at)) for at in range(0, ff, 256)]
    serve(until=early)
    with jax.named_scope("wait_early"):
        for part in range(DOWN):
            wait_blocks(part, 2 * (EARLY - 1), r_ya.at[2 * part])
    for at, n in chunks:
        for part in range(DOWN):
            with jax.named_scope("early"):
                acc[:, part * ff + at : part * ff + at + n] = planes(0, EARLY, part, at, n)
            serve(1)
    serve(until=a_last)
    serve(TAIL[0])
    with jax.named_scope("wait_gate_up"):
        for part in range(DOWN):
            wait_blocks(part, 2 * (NZ - EARLY), r_ya.at[2 * part + 1])

    with jax.named_scope("gate_up"):
        for at, n in chunks:
            g, u = (
                acc[:, part * ff + at : part * ff + at + n] + planes(EARLY, NZ, part, at, n)
                for part in range(DOWN)
            )
            hid[:, at : at + n] = (g / (1.0 + jnp.exp(-g)) * u).astype(bf16)

    serve(TAIL[1])

    def down_planes(lo, hi):
        for i in range(lo, hi, 2):
            both = [wall[rows(plane_of(j), 0, 0, plane), ca:] for j in range(i, min(i + 2, hi))]
            w = both[0] if len(both) == 1 else jnp.concatenate(both, axis=0)
            d = lax.dot_general(hid[...], w, NT, preferred_element_type=f32)
            for t in range(NTP):
                own = d[t * own_rows : (t + 1) * own_rows].astype(bf16)
                for j in range(len(both)):
                    parts[t % NC, i + j, t // NC] = own[:, j * plane : (j + 1) * plane]

    def pair(g):
        lo, hi = GROUPS[g]
        return rcopy(
            parts.at[1 - c, lo:hi], pair_in.at[lo:hi], send.at[5], r_pair.at[g], partner
        )

    def across_x(g):
        lo, hi = GROUPS[g]
        out = []
        for d in range(1, NX):
            xx = (x + d) % NX
            out.append(
                rcopy(
                    pair_sum.at[xx, lo:hi], last_in.at[d - 1, lo:hi], send.at[6],
                    r_last.at[g], dev(tt=xx * NC + c),
                )
            )
        return out

    def sum_pair(g):
        with jax.named_scope(f"pair_{g}"):
            pair(g).wait_recv()
        lo, hi = GROUPS[g]
        for xx in range(NX):
            both = parts[c, lo:hi, xx].astype(f32) + pair_in[lo:hi, xx].astype(f32)
            pair_sum[xx, lo:hi] = both.astype(bf16)
        start(across_x(g))

    for g, (lo, hi) in enumerate(GROUPS):
        if b_last[hi // 2 - 1] in work:
            serve(until=b_last[hi // 2 - 1])
        with jax.named_scope(f"wait_down_{g}"):
            wait_blocks(DOWN, 2 * (hi - max(lo, 1)), r_yb.at[g])
        with jax.named_scope(f"down_{g}"):
            down_planes(lo, hi)
        pair(g).start()
        if g > 0:
            sum_pair(g - 1)
    sum_pair(len(GROUPS) - 1)

    my_rows = pl.ds(pl.multiple_of(tp * own_rows, 8), own_rows)
    for g, (lo, hi) in enumerate(GROUPS):
        with jax.named_scope(f"last_{g}"):
            wait_bytes(last_in.at[:, lo:hi], r_last.at[g])
        for i in range(lo, hi):
            to = pl.ds(pl.multiple_of(plane_of(i) * plane, plane), plane)
            t = parts[c, i, x].astype(f32) + pair_in[i, x].astype(f32)
            for d in range(1, NX):
                t = t + last_in[d - 1, i].astype(f32)
            out_ref[:, to] = after[my_rows, to] + t

    drain = jax.named_scope("drain")
    drain.__enter__()
    wait_bytes(wall.at[0 : (2 * (2 * HOPS - 1) + 2 * NZ + 1) * depth, :], send.at[0])
    wait_bytes(wo.at[0 : (2 * NX - 1) * LANES, :], send.at[1])
    wait_bytes(ybuf.at[0:3], send.at[2])
    wait_bytes(zbuf.at[0:3], send.at[3])
    for d in range(1, NG):
        @pl.when(zg + d < NG)
        def _(d=d):
            wait_bytes(gbuf.at[0, 0 : LANES // NY + 16, :], x_l3.at[d - 1])
    for d in range(1, NG):
        @pl.when(zg >= d)
        def _(d=d):
            wait_bytes(gbuf.at[0, 0 : LANES // NY * (NY - 1), :], x_l4.at[d - 1])
    wait_bytes(mixed.at[0 : NTP - 1], send.at[4])
    wait_bytes(pair_in, send.at[5])
    wait_bytes(pair_sum.at[0 : NX - 1], send.at[6])
    drain.__exit__(None, None, None)


DOWN = 2
EARLY = 12
LAG = 1
GROUPS = ((0, 3), (3, 7), (7, 11), (11, 15), (15, 16))
VMEM_MB = 58
MID = 1
SERVE = (5, 5, 4, 7, 8, 10)
TAIL = (0, 1)


def layer(r, k, v, dw, lw, gate, tw, hg, wg, wu, wd, gain, wo, residual):
    f32, bf16 = jnp.float32, jnp.bfloat16
    steps = r.shape[0]
    depth, ff = wg.shape
    model = residual.shape[1]
    own_rows = steps // NTP
    vmem = pl.BlockSpec(memory_space=pltpu.VMEM)
    dma = pltpu.SemaphoreType.DMA
    return pl.pallas_call(
        layer_kernel,
        in_specs=[pl.BlockSpec(memory_space=pltpu.HBM)] * 14,
        out_specs=vmem,
        out_shape=pltpu.VMEM((own_rows, model), f32),
        scratch_shapes=[
            pltpu.VMEM((model, 3 * ff), bf16),
            pltpu.VMEM((NTP * LANES, model), bf16),
            pltpu.VMEM((NTP, steps, LANES), bf16),
            pltpu.VMEM((steps, model), bf16),
            pltpu.VMEM((steps, model), f32),
            pltpu.VMEM((steps, model), bf16),
            pltpu.VMEM((steps, ff), bf16),
            pltpu.VMEM((NC, NZ, NX, own_rows, LANES), bf16),
            pltpu.VMEM((NZ, NX, own_rows, LANES), bf16),
            pltpu.VMEM((NX, NZ, own_rows, LANES), bf16),
            pltpu.VMEM((NX - 1, NZ, own_rows, LANES), bf16),
            *[pltpu.VMEM(a.shape, a.dtype) for a in (r, k, v, dw, lw, gate, tw, hg, gain)],
            pltpu.VMEM((NY, PACKET, LANES), bf16),
            pltpu.VMEM((NG, PACKET, LANES), bf16),
            pltpu.VMEM((NG, PACKET, LANES), bf16),
            pltpu.VMEM((steps, LANES), f32),
            pltpu.VMEM((steps, LANES), f32),
            pltpu.VMEM((2, LANES, LANES), f32),
            pltpu.VMEM((steps, 1), f32),
            pltpu.VMEM((steps, 2 * ff), f32),
            dma((7,)),
            dma((NX,)),
            dma((6, HOPS)),
            dma((3,)),
            dma((3,)),
            dma((2 * DOWN,)),
            dma((len(GROUPS),)),
            dma((1,)),
            dma((1,)),
            dma((NG - 1,)),
            dma((NG - 1,)),
            dma((NG - 1,)),
            dma((NG - 1,)),
            dma((1,)),
            dma((len(GROUPS),)),
            dma((len(GROUPS),)),
            dma((14,)),
            pltpu.SemaphoreType.REGULAR((3,)),
        ],
        compiler_params=pltpu.CompilerParams(
            collective_id=0, has_side_effects=True, vmem_limit_bytes=VMEM_MB * 1024 * 1024
        ),
        cost_estimate=pl.CostEstimate(
            flops=3_000_000_000, bytes_accessed=8_000_000, transcendentals=1_000_000
        ),
        name="layer",
    )(r, k, v, dw, lw, gate, tw, hg, gain, wg, wu, wd, wo, residual)


def per_device(r, k, v, dw, lw, gate, tw, hg, w_out, residual, gain, w_gate, w_up, w_down):
    return layer(
        r, k, v, dw, lw, gate, tw, hg.reshape(1, -1), w_gate, w_up, w_down.T,
        gain.reshape(1, -1), w_out, residual,
    ).astype(jnp.bfloat16)


def solution(mesh):
    split_both = P("sp", "tp")
    placed = (split_both,) * 6 + (
        P("tp", None),
        P("tp"),
        P("tp", None),
        P("sp", None),
        P(),
        split_both,
        split_both,
        P("tp", "sp"),
    )
    return jax.shard_map(
        per_device, mesh=mesh, in_specs=placed, out_specs=P(("sp", "tp"), None), check_vma=False
    )
```
